32 devices in a mesh: ep: 8 (over z, y), tp: 4 (over x, core).
Axes of the slice: x: 2, y: 2, z: 4, core: 2. Of those that a mesh axis runs over, the one named last changes fastest.
Arguments:
- mixer_in: bfloat16 [3072, 2048], P(('ep', 'tp')), may hold values from -6 to 6
- expert_in: bfloat16 [3072, 2048], P(('ep', 'tp')), may hold values from -6 to 6
- mixer_gain: float32 [2048], replicated, may hold values from 0.1 to 1.9
- in_gate_weight: bfloat16 [2048, 2048], P(None, 'tp'), may hold values from -0.125 to 0.125
- out_gate_weight: bfloat16 [2048, 2048], P(None, 'tp'), may hold values from -0.125 to 0.125
- value_weight: bfloat16 [2048, 2048], P(None, 'tp'), may hold values from -0.125 to 0.125
- conv_taps: float32 [3, 2048], replicated, may hold values from -3 to 3
- mixer_proj: bfloat16 [2048, 2048], P(None, 'tp'), may hold values from -0.125 to 0.125
- expert_gain: float32 [2048], replicated, may hold values from 0.1 to 1.9
- route_ids: int32 [3072, 2], P('ep'), may hold values from 0 to 7, all different within a row; in each aligned block of 96 rows (0 to 95, 96 to 191, ...) at most 48 rows name the same one
- route_weights: float32 [3072, 2], P('ep'), may hold values from 0.1 to 1
- gate_weight: bfloat16 [8, 2048, 1024], P('ep', None, 'tp'), may hold values from -0.125 to 0.125
- up_weight: bfloat16 [8, 2048, 1024], P('ep', None, 'tp'), may hold values from -0.125 to 0.125
- down_weight: bfloat16 [8, 1024, 2048], P('ep', None, 'tp'), may hold values from -0.1875 to 0.1875
Outputs:
- mixer_out: bfloat16 [3072, 2048], P('ep', 'tp')
- expert_out: bfloat16 [3072, 2048], P('ep', 'tp')
The draws below stay inside these ranges and needn't reach their ends.
Inputs may be any that keep to these rules, and one draw needn't show every extreme that they name: `route_ids`: each row names 2 different experts. In each aligned block of 96 rows no expert is named by more than 48 rows, a bound that some block reaches.
All inputs are finite; a program needn't handle non-finite values.
Results may differ from the reference program's by a relative error of at most 0.0076.
Values may be sent and summed in bfloat16 or wider, within the bound.
A program may use at most 64 MiB of HBM per device.

```python
import math
import jax
import jax.numpy as jnp
import numpy as np
from jax import lax

D = 2048
F = 1024
CONV = 3
TOP_K = 2
TOK_DEV = 96
EXPERTS = 8
CAPQ = 48
TOKENS = 3072
N_EP = 8
N_TP = 4


def shard_levels(rng, extent, pieces, low, high):
    def one(position, blocks):
        draws = jax.random.uniform(jax.random.fold_in(jax.random.fold_in(rng, 6), position), (blocks,), jnp.float32, low / len(pieces), high / len(pieces))
        return jnp.repeat(jnp.exp(draws), extent[position] // blocks).reshape((-1,) + (1,) * (len(extent) - position - 1))

    level = one(*pieces[0])
    for cut in pieces[1:]:
        level = level * one(*cut)
    return level


def routed_block(own_key, own, number, rows, amount, top, limit, slope):
    order = jax.random.permutation(own_key, amount)
    heavy_load, common = portions_of(amount, rows * top, limit, slope, True), portions_of(amount, rows * top, limit, slope, False)
    places = jnp.arange(amount)

    def named(lengths, rotation):
        used = int((lengths > 0).sum())
        fixed = max(1, used // 4)
        passed = fixed + (places - fixed + rotation * (used - fixed)) % max(1, amount - fixed)
        return jnp.zeros((amount,), jnp.int32).at[order[jnp.where(places < fixed, places, passed)]].set(jnp.asarray(lengths, jnp.int32))

    lengths = jnp.where(number % 4 == 0, named(heavy_load, number // 4), named(common, number - number // 4 - 1))
    mixed = jax.random.permutation(jax.random.fold_in(own, 3), amount)
    donor, receiver = mixed[0:amount // 2 * 2:2], mixed[1:amount // 2 * 2:2]
    margin = jnp.minimum(lengths[donor] - 1, limit - lengths[receiver]) // 2
    margin = jnp.where((donor == order[0]) | (receiver == order[0]) | (lengths[receiver] == 0), 0, jnp.maximum(margin, 0))
    passed = jax.random.randint(jax.random.fold_in(own, 4), (amount // 2,), 0, 1 << 20) % (margin + 1)
    lengths = lengths.at[donor].add(-passed).at[receiver].add(passed)
    items = jnp.searchsorted(jnp.cumsum(lengths), jnp.arange(rows * top), side="right").astype(jnp.int32)
    table = items.reshape(top, rows).T
    table = table[jax.random.permutation(jax.random.fold_in(own, 1), rows)]
    rotation = jax.random.randint(jax.random.fold_in(own, 2), (rows, 1), 0, top)
    return jnp.take_along_axis(table, (jnp.arange(top)[None, :] + rotation) % top, axis=1)


def portions_of(count, total, most, skew, full):
    loads = [(1 << 20) // math.isqrt(standing ** skew) + 1 for standing in range(1, count + 1)]
    largest = most if full else min(most, max(-(-total // count), total * loads[0] // sum(loads)))
    least = 1 if total - largest >= count - 1 else 0
    given, surplus = [largest] + [least] * (count - 1), total - largest - least * (count - 1)
    while surplus > 0:
        candidates = [i for i in range(1, count) if given[i] < largest] or [i for i in range(1, count) if given[i] < most]
        mass, left = sum([loads[i] for i in candidates]), surplus
        for i in candidates:
            extra = min(most - given[i], max(1, left * loads[i] // mass), surplus)
            given[i] = given[i] + extra
            surplus = surplus - extra
    return np.array(given)


def centred(stream_key, dims, width, limit, pieces=(), held_as=jnp.bfloat16):
    loudness = shard_levels(stream_key, dims, pieces, -0.22, 0.18) if pieces else 1.0
    entries = jax.random.normal(stream_key, dims, jnp.float32) * width * loudness
    return jnp.minimum(jnp.maximum(entries, -limit), limit).astype(held_as)


def setup_inputs(seed: int = 0) -> dict:
    key_of = jax.random.split(jax.random.key(seed), 15)
    mixer_in = centred(key_of[0], (TOKENS, D), 1.0, 6.0, ((0, 32),))
    expert_in = centred(key_of[1], (TOKENS, D), 1.0, 6.0, ((0, 32),))
    mixer_gain = jnp.clip(1.0 + 0.18 * jax.random.normal(key_of[2], (D,), jnp.float32), 0.1, 1.9)
    in_gate_weight = centred(key_of[3], (D, D), D ** -0.5, 0.125, ((1, 4),))
    out_gate_weight = centred(key_of[4], (D, D), D ** -0.5, 0.125, ((1, 4),))
    value_weight = centred(key_of[5], (D, D), D ** -0.5, 0.125, ((1, 4),))
    conv_taps = centred(key_of[6], (CONV, D), 0.577, 3.0, (), jnp.float32)
    mixer_proj = centred(key_of[7], (D, D), D ** -0.5, 0.125, ((1, 4),))
    expert_gain = jnp.clip(1.0 + 0.18 * jax.random.normal(key_of[8], (D,), jnp.float32), 0.1, 1.9)
    route_ids_keys = jax.random.split(jax.random.fold_in(key_of[9], 1), TOKENS // TOK_DEV)
    route_ids_turns = jax.random.permutation(jax.random.fold_in(key_of[9], 3), TOKENS // TOK_DEV)
    route_ids = jax.vmap(lambda own, number: routed_block(jax.random.fold_in(key_of[9], 2), own, number, TOK_DEV, EXPERTS, TOP_K, CAPQ, 1))(route_ids_keys, route_ids_turns).reshape((TOKENS, TOP_K))
    route_weights = jnp.clip(jnp.exp(math.log(1.0) - 2.3025851 * jax.random.uniform(key_of[10], (TOKENS, TOP_K), jnp.float32) ** shard_levels(key_of[10], (TOKENS, TOP_K), ((0, 8),), -0.2, 0.2)), 0.1, 1.0)
    gate_weight = centred(key_of[11], (EXPERTS, D, F), D ** -0.5, 0.125, ((0, 8), (2, 4)))
    up_weight = centred(key_of[12], (EXPERTS, D, F), D ** -0.5, 0.125, ((0, 8), (2, 4)))
    down_weight = centred(key_of[13], (EXPERTS, F, D), F ** -0.5, 0.1875, ((0, 8), (2, 4)))
    return dict(mixer_in=mixer_in, expert_in=expert_in, mixer_gain=mixer_gain, in_gate_weight=in_gate_weight, out_gate_weight=out_gate_weight, value_weight=value_weight, conv_taps=conv_taps, mixer_proj=mixer_proj, expert_gain=expert_gain, route_ids=route_ids, route_weights=route_weights, gate_weight=gate_weight, up_weight=up_weight, down_weight=down_weight)


norm_eps = 1e-06

def rms_rows(values, gain_row):
    wide = values.astype(jnp.float32)
    scale = lax.rsqrt(lax.optimization_barrier(jnp.mean(wide * wide, axis=-1, keepdims=True)) + norm_eps)
    return (wide * scale * gain_row.astype(jnp.float32)).astype(jnp.bfloat16)

def place_slots(route_ids, group_rows, experts, slot_cap):
    row_total, top_count = route_ids.shape
    groups = row_total // group_rows
    labels = jnp.arange(experts, dtype=jnp.int32)
    onehot = (route_ids.reshape(groups, group_rows * top_count)[:, :, None] == labels[None, None, :]).astype(jnp.int32)
    earlier = jnp.cumsum(onehot, axis=1) - onehot
    within = lax.optimization_barrier(jnp.sum(earlier * onehot, axis=2))
    slot_index = jnp.arange(groups, dtype=jnp.int32)[:, None] * slot_cap + within
    return slot_index.reshape(row_total, top_count).astype(jnp.int32)

def reference(mixer_in, expert_in, mixer_gain, in_gate_weight, out_gate_weight, value_weight, conv_taps, mixer_proj, expert_gain, route_ids, route_weights, gate_weight, up_weight, down_weight):
    mixer_normed = rms_rows(mixer_in, mixer_gain)
    in_gate = jnp.dot(mixer_normed, in_gate_weight, preferred_element_type=jnp.float32)
    out_gate = jnp.dot(mixer_normed, out_gate_weight, preferred_element_type=jnp.float32)
    values = jnp.dot(mixer_normed, value_weight, preferred_element_type=jnp.float32)
    product = (in_gate * values).astype(jnp.bfloat16)
    product = lax.optimization_barrier(product)
    row_count = product.shape[0]
    tap_count = conv_taps.shape[0]
    padded = jnp.pad(product.astype(jnp.float32), ((tap_count - 1, 0), (0, 0)))
    tap_rows = conv_taps.astype(jnp.float32)
    conv_sum = tap_rows[0] * padded[0:row_count]
    for tap_index in range(1, tap_count):
        conv_sum = conv_sum + tap_rows[tap_index] * padded[tap_index:tap_index + row_count]
    gated = (out_gate * conv_sum).astype(jnp.bfloat16)
    mixer_out = jnp.dot(gated, mixer_proj, preferred_element_type=jnp.float32).astype(jnp.bfloat16)
    expert_normed = rms_rows(expert_in, expert_gain)
    token_count = expert_normed.shape[0]
    top_count = route_ids.shape[1]
    per_expert = N_EP * N_TP * CAPQ
    slot_index = place_slots(route_ids, TOK_DEV, EXPERTS, CAPQ)
    flat_index = (route_ids * per_expert + slot_index).reshape(-1)
    shares = (route_weights / lax.optimization_barrier(jnp.sum(route_weights, axis=1, keepdims=True))).reshape(-1)
    row_table = jnp.full((EXPERTS * per_expert,), token_count, jnp.int32).at[flat_index].set(jnp.repeat(jnp.arange(token_count, dtype=jnp.int32), top_count))
    share_table = jnp.zeros((EXPERTS * per_expert,), jnp.float32).at[flat_index].set(shares)
    padded_rows = jnp.concatenate([expert_normed, jnp.zeros((1, expert_normed.shape[1]), jnp.bfloat16)], axis=0)

    def one_expert(running, expert_idx):
        rows_here = lax.dynamic_slice_in_dim(row_table, expert_idx * per_expert, per_expert)
        share_here = lax.dynamic_slice_in_dim(share_table, expert_idx * per_expert, per_expert)
        chosen = padded_rows[rows_here]
        gate_pre = jnp.dot(chosen, gate_weight[expert_idx], preferred_element_type=jnp.float32)
        up_pre = jnp.dot(chosen, up_weight[expert_idx], preferred_element_type=jnp.float32)
        hidden = (jax.nn.silu(gate_pre) * up_pre).astype(jnp.bfloat16)
        result = jnp.dot(hidden, down_weight[expert_idx], preferred_element_type=jnp.float32).astype(jnp.bfloat16)
        running = running.at[rows_here].add(share_here[:, None] * result.astype(jnp.float32))
        return (running, None)
    running, _ = lax.scan(one_expert, jnp.zeros((token_count + 1, expert_normed.shape[1]), jnp.float32), jnp.arange(EXPERTS, dtype=jnp.int32))
    expert_out = running[:token_count].astype(jnp.bfloat16)
    return (mixer_out, expert_out)
```

```python
import functools

import jax
import jax.numpy as jnp
from jax import lax
from jax.experimental import pallas as pl
from jax.experimental.pallas import tpu as pltpu
from jax.sharding import PartitionSpec as P

norm_eps = 1e-06


def passed_along(value, axis, steps):
    count = lax.axis_size(axis)
    leading, last = (max(0, -steps), min(count, count - steps))
    return lax.ppermute(value, axis, [(source, source + steps) for source in range(leading, last)])


def rms_rows(values, gain_row):
    wide = values.astype(jnp.float32)
    scale = lax.rsqrt(jnp.mean(wide * wide, axis=-1, keepdims=True) + norm_eps)
    return (wide * scale * gain_row).astype(jnp.bfloat16)


def place_slots(route_ids, group_rows, experts, slot_cap):
    row_total, top_count = route_ids.shape
    groups = row_total // group_rows
    labels = jnp.arange(experts, dtype=jnp.int32)
    onehot = (
        route_ids.reshape(groups, group_rows * top_count)[:, :, None] == labels[None, None, :]
    ).astype(jnp.int32)
    earlier = jnp.cumsum(onehot, axis=1) - onehot
    within = jnp.sum(earlier * onehot, axis=2)
    slot_index = jnp.arange(groups, dtype=jnp.int32)[:, None] * slot_cap + within
    return slot_index.reshape(row_total, top_count)


def on_device(
    mixer_in,
    expert_in,
    mixer_gain,
    in_gate_weight,
    out_gate_weight,
    value_weight,
    conv_taps,
    mixer_proj,
    expert_gain,
    route_ids,
    route_weights,
    gate_weight,
    up_weight,
    down_weight,
):
    tok_dev = mixer_in.shape[0]
    tp_count = lax.axis_size("tp")
    ep_count = lax.axis_size("ep")
    top_count = route_ids.shape[1]
    experts = ep_count * gate_weight.shape[0]
    slot_cap = max(2, 2 * tok_dev * top_count // experts)
    tp_index = lax.axis_index("tp")
    mixer_normed = rms_rows(mixer_in, mixer_gain)
    expert_normed = rms_rows(expert_in, expert_gain)
    block_slot = place_slots(route_ids, tok_dev, experts, slot_cap)
    mixer_rows = lax.all_gather(mixer_normed, "tp", axis=0, tiled=True)
    send_ids = lax.dynamic_slice_in_dim(route_ids, tp_index * tok_dev, tok_dev, 0)
    send_slot = (
        lax.dynamic_slice_in_dim(block_slot, tp_index * tok_dev, tok_dev, 0) - tp_index * slot_cap
    )
    source_count = expert_normed.shape[0]
    flat_index = (send_ids * slot_cap + send_slot).reshape(-1)
    row_table = (
        jnp.full((experts * slot_cap,), source_count, jnp.int32)
        .at[flat_index]
        .set(jnp.repeat(jnp.arange(source_count, dtype=jnp.int32), top_count))
    )
    padded_rows = jnp.concatenate(
        [expert_normed, jnp.zeros((1, expert_normed.shape[1]), jnp.bfloat16)], axis=0
    )
    outgoing = padded_rows[row_table].reshape(experts, slot_cap, expert_normed.shape[1])
    arrived = lax.all_to_all(outgoing, "ep", split_axis=0, concat_axis=0, tiled=True)
    arrived = lax.all_gather(arrived, "tp", axis=1, tiled=True)
    chan_width = in_gate_weight.shape[1]
    in_gate = jnp.dot(mixer_rows, in_gate_weight, preferred_element_type=jnp.float32)
    out_gate = jnp.dot(mixer_rows, out_gate_weight, preferred_element_type=jnp.float32)
    values = jnp.dot(mixer_rows, value_weight, preferred_element_type=jnp.float32)
    product = (in_gate * values).astype(jnp.bfloat16)
    tap_count = conv_taps.shape[0]
    rim_rows = passed_along(product[product.shape[0] - (tap_count - 1) :], "ep", 1)
    extended = jnp.concatenate([rim_rows, product], axis=0).astype(jnp.float32)
    tap_rows = lax.dynamic_slice_in_dim(conv_taps, tp_index * chan_width, chan_width, 1)
    row_count = product.shape[0]
    conv_sum = tap_rows[0] * extended[0:row_count]
    for tap_index in range(1, tap_count):
        conv_sum = conv_sum + tap_rows[tap_index] * extended[tap_index : tap_index + row_count]
    gated = (out_gate * conv_sum).astype(jnp.bfloat16)
    slots_in = arrived.reshape(-1, arrived.shape[2])
    gate_pre = jnp.dot(slots_in, gate_weight[0], preferred_element_type=jnp.float32)
    up_pre = jnp.dot(slots_in, up_weight[0], preferred_element_type=jnp.float32)
    hidden = (jax.nn.silu(gate_pre) * up_pre).astype(jnp.bfloat16)
    down_slice = down_weight[0]
    gated_all, hidden_all = (
        lax.all_gather(gated, "tp", axis=1, tiled=True),
        lax.all_gather(hidden, "tp", axis=1, tiled=True),
    )
    mixer_sum = jnp.dot(gated_all, mixer_proj, preferred_element_type=jnp.float32)
    expert_sum = jnp.dot(hidden_all, down_slice, preferred_element_type=jnp.float32)
    mixer_out = mixer_sum.astype(jnp.bfloat16)
    results = expert_sum.astype(jnp.bfloat16).reshape(ep_count, -1, expert_sum.shape[1])
    returned = lax.all_to_all(results, "ep", split_axis=0, concat_axis=0, tiled=True)
    back_index = (route_ids * (tp_count * slot_cap) + block_slot).reshape(-1)
    picked = returned.reshape(-1, returned.shape[2])[back_index].reshape(
        route_ids.shape[0], top_count, -1
    )
    shares = route_weights / jnp.sum(route_weights, axis=1, keepdims=True)
    expert_out = jnp.sum(picked.astype(jnp.float32) * shares[:, :, None], axis=1).astype(
        jnp.bfloat16
    )
    return (mixer_out, expert_out)


MESH = pl.DeviceIdType.MESH
F32 = jnp.float32
BF16 = jnp.bfloat16
VMEM_BYTES = 60 * 1024 * 1024


def dot(a, b):
    return jnp.dot(a, b, preferred_element_type=F32)


def prepare(slot_cap, me, expert_in, expert_gain, ids, weights, own_rows, outgoing, partner_table, combine):
    tok_dev = expert_in.shape[0]
    picks, all_rows = ids.shape
    blocks = all_rows // tok_dev
    slots = combine.shape[1]
    experts = slots // slot_cap
    rows = own_rows[...]
    partner = (me + 2) % blocks
    filler = jnp.zeros((8 - 2 * picks, all_rows), F32)
    columns = jnp.transpose(jnp.concatenate([ids[...].astype(F32), weights[...], filler], axis=0))
    below = (
        lax.broadcasted_iota(jnp.int32, (tok_dev, tok_dev), 1)
        < lax.broadcasted_iota(jnp.int32, (tok_dev, tok_dev), 0)
    ).astype(BF16)
    labels = lax.broadcasted_iota(jnp.int32, (tok_dev, 128), 1)
    places = lax.broadcasted_iota(jnp.int32, (tok_dev, slots), 1)
    chosen = jnp.zeros((tok_dev, slots), F32)
    theirs = jnp.zeros((tok_dev, slots), F32)
    for block in range(blocks):
        part = slice(block * tok_dev, (block + 1) * tok_dev)
        named = [columns[part, k : k + 1].astype(jnp.int32) for k in range(picks)]
        share = [columns[part, picks + k : picks + k + 1] for k in range(picks)]
        total = functools.reduce(jnp.add, share)
        hot = [(labels == n).astype(F32) for n in named]
        rank = dot(below, functools.reduce(jnp.add, hot).astype(BF16))
        mixed = jnp.zeros((tok_dev, slots), F32)
        sent = jnp.zeros((tok_dev, slots), F32)
        for k in range(picks):
            within = jnp.sum(rank * hot[k], axis=1, keepdims=True).astype(jnp.int32)
            spot = places == named[k] * slot_cap + within
            mixed = mixed + jnp.where(spot, share[k] / total, 0.0)
            sent = sent + jnp.where(spot, 1.0, 0.0)
        combine[part, :] = mixed
        chosen = jnp.where(me == block, sent, chosen)
        theirs = jnp.where(partner == block, sent, theirs)
    table = jnp.transpose(chosen).astype(BF16)
    partner_table[...] = jnp.transpose(theirs).astype(BF16).reshape(experts, slot_cap, tok_dev)
    for expert in range(experts):
        outgoing[expert] = dot(table[expert * slot_cap : (expert + 1) * slot_cap], rows).astype(BF16)


MIX_AT = (0, 3, 4, 5, 8, 9)

LAGS = (0, 1, 2, 4, 5)

DISP, F2, F1, G1, H2, H1, HG, RET, DISP2 = range(9)
M2, M1, MG, Q2, Q1, QG, RIM, DX = range(8)


def chunk_order(count):
    half = count // 2
    far, close = list(range(half, count)), list(range(half))
    return close[:1] + far + close[1:]


def exchange_kernel(
    mixer_in, expert_in, mixer_gain, expert_gain, ids, shares, all_taps,
    w_in, w_out, w_val, w_proj, w_gate, w_up, w_down,
    mixer_out, expert_out,
    v_in, v_out, v_val, v_proj, v_gate, v_up, v_down,
    v_mixer, v_expert, v_mixer_gain, v_expert_gain, v_ids, v_shares, taps,
    normed, own_rows, outgoing, partner_table, combine,
    rows, arrived, hid, res, returned, gates, ext, rim_out, rim_in, gated, dense, outgoing2,
    send, recv, send1, recv1, wsem, fsem,
):
    count = outgoing.shape[0]
    group, tok_dev, width = rows.shape
    half = count // 2
    chan = v_in.shape[1]
    slot_cap = outgoing.shape[1]
    hid_width = v_gate.shape[1]
    e = lax.axis_index("ep")
    t = lax.axis_index("tp")
    t1 = t + 1 - 2 * (t % 2)
    t2 = (t + 2) % group
    t3 = (t1 + 2) % group

    firsts = [
        pltpu.make_async_copy(a, b, fsem.at[n])
        for n, (a, b) in enumerate(
            [(expert_in, v_expert), (expert_gain, v_expert_gain), (ids, v_ids), (shares, v_shares),
             (mixer_in, v_mixer), (mixer_gain, v_mixer_gain),
             (all_taps.at[:, pl.ds(pl.multiple_of(t * chan, 128), chan)], taps)]
        )
    ]
    for load in firsts:
        load.start()
    loads = [
        pltpu.make_async_copy(a, b, wsem.at[n])
        for n, (a, b) in enumerate(
            [(w_in, v_in), (w_val, v_val), (w_out, v_out), (w_gate.at[0], v_gate),
             (w_up.at[0], v_up), (w_down.at[0], v_down), (w_proj, v_proj)]
        )
    ]
    def mixed_with(s):
        value, bit = 0, 1
        while bit < count:
            value = value + ((e // bit + s // bit) % 2) * bit
            bit *= 2
        return value

    order = chunk_order(count)

    def shift_of(i):
        return functools.reduce(jnp.add, [jnp.where(i == n, s, 0) for n, s in enumerate(order)])

    def source_of(i):
        return mixed_with(shift_of(i))

    barrier = pltpu.get_barrier_semaphore()
    for s in range(1, count):
        pl.semaphore_signal(barrier, inc=1, device_id=(mixed_with(s), t), device_id_type=MESH)
    for peer in (t1, t2):
        pl.semaphore_signal(barrier, inc=1, device_id=(e, peer), device_id_type=MESH)
    for load in firsts[:4]:
        load.wait()
    for load in loads:
        load.start()
    own_rows[...] = rms_rows(v_expert[...], v_expert_gain[...])
    pl.semaphore_wait(barrier, count + 1)

    def chunk(kind, i, src, dst, dev):
        return pltpu.make_async_remote_copy(
            src_ref=src, dst_ref=dst, send_sem=send.at[kind, i], recv_sem=recv.at[kind, i],
            device_id=dev, device_id_type=MESH,
        )

    def once(kind, src, dst, dev):
        return pltpu.make_async_remote_copy(
            src_ref=src, dst_ref=dst, send_sem=send1.at[kind], recv_sem=recv1.at[kind],
            device_id=dev, device_id_type=MESH,
        )

    near, across = (e, t1), (e, t2)
    after = ((e + 1) % count, t)

    def disp(i):
        return chunk(DISP, i, outgoing.at[source_of(i)], arrived.at[e, t], (source_of(i), t))

    def ret(i):
        return chunk(RET, i, res.at[source_of(i)], returned.at[e], (source_of(i), t))

    def came(kind, i, dst):
        chunk(kind, i, dst, dst, near).wait_recv()

    def came_once(kind, dst):
        once(kind, dst, dst, near).wait_recv()

    def disp2(i):
        src = source_of(i)
        return chunk(DISP2, i, outgoing2.at[shift_of(i)], arrived.at[e, t2], (src, t))

    once(DX, own_rows, dense, across).start()
    prepare(
        slot_cap, t, v_expert, v_expert_gain, v_ids, v_shares, own_rows, outgoing, partner_table, combine
    )

    def start_disp(i, carry):
        @pl.when(shift_of(i) != 0)
        def _():
            disp(i).start()

        return carry

    lax.fori_loop(0, count, start_disp, 0)
    for load in firsts[4:]:
        load.wait()
    normed[...] = rms_rows(v_mixer[...], v_mixer_gain[...])
    rows[t] = normed[...]
    arrived[e, t] = outgoing[e]
    once(M1, normed, rows.at[t], near).start()
    came_once(DX, dense)

    def pass_on(i, carry):
        shift = shift_of(i)

        @pl.when(shift < half)
        def _():
            picked = dot(partner_table[source_of(i)], dense[...]).astype(BF16)

            @pl.when(shift == 0)
            def _():
                arrived[e, t2] = picked

            @pl.when(shift != 0)
            def _():
                outgoing2[shift] = picked
                disp2(i).start()

        return carry

    lax.fori_loop(0, count, pass_on, 0)

    def finish(i):
        src = source_of(i)
        came(H1, i, hid.at[src, t1])
        came(HG, i, hid.at[src, t3])
        total = dot(hid[src, 0], v_down[0:hid_width, :])
        for other in range(1, group):
            total += dot(hid[src, other], v_down[other * hid_width : (other + 1) * hid_width, :])
        total = total.astype(BF16).reshape(group, slot_cap, chan)

        @pl.when(shift_of(i) != 0)
        def _():
            res[src] = total
            ret(i).start()

        @pl.when(shift_of(i) == 0)
        def _():
            returned[src] = total

    def hand_hidden(i):
        src = source_of(i)
        came(H2, i, hid.at[src, t2])
        chunk(HG, i, hid.at[src, t2], hid.at[src, t2], near).start()

    def expand(i):
        src = source_of(i)
        came(F1, i, arrived.at[src, t1])
        came(G1, i, arrived.at[src, t3])
        x = arrived[src].reshape(group * slot_cap, width)
        gate = dot(x, v_gate[...])
        up = dot(x, v_up[...])
        hid[src, t] = (gate / (1.0 + jnp.exp(-gate)) * up).astype(BF16)
        chunk(H2, i, hid.at[src, t], hid.at[src, t], across).start()
        chunk(H1, i, hid.at[src, t], hid.at[src, t], near).start()

    def hand_rows(i):
        src = source_of(i)
        shift = shift_of(i)

        @pl.when(shift >= half)
        def _():
            came(F2, i, arrived.at[src, t2])

        @pl.when((shift < half) & (shift != 0))
        def _():
            came(DISP2, i, arrived.at[src, t2])

        chunk(G1, i, arrived.at[src, t2], arrived.at[src, t2], near).start()

    def take(i):
        src = source_of(i)

        @pl.when(shift_of(i) != 0)
        def _():
            came(DISP, i, arrived.at[src, t])

        @pl.when(shift_of(i) >= half)
        def _():
            chunk(F2, i, arrived.at[src, t], arrived.at[src, t], across).start()

        chunk(F1, i, arrived.at[src, t], arrived.at[src, t], near).start()

    all_rows = group * tok_dev
    tile = 256

    def mixer_products():
        came_once(M1, rows.at[t1])
        came_once(MG, rows.at[t3])

        def one(n, carry):
            cols = pl.ds(pl.multiple_of(n * tile, tile), tile)
            x = rows[...].reshape(all_rows, width)
            product = (dot(x, v_in[:, cols]) * dot(x, v_val[:, cols])).astype(BF16)
            ext[pl.ds(8, all_rows), cols] = product.astype(F32)
            rim_out[:, cols] = product[all_rows - 16 :]
            gates[:, cols] = dot(x, v_out[:, cols])
            return carry

        lax.fori_loop(0, chan // tile, one, 0)
        once(RIM, rim_out, rim_in, after).start()

    def mixer_conv():
        came_once(RIM, rim_in)
        edge = rim_in[...].astype(F32)[8:16]
        ext[0:8, :] = jnp.where(e == 0, jnp.zeros_like(edge), edge)
        tap_count = taps.shape[0]
        total = taps[0:1, :] * ext[pl.ds(8 - (tap_count - 1), all_rows), :]
        for n in range(1, tap_count):
            total += taps[n : n + 1, :] * ext[pl.ds(8 - (tap_count - 1) + n, all_rows), :]
        gated[t] = (gates[...] * total).astype(BF16)
        once(Q2, gated.at[t], gated.at[t], across).start()
        once(Q1, gated.at[t], gated.at[t], near).start()

    def mixer_project():
        came_once(Q1, gated.at[t1])
        came_once(QG, gated.at[t3])

        def one(n, carry):
            cols = pl.ds(pl.multiple_of(n * tile, tile), tile)
            total = dot(gated[0], v_proj[0:chan, cols])
            for other in range(1, group):
                total += dot(gated[other], v_proj[other * chan : (other + 1) * chan, cols])
            mixer_out[:, cols] = total.astype(BF16)
            return carry

        lax.fori_loop(0, chan // tile, one, 0)

    stages = (take, hand_rows, expand, hand_hidden, finish)

    def step(i, carry):
        for stage, lag in reversed(list(zip(stages, LAGS))):
            @pl.when((i >= lag) & (i < count + lag))
            def _(stage=stage, lag=lag):
                stage(i - lag)

        @pl.when(i == MIX_AT[0])
        def _():
            once(M2, normed, rows.at[t], across).start()
            for load in loads:
                load.wait()

        @pl.when(i == MIX_AT[1])
        def _():
            came_once(M2, rows.at[t2])
            once(MG, rows.at[t2], rows.at[t2], near).start()

        @pl.when(i == MIX_AT[2])
        def _():
            mixer_products()

        @pl.when(i == MIX_AT[3])
        def _():
            mixer_conv()

        @pl.when(i == MIX_AT[4])
        def _():
            came_once(Q2, gated.at[t2])
            once(QG, gated.at[t2], gated.at[t2], near).start()

        @pl.when(i == MIX_AT[5])
        def _():
            mixer_project()

        return carry

    lax.fori_loop(0, count + LAGS[-1], step, 0)

    def landed(i, carry):
        @pl.when(shift_of(i) != 0)
        def _():
            came(RET, i, returned.at[source_of(i)])

        return carry

    lax.fori_loop(0, count, landed, 0)
    for block in range(group):
        part = pl.ds(block * tok_dev, tok_dev)
        mix = combine[part, :]
        high = mix.astype(BF16)
        low = (mix - high.astype(F32)).astype(BF16)
        values = returned[:, block].reshape(count * slot_cap, chan)
        expert_out[part, :] = (dot(high, values) + dot(low, values)).astype(BF16)

    def drain(i, carry):
        src = source_of(i)
        chunk(F1, i, arrived.at[src, t], arrived.at[src, t], near).wait_send()

        @pl.when(shift_of(i) >= half)
        def _():
            chunk(F2, i, arrived.at[src, t], arrived.at[src, t], near).wait_send()

        @pl.when(shift_of(i) != 0)
        def _():
            disp(i).wait_send()
            ret(i).wait_send()

        @pl.when((shift_of(i) != 0) & (shift_of(i) < half))
        def _():
            disp2(i).wait_send()

        chunk(G1, i, arrived.at[src, t2], arrived.at[src, t2], near).wait_send()
        for kind in (H2, H1):
            chunk(kind, i, hid.at[src, t], hid.at[src, t], near).wait_send()
        chunk(HG, i, hid.at[src, t2], hid.at[src, t2], near).wait_send()
        return carry

    lax.fori_loop(0, count, drain, 0)
    for kind in (M2, M1):
        once(kind, normed, rows.at[t], near).wait_send()
    once(MG, rows.at[t2], rows.at[t2], near).wait_send()
    once(DX, own_rows, dense, near).wait_send()
    for kind in (Q2, Q1):
        once(kind, gated.at[t], gated.at[t], near).wait_send()
    once(QG, gated.at[t2], gated.at[t2], near).wait_send()
    once(RIM, rim_out, rim_in, after).wait_send()


def write_kernel(mixer_sum, expert_sum, mixer_out, expert_out, held, sem):
    pairs = [(mixer_sum, mixer_out), (expert_sum, expert_out)]
    inward = [pltpu.make_async_copy(a, held.at[n], sem.at[n]) for n, (a, _) in enumerate(pairs)]
    outward = [pltpu.make_async_copy(held.at[n], b, sem.at[2 + n]) for n, (_, b) in enumerate(pairs)]
    for copy in inward:
        copy.start()
    for first, second in zip(inward, outward):
        first.wait()
        second.start()
    for copy in outward:
        copy.wait()


def fused_on_device(
    mixer_in, expert_in, mixer_gain, in_gate_weight, out_gate_weight, value_weight, conv_taps,
    mixer_proj, expert_gain, route_ids, route_weights, gate_weight, up_weight, down_weight,
):
    tok_dev, width = mixer_in.shape
    group = lax.axis_size("tp")
    count = lax.axis_size("ep")
    experts = count * gate_weight.shape[0]
    slot_cap = 2 * tok_dev * route_ids.shape[1] // experts
    chan = in_gate_weight.shape[1]
    hid_width = gate_weight.shape[2]
    all_rows = group * tok_dev
    vm = pl.BlockSpec(memory_space=pltpu.VMEM)
    anywhere = pl.BlockSpec(memory_space=pl.ANY)
    shape = jax.ShapeDtypeStruct
    weights = (
        in_gate_weight, out_gate_weight, value_weight, mixer_proj, gate_weight, up_weight, down_weight,
    )
    dma = pltpu.SemaphoreType.DMA
    results = pl.pallas_call(
        exchange_kernel,
        out_shape=(shape((all_rows, chan), BF16), shape((all_rows, chan), BF16)),
        in_specs=[pl.BlockSpec(memory_space=pltpu.HBM)] * 14,
        out_specs=(vm, vm),
        scratch_shapes=[
            pltpu.VMEM(w.shape[-2:], BF16)
            for w in (in_gate_weight, out_gate_weight, value_weight, mixer_proj,
                      gate_weight, up_weight, down_weight)
        ] + [
            pltpu.VMEM((tok_dev, width), BF16),
            pltpu.VMEM((tok_dev, width), BF16),
            pltpu.VMEM((1, width), F32),
            pltpu.VMEM((1, width), F32),
            pltpu.VMEM(route_ids.shape[::-1], jnp.int32),
            pltpu.VMEM(route_ids.shape[::-1], F32),
            pltpu.VMEM((conv_taps.shape[0], chan), F32),
            pltpu.VMEM((tok_dev, width), BF16),
            pltpu.VMEM((tok_dev, width), BF16),
            pltpu.VMEM((experts, slot_cap, width), BF16),
            pltpu.VMEM((experts, slot_cap, tok_dev), BF16),
            pltpu.VMEM((all_rows, experts * slot_cap), F32),
            pltpu.VMEM((group, tok_dev, width), BF16),
            pltpu.VMEM((count, group, slot_cap, width), BF16),
            pltpu.VMEM((count, group, group * slot_cap, hid_width), BF16),
            pltpu.VMEM((count, group, slot_cap, chan), BF16),
            pltpu.VMEM((count, group, slot_cap, chan), BF16),
            pltpu.VMEM((all_rows, chan), F32),
            pltpu.VMEM((all_rows + 8, chan), F32),
            pltpu.VMEM((16, chan), BF16),
            pltpu.VMEM((16, chan), BF16),
            pltpu.VMEM((group, all_rows, chan), BF16),
            pltpu.VMEM((tok_dev, width), BF16),
            pltpu.VMEM((count // 2, slot_cap, width), BF16),
            dma((9, count)), dma((9, count)), dma((8,)), dma((8,)), dma((7,)), dma((7,)),
        ],
        compiler_params=pltpu.CompilerParams(
            collective_id=0, has_side_effects=True, vmem_limit_bytes=VMEM_BYTES
        ),
        name="exchange",
    )(
        mixer_in, expert_in, mixer_gain[None, :], expert_gain[None, :],
        route_ids.T, route_weights.T, conv_taps, *weights,
    )
    return pl.pallas_call(
        write_kernel,
        out_shape=(shape((all_rows, chan), BF16), shape((all_rows, chan), BF16)),
        in_specs=[anywhere, anywhere],
        out_specs=(anywhere, anywhere),
        scratch_shapes=[pltpu.VMEM((2, all_rows, chan), BF16), dma((4,))],
        compiler_params=pltpu.CompilerParams(vmem_limit_bytes=VMEM_BYTES),
        name="write",
    )(*results)


def body_for(mesh):
    count, group = mesh.shape["ep"], mesh.shape["tp"]

    def body(*args):
        tok_dev, picks, held = args[0].shape[0], args[9].shape[1], args[11].shape[0]
        slot_cap = 2 * tok_dev * picks // (count * held)
        fits = count in (4, 8, 16) and group == 4 and held == 1 and slot_cap % 16 == 0
        return (fused_on_device if fits and tok_dev % 16 == 0 else on_device)(*args)

    return body


def solution(mesh):
    return jax.shard_map(
        body_for(mesh),
        mesh=mesh,
        in_specs=(
            P(("ep", "tp"), None),
            P(("ep", "tp"), None),
            P(),
            P(None, "tp"),
            P(None, "tp"),
            P(None, "tp"),
            P(),
            P(None, "tp"),
            P(),
            P("ep", None),
            P("ep", None),
            P("ep", None, "tp"),
            P("ep", None, "tp"),
            P("ep", None, "tp"),
        ),
        out_specs=(P("ep", "tp"), P("ep", "tp")),
        check_vma=False,
    )
```

```python
import functools

import jax
import jax.numpy as jnp
from jax import lax
from jax.experimental import pallas as pl
from jax.experimental.pallas import tpu as pltpu
from jax.sharding import PartitionSpec as P

norm_eps = 1e-06


def passed_along(value, axis, steps):
    count = lax.axis_size(axis)
    leading, last = (max(0, -steps), min(count, count - steps))
    return lax.ppermute(value, axis, [(source, source + steps) for source in range(leading, last)])


def rms_rows(values, gain_row):
    wide = values.astype(jnp.float32)
    scale = lax.rsqrt(jnp.mean(wide * wide, axis=-1, keepdims=True) + norm_eps)
    return (wide * scale * gain_row).astype(jnp.bfloat16)


def place_slots(route_ids, group_rows, experts, slot_cap):
    row_total, top_count = route_ids.shape
    groups = row_total // group_rows
    labels = jnp.arange(experts, dtype=jnp.int32)
    onehot = (
        route_ids.reshape(groups, group_rows * top_count)[:, :, None] == labels[None, None, :]
    ).astype(jnp.int32)
    earlier = jnp.cumsum(onehot, axis=1) - onehot
    within = jnp.sum(earlier * onehot, axis=2)
    slot_index = jnp.arange(groups, dtype=jnp.int32)[:, None] * slot_cap + within
    return slot_index.reshape(row_total, top_count)


def on_device(
    mixer_in,
    expert_in,
    mixer_gain,
    in_gate_weight,
    out_gate_weight,
    value_weight,
    conv_taps,
    mixer_proj,
    expert_gain,
    route_ids,
    route_weights,
    gate_weight,
    up_weight,
    down_weight,
):
    tok_dev = mixer_in.shape[0]
    tp_count = lax.axis_size("tp")
    ep_count = lax.axis_size("ep")
    top_count = route_ids.shape[1]
    experts = ep_count * gate_weight.shape[0]
    slot_cap = max(2, 2 * tok_dev * top_count // experts)
    tp_index = lax.axis_index("tp")
    mixer_normed = rms_rows(mixer_in, mixer_gain)
    expert_normed = rms_rows(expert_in, expert_gain)
    block_slot = place_slots(route_ids, tok_dev, experts, slot_cap)
    mixer_rows = lax.all_gather(mixer_normed, "tp", axis=0, tiled=True)
    send_ids = lax.dynamic_slice_in_dim(route_ids, tp_index * tok_dev, tok_dev, 0)
    send_slot = (
        lax.dynamic_slice_in_dim(block_slot, tp_index * tok_dev, tok_dev, 0) - tp_index * slot_cap
    )
    source_count = expert_normed.shape[0]
    flat_index = (send_ids * slot_cap + send_slot).reshape(-1)
    row_table = (
        jnp.full((experts * slot_cap,), source_count, jnp.int32)
        .at[flat_index]
        .set(jnp.repeat(jnp.arange(source_count, dtype=jnp.int32), top_count))
    )
    padded_rows = jnp.concatenate(
        [expert_normed, jnp.zeros((1, expert_normed.shape[1]), jnp.bfloat16)], axis=0
    )
    outgoing = padded_rows[row_table].reshape(experts, slot_cap, expert_normed.shape[1])
    arrived = lax.all_to_all(outgoing, "ep", split_axis=0, concat_axis=0, tiled=True)
    arrived = lax.all_gather(arrived, "tp", axis=1, tiled=True)
    chan_width = in_gate_weight.shape[1]
    in_gate = jnp.dot(mixer_rows, in_gate_weight, preferred_element_type=jnp.float32)
    out_gate = jnp.dot(mixer_rows, out_gate_weight, preferred_element_type=jnp.float32)
    values = jnp.dot(mixer_rows, value_weight, preferred_element_type=jnp.float32)
    product = (in_gate * values).astype(jnp.bfloat16)
    tap_count = conv_taps.shape[0]
    rim_rows = passed_along(product[product.shape[0] - (tap_count - 1) :], "ep", 1)
    extended = jnp.concatenate([rim_rows, product], axis=0).astype(jnp.float32)
    tap_rows = lax.dynamic_slice_in_dim(conv_taps, tp_index * chan_width, chan_width, 1)
    row_count = product.shape[0]
    conv_sum = tap_rows[0] * extended[0:row_count]
    for tap_index in range(1, tap_count):
        conv_sum = conv_sum + tap_rows[tap_index] * extended[tap_index : tap_index + row_count]
    gated = (out_gate * conv_sum).astype(jnp.bfloat16)
    slots_in = arrived.reshape(-1, arrived.shape[2])
    gate_pre = jnp.dot(slots_in, gate_weight[0], preferred_element_type=jnp.float32)
    up_pre = jnp.dot(slots_in, up_weight[0], preferred_element_type=jnp.float32)
    hidden = (jax.nn.silu(gate_pre) * up_pre).astype(jnp.bfloat16)
    down_slice = down_weight[0]
    gated_all, hidden_all = (
        lax.all_gather(gated, "tp", axis=1, tiled=True),
        lax.all_gather(hidden, "tp", axis=1, tiled=True),
    )
    mixer_sum = jnp.dot(gated_all, mixer_proj, preferred_element_type=jnp.float32)
    expert_sum = jnp.dot(hidden_all, down_slice, preferred_element_type=jnp.float32)
    mixer_out = mixer_sum.astype(jnp.bfloat16)
    results = expert_sum.astype(jnp.bfloat16).reshape(ep_count, -1, expert_sum.shape[1])
    returned = lax.all_to_all(results, "ep", split_axis=0, concat_axis=0, tiled=True)
    back_index = (route_ids * (tp_count * slot_cap) + block_slot).reshape(-1)
    picked = returned.reshape(-1, returned.shape[2])[back_index].reshape(
        route_ids.shape[0], top_count, -1
    )
    shares = route_weights / jnp.sum(route_weights, axis=1, keepdims=True)
    expert_out = jnp.sum(picked.astype(jnp.float32) * shares[:, :, None], axis=1).astype(
        jnp.bfloat16
    )
    return (mixer_out, expert_out)


MESH = pl.DeviceIdType.MESH
F32 = jnp.float32
BF16 = jnp.bfloat16
VMEM_BYTES = 60 * 1024 * 1024


def dot(a, b):
    return jnp.dot(a, b, preferred_element_type=F32)


def prepare(slot_cap, me, tok_dev, ids, weights, own_table, partner_table, combine):
    picks, all_rows = ids.shape
    blocks = all_rows // tok_dev
    slots = combine.shape[1]
    experts = slots // slot_cap
    partner = (me + 2) % blocks
    filler = jnp.zeros((8 - 2 * picks, all_rows), F32)
    columns = jnp.transpose(jnp.concatenate([ids[...].astype(F32), weights[...], filler], axis=0))
    below = (
        lax.broadcasted_iota(jnp.int32, (tok_dev, tok_dev), 1)
        < lax.broadcasted_iota(jnp.int32, (tok_dev, tok_dev), 0)
    ).astype(BF16)
    labels = lax.broadcasted_iota(jnp.int32, (tok_dev, 128), 1)
    places = lax.broadcasted_iota(jnp.int32, (tok_dev, slots), 1)
    chosen = jnp.zeros((tok_dev, slots), F32)
    theirs = jnp.zeros((tok_dev, slots), F32)
    for block in range(blocks):
        part = slice(block * tok_dev, (block + 1) * tok_dev)
        named = [columns[part, k : k + 1].astype(jnp.int32) for k in range(picks)]
        share = [columns[part, picks + k : picks + k + 1] for k in range(picks)]
        total = functools.reduce(jnp.add, share)
        hot = [(labels == n).astype(F32) for n in named]
        rank = dot(below, functools.reduce(jnp.add, hot).astype(BF16))
        mixed = jnp.zeros((tok_dev, slots), F32)
        sent = jnp.zeros((tok_dev, slots), F32)
        for k in range(picks):
            within = jnp.sum(rank * hot[k], axis=1, keepdims=True).astype(jnp.int32)
            spot = places == named[k] * slot_cap + within
            mixed = mixed + jnp.where(spot, share[k] / total, 0.0)
            sent = sent + jnp.where(spot, 1.0, 0.0)
        combine[part, :] = mixed
        chosen = jnp.where(me == block, sent, chosen)
        theirs = jnp.where(partner == block, sent, theirs)
    own_table[...] = jnp.transpose(chosen).astype(BF16).reshape(experts, slot_cap, tok_dev)
    partner_table[...] = jnp.transpose(theirs).astype(BF16).reshape(experts, slot_cap, tok_dev)


(
    SEL, DXW, D2, MIXP, M2S, MIXG, LOADW, MIXPROD, CONV, Q2S, CONVG, PROJ, TAKE, ROWS, EXP, HH, FIN,
) = range(17)

STEPS = (
    (SEL, 4), (MIXP, 0), (SEL, 3), (SEL, 2), (M2S, 0), (SEL, 6), (SEL, 0), (DXW, 0),
    (D2, 1), (TAKE, 3), (SEL, 5), (TAKE, 4), (D2, 3), (TAKE, 6), (TAKE, 0), (SEL, 7),
    (SEL, 1), (ROWS, 4), (LOADW, 0), (EXP, 4), (MIXG, 0), (ROWS, 6), (TAKE, 5), (EXP, 6),
    (D2, 2), (MIXPROD, 0), (HH, 4), (D2, 0), (TAKE, 7), (ROWS, 1), (ROWS, 5), (FIN, 4),
    (ROWS, 0), (CONV, 0), (HH, 6), (EXP, 5), (ROWS, 7), (EXP, 0), (TAKE, 1), (ROWS, 3),
    (EXP, 7), (FIN, 6), (EXP, 3), (ROWS, 2), (TAKE, 2), (HH, 0), (HH, 5), (EXP, 1),
    (FIN, 0), (HH, 3), (Q2S, 0), (FIN, 5), (FIN, 3), (EXP, 2), (HH, 7), (HH, 1),
    (FIN, 7), (FIN, 1), (HH, 2), (FIN, 2), (CONVG, 0), (PROJ, 0),
)


DISP, F2, F1, G1, H2, H1, HG, RET, DISP2 = range(9)
M2, M1, MG, Q2, Q1, QG, RIM, DX = range(8)


def looked_up(values, i):
    bit = 1
    while len(values) > 1:
        odd = (i // bit) % 2 == 1
        values = [
            jnp.where(odd, pair[-1], pair[0]) if pair[0] is not pair[-1] else pair[0]
            for pair in (values[n : n + 2] for n in range(0, len(values), 2))
        ]
        bit *= 2
    return values[0]


def choose(stage, low, high, bodies):
    if high - low == 1:
        bodies[low]()
        return
    middle = (low + high) // 2
    for below in (True, False):
        @pl.when((stage < middle) if below else (stage >= middle))
        def _(below=below):
            choose(stage, *((low, middle) if below else (middle, high)), bodies)


def exchange_kernel(
    mixer_in, expert_in, mixer_gain, expert_gain, ids, shares, all_taps,
    w_in, w_out, w_val, w_proj, w_gate, w_up, w_down,
    mixer_out, expert_out,
    v_in, v_out, v_val, v_proj, v_gate, v_up, v_down,
    v_mixer, v_expert, v_mixer_gain, v_expert_gain, v_ids, v_shares, taps,
    normed, own_rows, own_table, outgoing, partner_table, combine,
    rows, arrived, hid, res, returned, gates, ext, rim_out, rim_in, gated, dense, outgoing2,
    send, recv, send1, recv1, wsem, fsem,
):
    count = outgoing.shape[0]
    group, tok_dev, width = rows.shape
    half = count // 2
    chan = v_in.shape[1]
    slot_cap = outgoing.shape[1]
    hid_width = v_gate.shape[1]
    e = lax.axis_index("ep")
    t = lax.axis_index("tp")
    t1 = t + 1 - 2 * (t % 2)
    t2 = (t + 2) % group
    t3 = (t1 + 2) % group

    firsts = [
        pltpu.make_async_copy(a, b, fsem.at[n])
        for n, (a, b) in enumerate(
            [(expert_in, v_expert), (expert_gain, v_expert_gain), (ids, v_ids), (shares, v_shares),
             (mixer_in, v_mixer), (mixer_gain, v_mixer_gain),
             (all_taps.at[:, pl.ds(pl.multiple_of(t * chan, 128), chan)], taps)]
        )
    ]
    for load in firsts:
        load.start()
    loads = [
        pltpu.make_async_copy(a, b, wsem.at[n])
        for n, (a, b) in enumerate(
            [(w_in, v_in), (w_val, v_val), (w_out, v_out), (w_gate.at[0], v_gate),
             (w_up.at[0], v_up), (w_down.at[0], v_down), (w_proj, v_proj)]
        )
    ]
    def mixed_with(s):
        value, bit = 0, 1
        while bit < count:
            value = value + ((e // bit + s // bit) % 2) * bit
            bit *= 2
        return value

    barrier = pltpu.get_barrier_semaphore()
    for s in range(1, count):
        pl.semaphore_signal(barrier, inc=1, device_id=(mixed_with(s), t), device_id_type=MESH)
    for peer in (t1, t2):
        pl.semaphore_signal(barrier, inc=1, device_id=(e, peer), device_id_type=MESH)
    for load in firsts[:4]:
        load.wait()
    for load in loads:
        load.start()
    own_rows[...] = rms_rows(v_expert[...], v_expert_gain[...])
    pl.semaphore_wait(barrier, count + 1)

    def chunk(kind, i, src, dst, dev):
        return pltpu.make_async_remote_copy(
            src_ref=src, dst_ref=dst, send_sem=send.at[kind, i], recv_sem=recv.at[kind, i],
            device_id=dev, device_id_type=MESH,
        )

    def once(kind, src, dst, dev):
        return pltpu.make_async_remote_copy(
            src_ref=src, dst_ref=dst, send_sem=send1.at[kind], recv_sem=recv1.at[kind],
            device_id=dev, device_id_type=MESH,
        )

    near, across = (e, t1), (e, t2)
    after = ((e + 1) % count, t)

    def came(kind, i, dst):
        chunk(kind, i, dst, dst, near).wait_recv()

    def came_once(kind, dst):
        once(kind, dst, dst, near).wait_recv()

    def disp(i):
        return chunk(DISP, i, outgoing.at[i], arrived.at[e, t], (mixed_with(i), t))

    def disp2(i):
        return chunk(DISP2, i, outgoing2.at[i], arrived.at[e, t2], (mixed_with(i), t))

    def ret(i):
        return chunk(RET, i, res.at[i], returned.at[e], (mixed_with(i), t))

    once(DX, own_rows, dense, across).start()
    prepare(slot_cap, t, tok_dev, v_ids, v_shares, own_table, partner_table, combine)

    def sel(i):
        picked = dot(own_table[mixed_with(i)], own_rows[...]).astype(BF16)

        @pl.when(i == 0)
        def _():
            arrived[e, t] = picked

        @pl.when(i != 0)
        def _():
            outgoing[i] = picked
            disp(i).start()

    def dxw(i):
        came_once(DX, dense)

    def d2(i):
        picked = dot(partner_table[mixed_with(i)], dense[...]).astype(BF16)

        @pl.when(i == 0)
        def _():
            arrived[e, t2] = picked

        @pl.when(i != 0)
        def _():
            outgoing2[i] = picked
            disp2(i).start()

    def mixp(i):
        for load in firsts[4:]:
            load.wait()
        normed[...] = rms_rows(v_mixer[...], v_mixer_gain[...])
        rows[t] = normed[...]
        once(M1, normed, rows.at[t], near).start()

    def m2(i):
        once(M2, normed, rows.at[t], across).start()

    def mixg(i):
        came_once(M2, rows.at[t2])
        once(MG, rows.at[t2], rows.at[t2], near).start()

    def loadw(i):
        for load in loads:
            load.wait()

    def take(i):
        src = mixed_with(i)

        @pl.when(i != 0)
        def _():
            came(DISP, i, arrived.at[src, t])

        @pl.when(i >= half)
        def _():
            chunk(F2, i, arrived.at[src, t], arrived.at[src, t], across).start()

        chunk(F1, i, arrived.at[src, t], arrived.at[src, t], near).start()

    def hand_rows(i):
        src = mixed_with(i)

        @pl.when(i >= half)
        def _():
            came(F2, i, arrived.at[src, t2])

        @pl.when((i < half) & (i != 0))
        def _():
            came(DISP2, i, arrived.at[src, t2])

        chunk(G1, i, arrived.at[src, t2], arrived.at[src, t2], near).start()

    def expand(i):
        src = mixed_with(i)
        came(F1, i, arrived.at[src, t1])
        came(G1, i, arrived.at[src, t3])
        x = arrived[src].reshape(group * slot_cap, width)
        gate = dot(x, v_gate[...])
        up = dot(x, v_up[...])
        hid[src, t] = (gate / (1.0 + jnp.exp(-gate)) * up).astype(BF16)
        chunk(H2, i, hid.at[src, t], hid.at[src, t], across).start()
        chunk(H1, i, hid.at[src, t], hid.at[src, t], near).start()

    def hand_hidden(i):
        src = mixed_with(i)
        came(H2, i, hid.at[src, t2])
        chunk(HG, i, hid.at[src, t2], hid.at[src, t2], near).start()

    def finish(i):
        src = mixed_with(i)
        came(H1, i, hid.at[src, t1])
        came(HG, i, hid.at[src, t3])
        total = dot(hid[src, 0], v_down[0:hid_width, :])
        for other in range(1, group):
            total += dot(hid[src, other], v_down[other * hid_width : (other + 1) * hid_width, :])
        total = total.astype(BF16).reshape(group, slot_cap, chan)

        @pl.when(i != 0)
        def _():
            res[i] = total
            ret(i).start()

        @pl.when(i == 0)
        def _():
            returned[src] = total

    all_rows = group * tok_dev
    tile = 256

    def mixer_products(i):
        came_once(M1, rows.at[t1])
        came_once(MG, rows.at[t3])

        def one(n, carry):
            cols = pl.ds(pl.multiple_of(n * tile, tile), tile)
            x = rows[...].reshape(all_rows, width)
            product = (dot(x, v_in[:, cols]) * dot(x, v_val[:, cols])).astype(BF16)
            ext[pl.ds(8, all_rows), cols] = product.astype(F32)
            rim_out[:, cols] = product[all_rows - 16 :]
            gates[:, cols] = dot(x, v_out[:, cols])
            return carry

        lax.fori_loop(0, chan // tile, one, 0)
        once(RIM, rim_out, rim_in, after).start()

    def mixer_conv(i):
        came_once(RIM, rim_in)
        edge = rim_in[...].astype(F32)[8:16]
        ext[0:8, :] = jnp.where(e == 0, jnp.zeros_like(edge), edge)
        tap_count = taps.shape[0]
        total = taps[0:1, :] * ext[pl.ds(8 - (tap_count - 1), all_rows), :]
        for n in range(1, tap_count):
            total += taps[n : n + 1, :] * ext[pl.ds(8 - (tap_count - 1) + n, all_rows), :]
        gated[t] = (gates[...] * total).astype(BF16)
        once(Q1, gated.at[t], gated.at[t], near).start()

    def q2(i):
        once(Q2, gated.at[t], gated.at[t], across).start()

    def convg(i):
        came_once(Q2, gated.at[t2])
        once(QG, gated.at[t2], gated.at[t2], near).start()

    def mixer_project(i):
        came_once(Q1, gated.at[t1])
        came_once(QG, gated.at[t3])

        def one(n, carry):
            cols = pl.ds(pl.multiple_of(n * tile, tile), tile)
            total = dot(gated[0], v_proj[0:chan, cols])
            for other in range(1, group):
                total += dot(gated[other], v_proj[other * chan : (other + 1) * chan, cols])
            mixer_out[:, cols] = total.astype(BF16)
            return carry

        lax.fori_loop(0, chan // tile, one, 0)

    bodies = (
        sel, dxw, d2, mixp, m2, mixg, loadw, mixer_products, mixer_conv, q2, convg, mixer_project,
        take, hand_rows, expand, hand_hidden, finish,
    )
    stage_list, shift_list = zip(*STEPS)

    def step(n, carry):
        stage, shift = looked_up(stage_list, n), looked_up(shift_list, n)
        choose(stage, 0, len(bodies), [functools.partial(body, shift) for body in bodies])
        return carry

    lax.fori_loop(0, len(stage_list), step, 0)

    def landed(i, carry):
        came(RET, i, returned.at[mixed_with(i)])
        return carry

    lax.fori_loop(1, count, landed, 0)
    for block in range(group):
        part = pl.ds(block * tok_dev, tok_dev)
        mix = combine[part, :]
        high = mix.astype(BF16)
        low = (mix - high.astype(F32)).astype(BF16)
        values = returned[:, block].reshape(count * slot_cap, chan)
        expert_out[part, :] = (dot(high, values) + dot(low, values)).astype(BF16)

    def drain(i, carry):
        src = mixed_with(i)
        chunk(F1, i, arrived.at[src, t], arrived.at[src, t], near).wait_send()

        @pl.when(i >= half)
        def _():
            chunk(F2, i, arrived.at[src, t], arrived.at[src, t], near).wait_send()

        @pl.when(i != 0)
        def _():
            disp(i).wait_send()
            ret(i).wait_send()

        @pl.when((i != 0) & (i < half))
        def _():
            disp2(i).wait_send()

        chunk(G1, i, arrived.at[src, t2], arrived.at[src, t2], near).wait_send()
        for kind in (H2, H1):
            chunk(kind, i, hid.at[src, t], hid.at[src, t], near).wait_send()
        chunk(HG, i, hid.at[src, t2], hid.at[src, t2], near).wait_send()
        return carry

    lax.fori_loop(0, count, drain, 0)
    for kind in (M2, M1):
        once(kind, normed, rows.at[t], near).wait_send()
    once(MG, rows.at[t2], rows.at[t2], near).wait_send()
    once(DX, own_rows, dense, near).wait_send()
    for kind in (Q2, Q1):
        once(kind, gated.at[t], gated.at[t], near).wait_send()
    once(QG, gated.at[t2], gated.at[t2], near).wait_send()
    once(RIM, rim_out, rim_in, after).wait_send()


def write_kernel(mixer_sum, expert_sum, mixer_out, expert_out, held, sem):
    pairs = [(mixer_sum, mixer_out), (expert_sum, expert_out)]
    inward = [pltpu.make_async_copy(a, held.at[n], sem.at[n]) for n, (a, _) in enumerate(pairs)]
    outward = [pltpu.make_async_copy(held.at[n], b, sem.at[2 + n]) for n, (_, b) in enumerate(pairs)]
    for copy in inward:
        copy.start()
    for first, second in zip(inward, outward):
        first.wait()
        second.start()
    for copy in outward:
        copy.wait()


def fused_on_device(
    mixer_in, expert_in, mixer_gain, in_gate_weight, out_gate_weight, value_weight, conv_taps,
    mixer_proj, expert_gain, route_ids, route_weights, gate_weight, up_weight, down_weight,
):
    tok_dev, width = mixer_in.shape
    group = lax.axis_size("tp")
    count = lax.axis_size("ep")
    experts = count * gate_weight.shape[0]
    slot_cap = 2 * tok_dev * route_ids.shape[1] // experts
    chan = in_gate_weight.shape[1]
    hid_width = gate_weight.shape[2]
    all_rows = group * tok_dev
    vm = pl.BlockSpec(memory_space=pltpu.VMEM)
    anywhere = pl.BlockSpec(memory_space=pl.ANY)
    shape = jax.ShapeDtypeStruct
    weights = (
        in_gate_weight, out_gate_weight, value_weight, mixer_proj, gate_weight, up_weight, down_weight,
    )
    dma = pltpu.SemaphoreType.DMA
    results = pl.pallas_call(
        exchange_kernel,
        out_shape=(shape((all_rows, chan), BF16), shape((all_rows, chan), BF16)),
        in_specs=[pl.BlockSpec(memory_space=pltpu.HBM)] * 14,
        out_specs=(vm, vm),
        scratch_shapes=[
            pltpu.VMEM(w.shape[-2:], BF16)
            for w in (in_gate_weight, out_gate_weight, value_weight, mixer_proj,
                      gate_weight, up_weight, down_weight)
        ] + [
            pltpu.VMEM((tok_dev, width), BF16),
            pltpu.VMEM((tok_dev, width), BF16),
            pltpu.VMEM((1, width), F32),
            pltpu.VMEM((1, width), F32),
            pltpu.VMEM(route_ids.shape[::-1], jnp.int32),
            pltpu.VMEM(route_ids.shape[::-1], F32),
            pltpu.VMEM((conv_taps.shape[0], chan), F32),
            pltpu.VMEM((tok_dev, width), BF16),
            pltpu.VMEM((tok_dev, width), BF16),
            pltpu.VMEM((experts, slot_cap, tok_dev), BF16),
            pltpu.VMEM((experts, slot_cap, width), BF16),
            pltpu.VMEM((experts, slot_cap, tok_dev), BF16),
            pltpu.VMEM((all_rows, experts * slot_cap), F32),
            pltpu.VMEM((group, tok_dev, width), BF16),
            pltpu.VMEM((count, group, slot_cap, width), BF16),
            pltpu.VMEM((count, group, group * slot_cap, hid_width), BF16),
            pltpu.VMEM((count, group, slot_cap, chan), BF16),
            pltpu.VMEM((count, group, slot_cap, chan), BF16),
            pltpu.VMEM((all_rows, chan), F32),
            pltpu.VMEM((all_rows + 8, chan), F32),
            pltpu.VMEM((16, chan), BF16),
            pltpu.VMEM((16, chan), BF16),
            pltpu.VMEM((group, all_rows, chan), BF16),
            pltpu.VMEM((tok_dev, width), BF16),
            pltpu.VMEM((count // 2, slot_cap, width), BF16),
            dma((9, count)), dma((9, count)), dma((8,)), dma((8,)), dma((7,)), dma((7,)),
        ],
        compiler_params=pltpu.CompilerParams(
            collective_id=0, has_side_effects=True, vmem_limit_bytes=VMEM_BYTES
        ),
        name="exchange",
    )(
        mixer_in, expert_in, mixer_gain[None, :], expert_gain[None, :],
        route_ids.T, route_weights.T, conv_taps, *weights,
    )
    return pl.pallas_call(
        write_kernel,
        out_shape=(shape((all_rows, chan), BF16), shape((all_rows, chan), BF16)),
        in_specs=[anywhere, anywhere],
        out_specs=(anywhere, anywhere),
        scratch_shapes=[pltpu.VMEM((2, all_rows, chan), BF16), dma((4,))],
        compiler_params=pltpu.CompilerParams(vmem_limit_bytes=VMEM_BYTES),
        name="write",
    )(*results)


def body_for(mesh):
    count, group = mesh.shape["ep"], mesh.shape["tp"]

    def body(*args):
        tok_dev, picks, held = args[0].shape[0], args[9].shape[1], args[11].shape[0]
        slot_cap = 2 * tok_dev * picks // (count * held)
        fits = count == 8 and group == 4 and held == 1 and slot_cap % 16 == 0
        return (fused_on_device if fits and tok_dev % 16 == 0 else on_device)(*args)

    return body


def solution(mesh):
    return jax.shard_map(
        body_for(mesh),
        mesh=mesh,
        in_specs=(
            P(("ep", "tp"), None),
            P(("ep", "tp"), None),
            P(),
            P(None, "tp"),
            P(None, "tp"),
            P(None, "tp"),
            P(),
            P(None, "tp"),
            P(),
            P("ep", None),
            P("ep", None),
            P("ep", None, "tp"),
            P("ep", None, "tp"),
            P("ep", None, "tp"),
        ),
        out_specs=(P("ep", "tp"), P("ep", "tp")),
        check_vma=False,
    )
```

```python
import functools

import jax
import jax.numpy as jnp
from jax import lax
from jax.experimental import pallas as pl
from jax.experimental.pallas import tpu as pltpu
from jax.sharding import PartitionSpec as P

norm_eps = 1e-06


def passed_along(value, axis, steps):
    count = lax.axis_size(axis)
    leading, last = (max(0, -steps), min(count, count - steps))
    return lax.ppermute(value, axis, [(source, source + steps) for source in range(leading, last)])


def rms_rows(values, gain_row):
    wide = values.astype(jnp.float32)
    scale = lax.rsqrt(jnp.mean(wide * wide, axis=-1, keepdims=True) + norm_eps)
    return (wide * scale * gain_row).astype(jnp.bfloat16)


def place_slots(route_ids, group_rows, experts, slot_cap):
    row_total, top_count = route_ids.shape
    groups = row_total // group_rows
    labels = jnp.arange(experts, dtype=jnp.int32)
    onehot = (
        route_ids.reshape(groups, group_rows * top_count)[:, :, None] == labels[None, None, :]
    ).astype(jnp.int32)
    earlier = jnp.cumsum(onehot, axis=1) - onehot
    within = jnp.sum(earlier * onehot, axis=2)
    slot_index = jnp.arange(groups, dtype=jnp.int32)[:, None] * slot_cap + within
    return slot_index.reshape(row_total, top_count)


def on_device(
    mixer_in,
    expert_in,
    mixer_gain,
    in_gate_weight,
    out_gate_weight,
    value_weight,
    conv_taps,
    mixer_proj,
    expert_gain,
    route_ids,
    route_weights,
    gate_weight,
    up_weight,
    down_weight,
):
    tok_dev = mixer_in.shape[0]
    tp_count = lax.axis_size("tp")
    ep_count = lax.axis_size("ep")
    top_count = route_ids.shape[1]
    experts = ep_count * gate_weight.shape[0]
    slot_cap = max(2, 2 * tok_dev * top_count // experts)
    tp_index = lax.axis_index("tp")
    mixer_normed = rms_rows(mixer_in, mixer_gain)
    expert_normed = rms_rows(expert_in, expert_gain)
    block_slot = place_slots(route_ids, tok_dev, experts, slot_cap)
    mixer_rows = lax.all_gather(mixer_normed, "tp", axis=0, tiled=True)
    send_ids = lax.dynamic_slice_in_dim(route_ids, tp_index * tok_dev, tok_dev, 0)
    send_slot = (
        lax.dynamic_slice_in_dim(block_slot, tp_index * tok_dev, tok_dev, 0) - tp_index * slot_cap
    )
    source_count = expert_normed.shape[0]
    flat_index = (send_ids * slot_cap + send_slot).reshape(-1)
    row_table = (
        jnp.full((experts * slot_cap,), source_count, jnp.int32)
        .at[flat_index]
        .set(jnp.repeat(jnp.arange(source_count, dtype=jnp.int32), top_count))
    )
    padded_rows = jnp.concatenate(
        [expert_normed, jnp.zeros((1, expert_normed.shape[1]), jnp.bfloat16)], axis=0
    )
    outgoing = padded_rows[row_table].reshape(experts, slot_cap, expert_normed.shape[1])
    arrived = lax.all_to_all(outgoing, "ep", split_axis=0, concat_axis=0, tiled=True)
    arrived = lax.all_gather(arrived, "tp", axis=1, tiled=True)
    chan_width = in_gate_weight.shape[1]
    in_gate = jnp.dot(mixer_rows, in_gate_weight, preferred_element_type=jnp.float32)
    out_gate = jnp.dot(mixer_rows, out_gate_weight, preferred_element_type=jnp.float32)
    values = jnp.dot(mixer_rows, value_weight, preferred_element_type=jnp.float32)
    product = (in_gate * values).astype(jnp.bfloat16)
    tap_count = conv_taps.shape[0]
    rim_rows = passed_along(product[product.shape[0] - (tap_count - 1) :], "ep", 1)
    extended = jnp.concatenate([rim_rows, product], axis=0).astype(jnp.float32)
    tap_rows = lax.dynamic_slice_in_dim(conv_taps, tp_index * chan_width, chan_width, 1)
    row_count = product.shape[0]
    conv_sum = tap_rows[0] * extended[0:row_count]
    for tap_index in range(1, tap_count):
        conv_sum = conv_sum + tap_rows[tap_index] * extended[tap_index : tap_index + row_count]
    gated = (out_gate * conv_sum).astype(jnp.bfloat16)
    slots_in = arrived.reshape(-1, arrived.shape[2])
    gate_pre = jnp.dot(slots_in, gate_weight[0], preferred_element_type=jnp.float32)
    up_pre = jnp.dot(slots_in, up_weight[0], preferred_element_type=jnp.float32)
    hidden = (jax.nn.silu(gate_pre) * up_pre).astype(jnp.bfloat16)
    down_slice = down_weight[0]
    gated_all, hidden_all = (
        lax.all_gather(gated, "tp", axis=1, tiled=True),
        lax.all_gather(hidden, "tp", axis=1, tiled=True),
    )
    mixer_sum = jnp.dot(gated_all, mixer_proj, preferred_element_type=jnp.float32)
    expert_sum = jnp.dot(hidden_all, down_slice, preferred_element_type=jnp.float32)
    mixer_out = mixer_sum.astype(jnp.bfloat16)
    results = expert_sum.astype(jnp.bfloat16).reshape(ep_count, -1, expert_sum.shape[1])
    returned = lax.all_to_all(results, "ep", split_axis=0, concat_axis=0, tiled=True)
    back_index = (route_ids * (tp_count * slot_cap) + block_slot).reshape(-1)
    picked = returned.reshape(-1, returned.shape[2])[back_index].reshape(
        route_ids.shape[0], top_count, -1
    )
    shares = route_weights / jnp.sum(route_weights, axis=1, keepdims=True)
    expert_out = jnp.sum(picked.astype(jnp.float32) * shares[:, :, None], axis=1).astype(
        jnp.bfloat16
    )
    return (mixer_out, expert_out)


MESH = pl.DeviceIdType.MESH
F32 = jnp.float32
BF16 = jnp.bfloat16
VMEM_BYTES = 60 * 1024 * 1024


def dot(a, b):
    return jnp.dot(a, b, preferred_element_type=F32)


def fill_columns(ids, weights, columns):
    picks, all_rows = ids.shape
    filler = jnp.zeros((8 - 2 * picks, all_rows), F32)
    columns[...] = jnp.transpose(jnp.concatenate([ids[...].astype(F32), weights[...], filler], axis=0))


def placed(columns, block, tok_dev, picks, slots, slot_cap, shared):
    own = columns[pl.ds(pl.multiple_of(block * tok_dev, tok_dev), tok_dev), :]
    below = (
        lax.broadcasted_iota(jnp.int32, (tok_dev, tok_dev), 1)
        < lax.broadcasted_iota(jnp.int32, (tok_dev, tok_dev), 0)
    ).astype(BF16)
    labels = lax.broadcasted_iota(jnp.int32, (tok_dev, 128), 1)
    places = lax.broadcasted_iota(jnp.int32, (tok_dev, slots), 1)
    named = [own[:, k : k + 1].astype(jnp.int32) for k in range(picks)]
    share = [own[:, picks + k : picks + k + 1] for k in range(picks)]
    total = functools.reduce(jnp.add, share)
    hot = [(labels == n).astype(F32) for n in named]
    rank = dot(below, functools.reduce(jnp.add, hot).astype(BF16))
    result = jnp.zeros((tok_dev, slots), F32)
    for k in range(picks):
        within = jnp.sum(rank * hot[k], axis=1, keepdims=True).astype(jnp.int32)
        spot = places == named[k] * slot_cap + within
        result = result + jnp.where(spot, share[k] / total if shared else 1.0, 0.0)
    return result


(
    SEL, DXW, D2, PTAB, COMB, MIXP, M2S, MIXG, LOADW, MIXPROD, CONV, Q2S, CONVG, PROJ,
    TAKE, ROWS, EXP, HH, FIN, REST,
) = range(20)

PIECES = 4

END_STEPS = (
    (SEL, 7), (MIXP, 0), (SEL, 2), (SEL, 5), (TAKE, 7), (PTAB, 0), (SEL, 0),
    (TAKE, 3), (M2S, 2), (M2S, 1), (SEL, 1), (TAKE, 0), (DXW, 0), (D2, 1),
    (M2S, 0), (M2S, 3), (D2, 2), (ROWS, 7), (SEL, 6), (COMB, 0), (LOADW, 0),
    (EXP, 7), (TAKE, 1), (SEL, 4), (SEL, 3), (TAKE, 2), (D2, 0), (TAKE, 4),
    (D2, 3), (MIXG, 0), (MIXPROD, 0), (HH, 7), (TAKE, 6), (FIN, 7), (TAKE, 5),
    (ROWS, 6), (CONV, 0), (ROWS, 3), (ROWS, 4), (ROWS, 1), (EXP, 6), (EXP, 4),
    (ROWS, 5), (ROWS, 0), (EXP, 5), (EXP, 3), (HH, 6), (ROWS, 2), (FIN, 6),
    (EXP, 1), (EXP, 2), (HH, 5), (FIN, 5), (Q2S, 2), (HH, 4), (HH, 1),
    (HH, 2), (Q2S, 3), (FIN, 4), (HH, 3), (FIN, 1), (Q2S, 1), (EXP, 0),
    (FIN, 2), (Q2S, 0), (HH, 0), (FIN, 3), (CONVG, 0), (FIN, 0), (PROJ, 0),
)

MIDDLE_STEPS = (
    (SEL, 7), (SEL, 3), (SEL, 2), (MIXP, 0), (M2S, 2), (SEL, 1), (M2S, 0),
    (M2S, 3), (SEL, 4), (PTAB, 0), (DXW, 0), (D2, 3), (M2S, 1), (TAKE, 7),
    (SEL, 0), (TAKE, 0), (D2, 0), (D2, 1), (TAKE, 2), (SEL, 5), (TAKE, 5),
    (ROWS, 2), (ROWS, 7), (MIXG, 0), (COMB, 0), (LOADW, 0), (EXP, 2), (SEL, 6),
    (EXP, 7), (ROWS, 5), (TAKE, 4), (MIXPROD, 0), (HH, 2), (ROWS, 1), (EXP, 5),
    (HH, 7), (D2, 2), (FIN, 7), (CONV, 0), (TAKE, 3), (TAKE, 1), (ROWS, 0),
    (Q2S, 1), (ROWS, 4), (FIN, 2), (HH, 5), (ROWS, 3), (TAKE, 6), (EXP, 4),
    (EXP, 3), (Q2S, 0), (FIN, 5), (EXP, 0), (EXP, 1), (Q2S, 2), (HH, 4),
    (HH, 3), (ROWS, 6), (FIN, 3), (FIN, 4), (HH, 1), (EXP, 6), (FIN, 1),
    (HH, 0), (FIN, 0), (Q2S, 3), (HH, 6), (FIN, 6), (CONVG, 0), (PROJ, 0),
)


DISP, F2, F1, G1, H2, H1, HG, RET, DISP2, M2, Q2 = range(11)
M1, MG, Q1, QG, RIM, DX = range(6)


def looked_up(values, i):
    bit = 1
    while len(values) > 1:
        odd = (i // bit) % 2 == 1
        values = [
            jnp.where(odd, pair[-1], pair[0]) if pair[0] is not pair[-1] else pair[0]
            for pair in (values[n : n + 2] for n in range(0, len(values), 2))
        ]
        bit *= 2
    return values[0]


def choose(stage, low, high, bodies):
    if high - low == 1:
        bodies[low]()
        return
    middle = (low + high) // 2
    for below in (True, False):
        @pl.when((stage < middle) if below else (stage >= middle))
        def _(below=below):
            choose(stage, *((low, middle) if below else (middle, high)), bodies)


def exchange_kernel(
    mixer_in, expert_in, mixer_gain, expert_gain, ids, shares, all_taps,
    w_in, w_out, w_val, w_proj, w_gate, w_up, w_down,
    mixer_out, expert_out,
    v_in, v_out, v_val, v_proj, v_gate, v_up, v_down,
    v_mixer, v_expert, v_mixer_gain, v_expert_gain, v_ids, v_shares, taps,
    columns, normed, own_rows, own_table, outgoing, partner_table, combine,
    rows, arrived, hid, res, returned, gates, ext, rim_out, rim_in, gated, dense, outgoing2,
    send, recv, send1, recv1, wsem, fsem,
):
    count = outgoing.shape[0]
    group, tok_dev, width = rows.shape
    half = count // 2
    all_rows = group * tok_dev
    chan = v_in.shape[1]
    slot_cap = outgoing.shape[1]
    hid_width = v_gate.shape[1]
    e = lax.axis_index("ep")
    t = lax.axis_index("tp")
    t1 = t + 1 - 2 * (t % 2)
    t2 = (t + 2) % group
    t3 = (t1 + 2) % group

    firsts = [
        pltpu.make_async_copy(a, b, fsem.at[n])
        for n, (a, b) in enumerate(
            [(expert_in, v_expert), (expert_gain, v_expert_gain), (ids, v_ids), (shares, v_shares),
             (mixer_in, v_mixer), (mixer_gain, v_mixer_gain),
             (all_taps.at[:, pl.ds(pl.multiple_of(t * chan, 128), chan)], taps)]
        )
    ]
    for load in firsts:
        load.start()
    loads = [
        pltpu.make_async_copy(a, b, wsem.at[n])
        for n, (a, b) in enumerate(
            [(w_in, v_in), (w_val, v_val), (w_out, v_out), (w_gate.at[0], v_gate),
             (w_up.at[0], v_up), (w_down.at[0], v_down), (w_proj, v_proj)]
        )
    ]
    def mixed_with(s):
        value, bit = 0, 1
        while bit < count:
            value = value + ((e // bit + s // bit) % 2) * bit
            bit *= 2
        return value

    barrier = pltpu.get_barrier_semaphore()
    for s in range(1, count):
        pl.semaphore_signal(barrier, inc=1, device_id=(mixed_with(s), t), device_id_type=MESH)
    for peer in (t1, t2):
        pl.semaphore_signal(barrier, inc=1, device_id=(e, peer), device_id_type=MESH)
    for load in firsts[:4]:
        load.wait()
    for load in loads:
        load.start()
    picks = v_ids.shape[0]
    slots = combine.shape[1]

    def table_of(block):
        sent = placed(columns, block, tok_dev, picks, slots, slot_cap, False)
        return jnp.transpose(sent).astype(BF16).reshape(slots // slot_cap, slot_cap, tok_dev)

    own_rows[...] = rms_rows(v_expert[...], v_expert_gain[...])
    fill_columns(v_ids, v_shares, columns)
    own_table[...] = table_of(t)
    pl.semaphore_wait(barrier, count + 1)

    def chunk(kind, i, src, dst, dev):
        return pltpu.make_async_remote_copy(
            src_ref=src, dst_ref=dst, send_sem=send.at[kind, i], recv_sem=recv.at[kind, i],
            device_id=dev, device_id_type=MESH,
        )

    def once(kind, src, dst, dev):
        return pltpu.make_async_remote_copy(
            src_ref=src, dst_ref=dst, send_sem=send1.at[kind], recv_sem=recv1.at[kind],
            device_id=dev, device_id_type=MESH,
        )

    near, across = (e, t1), (e, t2)
    after = ((e + 1) % count, t)

    def came(kind, i, dst):
        chunk(kind, i, dst, dst, near).wait_recv()

    def came_once(kind, dst):
        once(kind, dst, dst, near).wait_recv()

    def disp(i):
        return chunk(DISP, i, outgoing.at[i], arrived.at[e, t], (mixed_with(i), t))

    def disp2(i):
        return chunk(DISP2, i, outgoing2.at[i], arrived.at[e, t2], (mixed_with(i), t))

    def ret(i):
        return chunk(RET, i, res.at[i], returned.at[e], (mixed_with(i), t))

    once(DX, own_rows, dense, across).start()

    def sel(i):
        picked = dot(own_table[mixed_with(i)], own_rows[...]).astype(BF16)

        @pl.when(i == 0)
        def _():
            arrived[e, t] = picked

        @pl.when(i != 0)
        def _():
            outgoing[i] = picked
            disp(i).start()

    def dxw(i):
        came_once(DX, dense)

    def d2(i):
        picked = dot(partner_table[mixed_with(i)], dense[...]).astype(BF16)

        @pl.when(i == 0)
        def _():
            arrived[e, t2] = picked

        @pl.when(i != 0)
        def _():
            outgoing2[i] = picked
            disp2(i).start()

    def mixp(i):
        for load in firsts[4:]:
            load.wait()
        normed[...] = rms_rows(v_mixer[...], v_mixer_gain[...])
        rows[t] = normed[...]
        once(M1, normed, rows.at[t], near).start()

    def ptab(i):
        partner_table[...] = table_of(t2)

    def comb(i):
        def one(block, carry):
            part = pl.ds(pl.multiple_of(block * tok_dev, tok_dev), tok_dev)
            combine[part, :] = placed(columns, block, tok_dev, picks, slots, slot_cap, True)
            return carry

        lax.fori_loop(0, group, one, 0)

    def m2_piece(i, home, dev):
        cols = pl.ds(pl.multiple_of(i * (width // PIECES), 128), width // PIECES)
        return chunk(M2, i, normed.at[:, cols], rows.at[home, :, cols], dev)

    def q2_piece(i, home, dev):
        part = pl.ds(pl.multiple_of(i * (all_rows // PIECES), 16), all_rows // PIECES)
        return chunk(Q2, i, gated.at[home, part], gated.at[home, part], dev)

    def m2(i):
        m2_piece(i, t, across).start()

    def mixg(i):
        for n in range(PIECES):
            m2_piece(n, t2, near).wait_recv()
        once(MG, rows.at[t2], rows.at[t2], near).start()

    def loadw(i):
        for load in loads:
            load.wait()

    def take(i):
        src = mixed_with(i)

        @pl.when(i != 0)
        def _():
            came(DISP, i, arrived.at[src, t])

        @pl.when(i >= half)
        def _():
            chunk(F2, i, arrived.at[src, t], arrived.at[src, t], across).start()

        chunk(F1, i, arrived.at[src, t], arrived.at[src, t], near).start()

    def hand_rows(i):
        src = mixed_with(i)

        @pl.when(i >= half)
        def _():
            came(F2, i, arrived.at[src, t2])

        @pl.when((i < half) & (i != 0))
        def _():
            came(DISP2, i, arrived.at[src, t2])

        chunk(G1, i, arrived.at[src, t2], arrived.at[src, t2], near).start()

    def expand(i):
        src = mixed_with(i)
        came(F1, i, arrived.at[src, t1])
        came(G1, i, arrived.at[src, t3])
        x = arrived[src].reshape(group * slot_cap, width)
        gate = dot(x, v_gate[...])
        up = dot(x, v_up[...])
        hid[src, t] = (gate / (1.0 + jnp.exp(-gate)) * up).astype(BF16)
        chunk(H2, i, hid.at[src, t], hid.at[src, t], across).start()
        chunk(H1, i, hid.at[src, t], hid.at[src, t], near).start()

    def hand_hidden(i):
        src = mixed_with(i)
        came(H2, i, hid.at[src, t2])
        chunk(HG, i, hid.at[src, t2], hid.at[src, t2], near).start()

    def finish(i):
        src = mixed_with(i)
        came(H1, i, hid.at[src, t1])
        came(HG, i, hid.at[src, t3])
        total = dot(hid[src, 0], v_down[0:hid_width, :])
        for other in range(1, group):
            total += dot(hid[src, other], v_down[other * hid_width : (other + 1) * hid_width, :])
        total = total.astype(BF16).reshape(group, slot_cap, chan)

        @pl.when(i != 0)
        def _():
            res[i] = total
            ret(i).start()

        @pl.when(i == 0)
        def _():
            returned[src] = total

    tile = 256

    def mixer_products(i):
        came_once(M1, rows.at[t1])
        came_once(MG, rows.at[t3])

        def one(n, carry):
            cols = pl.ds(pl.multiple_of(n * tile, tile), tile)
            x = rows[...].reshape(all_rows, width)
            product = (dot(x, v_in[:, cols]) * dot(x, v_val[:, cols])).astype(BF16)
            ext[pl.ds(8, all_rows), cols] = product.astype(F32)
            rim_out[:, cols] = product[all_rows - 16 :]
            gates[:, cols] = dot(x, v_out[:, cols])
            return carry

        lax.fori_loop(0, chan // tile, one, 0)
        once(RIM, rim_out, rim_in, after).start()

    def mixer_conv(i):
        came_once(RIM, rim_in)
        edge = rim_in[...].astype(F32)[8:16]
        ext[0:8, :] = jnp.where(e == 0, jnp.zeros_like(edge), edge)
        tap_count = taps.shape[0]
        total = taps[0:1, :] * ext[pl.ds(8 - (tap_count - 1), all_rows), :]
        for n in range(1, tap_count):
            total += taps[n : n + 1, :] * ext[pl.ds(8 - (tap_count - 1) + n, all_rows), :]
        gated[t] = (gates[...] * total).astype(BF16)
        once(Q1, gated.at[t], gated.at[t], near).start()

    def q2(i):
        q2_piece(i, t, across).start()

    def convg(i):
        for n in range(PIECES):
            q2_piece(n, t2, near).wait_recv()
        once(QG, gated.at[t2], gated.at[t2], near).start()

    def mixer_project(i):
        came_once(Q1, gated.at[t1])
        came_once(QG, gated.at[t3])

        def one(n, carry):
            cols = pl.ds(pl.multiple_of(n * tile, tile), tile)
            total = dot(gated[0], v_proj[0:chan, cols])
            for other in range(1, group):
                total += dot(gated[other], v_proj[other * chan : (other + 1) * chan, cols])
            mixer_out[:, cols] = total.astype(BF16)
            return carry

        lax.fori_loop(0, chan // tile, one, 0)

    def rest(i):
        pass

    bodies = (
        sel, dxw, d2, ptab, comb, mixp, m2, mixg, loadw, mixer_products, mixer_conv, q2, convg, mixer_project,
        take, hand_rows, expand, hand_hidden, finish, rest,
    )
    middle = (e >= count // 4) & (e < 3 * count // 4)
    steps = max(len(END_STEPS), len(MIDDLE_STEPS))
    tables = [table + ((REST, 0),) * (steps - len(table)) for table in (END_STEPS, MIDDLE_STEPS)]

    def step(n, carry):
        at = [[looked_up(list(part), n) for part in zip(*table)] for table in tables]
        stage, shift = [jnp.where(middle, inner, outer) for outer, inner in zip(*at)]
        choose(stage, 0, len(bodies), [functools.partial(body, shift) for body in bodies])
        return carry

    lax.fori_loop(0, steps, step, 0)

    def landed(i, carry):
        came(RET, i, returned.at[mixed_with(i)])
        return carry

    lax.fori_loop(1, count, landed, 0)
    for block in range(group):
        part = pl.ds(block * tok_dev, tok_dev)
        mix = combine[part, :]
        high = mix.astype(BF16)
        low = (mix - high.astype(F32)).astype(BF16)
        values = returned[:, block].reshape(count * slot_cap, chan)
        expert_out[part, :] = (dot(high, values) + dot(low, values)).astype(BF16)

    def drain(i, carry):
        src = mixed_with(i)
        chunk(F1, i, arrived.at[src, t], arrived.at[src, t], near).wait_send()

        @pl.when(i >= half)
        def _():
            chunk(F2, i, arrived.at[src, t], arrived.at[src, t], near).wait_send()

        @pl.when(i != 0)
        def _():
            disp(i).wait_send()
            ret(i).wait_send()

        @pl.when((i != 0) & (i < half))
        def _():
            disp2(i).wait_send()

        chunk(G1, i, arrived.at[src, t2], arrived.at[src, t2], near).wait_send()
        for kind in (H2, H1):
            chunk(kind, i, hid.at[src, t], hid.at[src, t], near).wait_send()
        chunk(HG, i, hid.at[src, t2], hid.at[src, t2], near).wait_send()
        return carry

    lax.fori_loop(0, count, drain, 0)
    once(M1, normed, rows.at[t], near).wait_send()
    for n in range(PIECES):
        m2_piece(n, t, near).wait_send()
        q2_piece(n, t, near).wait_send()
    once(MG, rows.at[t2], rows.at[t2], near).wait_send()
    once(DX, own_rows, dense, near).wait_send()
    once(Q1, gated.at[t], gated.at[t], near).wait_send()
    once(QG, gated.at[t2], gated.at[t2], near).wait_send()
    once(RIM, rim_out, rim_in, after).wait_send()


def write_kernel(mixer_sum, expert_sum, mixer_out, expert_out, held, sem):
    pairs = [(mixer_sum, mixer_out), (expert_sum, expert_out)]
    inward = [pltpu.make_async_copy(a, held.at[n], sem.at[n]) for n, (a, _) in enumerate(pairs)]
    outward = [pltpu.make_async_copy(held.at[n], b, sem.at[2 + n]) for n, (_, b) in enumerate(pairs)]
    for copy in inward:
        copy.start()
    for first, second in zip(inward, outward):
        first.wait()
        second.start()
    for copy in outward:
        copy.wait()


def fused_on_device(
    mixer_in, expert_in, mixer_gain, in_gate_weight, out_gate_weight, value_weight, conv_taps,
    mixer_proj, expert_gain, route_ids, route_weights, gate_weight, up_weight, down_weight,
):
    tok_dev, width = mixer_in.shape
    group = lax.axis_size("tp")
    count = lax.axis_size("ep")
    experts = count * gate_weight.shape[0]
    slot_cap = 2 * tok_dev * route_ids.shape[1] // experts
    chan = in_gate_weight.shape[1]
    hid_width = gate_weight.shape[2]
    all_rows = group * tok_dev
    vm = pl.BlockSpec(memory_space=pltpu.VMEM)
    anywhere = pl.BlockSpec(memory_space=pl.ANY)
    shape = jax.ShapeDtypeStruct
    weights = (
        in_gate_weight, out_gate_weight, value_weight, mixer_proj, gate_weight, up_weight, down_weight,
    )
    dma = pltpu.SemaphoreType.DMA
    results = pl.pallas_call(
        exchange_kernel,
        out_shape=(shape((all_rows, chan), BF16), shape((all_rows, chan), BF16)),
        in_specs=[pl.BlockSpec(memory_space=pltpu.HBM)] * 14,
        out_specs=(vm, vm),
        scratch_shapes=[
            pltpu.VMEM(w.shape[-2:], BF16)
            for w in (in_gate_weight, out_gate_weight, value_weight, mixer_proj,
                      gate_weight, up_weight, down_weight)
        ] + [
            pltpu.VMEM((tok_dev, width), BF16),
            pltpu.VMEM((tok_dev, width), BF16),
            pltpu.VMEM((1, width), F32),
            pltpu.VMEM((1, width), F32),
            pltpu.VMEM(route_ids.shape[::-1], jnp.int32),
            pltpu.VMEM(route_ids.shape[::-1], F32),
            pltpu.VMEM((conv_taps.shape[0], chan), F32),
            pltpu.VMEM((all_rows, 8), F32),
            pltpu.VMEM((tok_dev, width), BF16),
            pltpu.VMEM((tok_dev, width), BF16),
            pltpu.VMEM((experts, slot_cap, tok_dev), BF16),
            pltpu.VMEM((experts, slot_cap, width), BF16),
            pltpu.VMEM((experts, slot_cap, tok_dev), BF16),
            pltpu.VMEM((all_rows, experts * slot_cap), F32),
            pltpu.VMEM((group, tok_dev, width), BF16),
            pltpu.VMEM((count, group, slot_cap, width), BF16),
            pltpu.VMEM((count, group, group * slot_cap, hid_width), BF16),
            pltpu.VMEM((count, group, slot_cap, chan), BF16),
            pltpu.VMEM((count, group, slot_cap, chan), BF16),
            pltpu.VMEM((all_rows, chan), F32),
            pltpu.VMEM((all_rows + 8, chan), F32),
            pltpu.VMEM((16, chan), BF16),
            pltpu.VMEM((16, chan), BF16),
            pltpu.VMEM((group, all_rows, chan), BF16),
            pltpu.VMEM((tok_dev, width), BF16),
            pltpu.VMEM((count // 2, slot_cap, width), BF16),
            dma((11, count)), dma((11, count)), dma((6,)), dma((6,)), dma((7,)), dma((7,)),
        ],
        compiler_params=pltpu.CompilerParams(
            collective_id=0, has_side_effects=True, vmem_limit_bytes=VMEM_BYTES
        ),
        name="exchange",
    )(
        mixer_in, expert_in, mixer_gain[None, :], expert_gain[None, :],
        route_ids.T, route_weights.T, conv_taps, *weights,
    )
    return pl.pallas_call(
        write_kernel,
        out_shape=(shape((all_rows, chan), BF16), shape((all_rows, chan), BF16)),
        in_specs=[anywhere, anywhere],
        out_specs=(anywhere, anywhere),
        scratch_shapes=[pltpu.VMEM((2, all_rows, chan), BF16), dma((4,))],
        compiler_params=pltpu.CompilerParams(vmem_limit_bytes=VMEM_BYTES),
        name="write",
    )(*results)


def body_for(mesh):
    count, group = mesh.shape["ep"], mesh.shape["tp"]

    def body(*args):
        tok_dev, picks, held = args[0].shape[0], args[9].shape[1], args[11].shape[0]
        slot_cap = 2 * tok_dev * picks // (count * held)
        fits = count == 8 and group == 4 and held == 1 and slot_cap % 16 == 0
        return (fused_on_device if fits and tok_dev % 16 == 0 else on_device)(*args)

    return body


def solution(mesh):
    return jax.shard_map(
        body_for(mesh),
        mesh=mesh,
        in_specs=(
            P(("ep", "tp"), None),
            P(("ep", "tp"), None),
            P(),
            P(None, "tp"),
            P(None, "tp"),
            P(None, "tp"),
            P(),
            P(None, "tp"),
            P(),
            P("ep", None),
            P("ep", None),
            P("ep", None, "tp"),
            P("ep", None, "tp"),
            P("ep", None, "tp"),
        ),
        out_specs=(P("ep", "tp"), P("ep", "tp")),
        check_vma=False,
    )
```

```python
import functools

import jax
import jax.numpy as jnp
from jax import lax
from jax.experimental import pallas as pl
from jax.experimental.pallas import tpu as pltpu
from jax.sharding import PartitionSpec as P

norm_eps = 1e-06


def passed_along(value, axis, steps):
    count = lax.axis_size(axis)
    leading, last = (max(0, -steps), min(count, count - steps))
    return lax.ppermute(value, axis, [(source, source + steps) for source in range(leading, last)])


def rms_rows(values, gain_row):
    wide = values.astype(jnp.float32)
    scale = lax.rsqrt(jnp.mean(wide * wide, axis=-1, keepdims=True) + norm_eps)
    return (wide * scale * gain_row).astype(jnp.bfloat16)


def place_slots(route_ids, group_rows, experts, slot_cap):
    row_total, top_count = route_ids.shape
    groups = row_total // group_rows
    labels = jnp.arange(experts, dtype=jnp.int32)
    onehot = (
        route_ids.reshape(groups, group_rows * top_count)[:, :, None] == labels[None, None, :]
    ).astype(jnp.int32)
    earlier = jnp.cumsum(onehot, axis=1) - onehot
    within = jnp.sum(earlier * onehot, axis=2)
    slot_index = jnp.arange(groups, dtype=jnp.int32)[:, None] * slot_cap + within
    return slot_index.reshape(row_total, top_count)


def on_device(
    mixer_in,
    expert_in,
    mixer_gain,
    in_gate_weight,
    out_gate_weight,
    value_weight,
    conv_taps,
    mixer_proj,
    expert_gain,
    route_ids,
    route_weights,
    gate_weight,
    up_weight,
    down_weight,
):
    tok_dev = mixer_in.shape[0]
    tp_count = lax.axis_size("tp")
    ep_count = lax.axis_size("ep")
    top_count = route_ids.shape[1]
    experts = ep_count * gate_weight.shape[0]
    slot_cap = max(2, 2 * tok_dev * top_count // experts)
    tp_index = lax.axis_index("tp")
    mixer_normed = rms_rows(mixer_in, mixer_gain)
    expert_normed = rms_rows(expert_in, expert_gain)
    block_slot = place_slots(route_ids, tok_dev, experts, slot_cap)
    mixer_rows = lax.all_gather(mixer_normed, "tp", axis=0, tiled=True)
    send_ids = lax.dynamic_slice_in_dim(route_ids, tp_index * tok_dev, tok_dev, 0)
    send_slot = (
        lax.dynamic_slice_in_dim(block_slot, tp_index * tok_dev, tok_dev, 0) - tp_index * slot_cap
    )
    source_count = expert_normed.shape[0]
    flat_index = (send_ids * slot_cap + send_slot).reshape(-1)
    row_table = (
        jnp.full((experts * slot_cap,), source_count, jnp.int32)
        .at[flat_index]
        .set(jnp.repeat(jnp.arange(source_count, dtype=jnp.int32), top_count))
    )
    padded_rows = jnp.concatenate(
        [expert_normed, jnp.zeros((1, expert_normed.shape[1]), jnp.bfloat16)], axis=0
    )
    outgoing = padded_rows[row_table].reshape(experts, slot_cap, expert_normed.shape[1])
    arrived = lax.all_to_all(outgoing, "ep", split_axis=0, concat_axis=0, tiled=True)
    arrived = lax.all_gather(arrived, "tp", axis=1, tiled=True)
    chan_width = in_gate_weight.shape[1]
    in_gate = jnp.dot(mixer_rows, in_gate_weight, preferred_element_type=jnp.float32)
    out_gate = jnp.dot(mixer_rows, out_gate_weight, preferred_element_type=jnp.float32)
    values = jnp.dot(mixer_rows, value_weight, preferred_element_type=jnp.float32)
    product = (in_gate * values).astype(jnp.bfloat16)
    tap_count = conv_taps.shape[0]
    rim_rows = passed_along(product[product.shape[0] - (tap_count - 1) :], "ep", 1)
    extended = jnp.concatenate([rim_rows, product], axis=0).astype(jnp.float32)
    tap_rows = lax.dynamic_slice_in_dim(conv_taps, tp_index * chan_width, chan_width, 1)
    row_count = product.shape[0]
    conv_sum = tap_rows[0] * extended[0:row_count]
    for tap_index in range(1, tap_count):
        conv_sum = conv_sum + tap_rows[tap_index] * extended[tap_index : tap_index + row_count]
    gated = (out_gate * conv_sum).astype(jnp.bfloat16)
    slots_in = arrived.reshape(-1, arrived.shape[2])
    gate_pre = jnp.dot(slots_in, gate_weight[0], preferred_element_type=jnp.float32)
    up_pre = jnp.dot(slots_in, up_weight[0], preferred_element_type=jnp.float32)
    hidden = (jax.nn.silu(gate_pre) * up_pre).astype(jnp.bfloat16)
    down_slice = down_weight[0]
    gated_all, hidden_all = (
        lax.all_gather(gated, "tp", axis=1, tiled=True),
        lax.all_gather(hidden, "tp", axis=1, tiled=True),
    )
    mixer_sum = jnp.dot(gated_all, mixer_proj, preferred_element_type=jnp.float32)
    expert_sum = jnp.dot(hidden_all, down_slice, preferred_element_type=jnp.float32)
    mixer_out = mixer_sum.astype(jnp.bfloat16)
    results = expert_sum.astype(jnp.bfloat16).reshape(ep_count, -1, expert_sum.shape[1])
    returned = lax.all_to_all(results, "ep", split_axis=0, concat_axis=0, tiled=True)
    back_index = (route_ids * (tp_count * slot_cap) + block_slot).reshape(-1)
    picked = returned.reshape(-1, returned.shape[2])[back_index].reshape(
        route_ids.shape[0], top_count, -1
    )
    shares = route_weights / jnp.sum(route_weights, axis=1, keepdims=True)
    expert_out = jnp.sum(picked.astype(jnp.float32) * shares[:, :, None], axis=1).astype(
        jnp.bfloat16
    )
    return (mixer_out, expert_out)


MESH = pl.DeviceIdType.MESH
F32 = jnp.float32
BF16 = jnp.bfloat16
VMEM_BYTES = 60 * 1024 * 1024


def dot(a, b):
    return jnp.dot(a, b, preferred_element_type=F32)


def fill_columns(ids, weights, routes, columns):
    picks, all_rows = ids.shape
    filler = jnp.zeros((8 - 2 * picks, all_rows), F32)
    routes[...] = jnp.concatenate([ids[...].astype(F32), weights[...], filler], axis=0)
    columns[...] = jnp.transpose(routes[...])


def placed(columns, block, tok_dev, picks, slots, slot_cap, shared):
    own = columns[pl.ds(pl.multiple_of(block * tok_dev, tok_dev), tok_dev), :]
    below = (
        lax.broadcasted_iota(jnp.int32, (tok_dev, tok_dev), 1)
        < lax.broadcasted_iota(jnp.int32, (tok_dev, tok_dev), 0)
    ).astype(BF16)
    labels = lax.broadcasted_iota(jnp.int32, (tok_dev, 128), 1)
    places = lax.broadcasted_iota(jnp.int32, (tok_dev, slots), 1)
    named = [own[:, k : k + 1].astype(jnp.int32) for k in range(picks)]
    share = [own[:, picks + k : picks + k + 1] for k in range(picks)]
    total = functools.reduce(jnp.add, share)
    hot = [(labels == n).astype(F32) for n in named]
    rank = dot(below, functools.reduce(jnp.add, hot).astype(BF16))
    result = jnp.zeros((tok_dev, slots), F32)
    for k in range(picks):
        within = jnp.sum(rank * hot[k], axis=1, keepdims=True).astype(jnp.int32)
        spot = places == named[k] * slot_cap + within
        result = result + jnp.where(spot, share[k] / total if shared else 1.0, 0.0)
    return result


(
    SEL, DXW, D2, PTAB, COMB, MIXP, M2S, MIXG, LOADW, MIXPROD, CONV, Q2S, CONVG, PROJ,
    TAKE, ROWS, EXP, HH, FIN, REST, FARW, GSEL,
) = range(22)

PIECES = 4

GATES = (4,)

END_STEPS = (
    (PTAB, 0), (MIXP, 0), (TAKE, 3), (M2S, 3), (SEL, 2), (M2S, 2), (M2S, 1),
    (TAKE, 4), (SEL, 1), (DXW, 0), (D2, 2), (M2S, 0), (ROWS, 4), (D2, 1),
    (ROWS, 3), (COMB, 0), (D2, 3), (LOADW, 0), (EXP, 4), (SEL, 3), (TAKE, 5),
    (MIXG, 0), (HH, 4), (TAKE, 7), (FIN, 4), (ROWS, 5), (TAKE, 6), (MIXPROD, 0),
    (ROWS, 7), (EXP, 5), (ROWS, 1), (ROWS, 2), (CONV, 0), (EXP, 7), (SEL, 0),
    (ROWS, 6), (EXP, 3), (D2, 0), (TAKE, 1), (EXP, 6), (ROWS, 0), (Q2S, 2),
    (HH, 7), (Q2S, 3), (FIN, 7), (TAKE, 0), (Q2S, 0), (HH, 3), (HH, 6),
    (TAKE, 2), (EXP, 1), (FIN, 6), (HH, 5), (EXP, 2), (FIN, 3), (Q2S, 1),
    (EXP, 0), (FIN, 5), (HH, 1), (HH, 2), (CONVG, 0), (FIN, 1), (FIN, 2),
    (PROJ, 0), (HH, 0), (FIN, 0),
)

MIDDLE_STEPS = (
    (SEL, 4), (SEL, 3), (MIXP, 0), (PTAB, 0), (M2S, 3), (SEL, 1), (SEL, 7),
    (COMB, 0), (SEL, 5), (DXW, 0), (D2, 3), (M2S, 1), (M2S, 0), (FARW, 4),
    (GSEL, 4), (GSEL, 5), (TAKE, 4), (TAKE, 1), (TAKE, 7), (D2, 1), (ROWS, 4),
    (D2, 0), (GSEL, 7), (LOADW, 0), (EXP, 4), (SEL, 6), (SEL, 0), (M2S, 2),
    (ROWS, 7), (GSEL, 6), (D2, 2), (EXP, 7), (TAKE, 5), (MIXG, 0), (MIXPROD, 0),
    (TAKE, 3), (HH, 4), (TAKE, 6), (HH, 7), (ROWS, 0), (ROWS, 2), (ROWS, 3),
    (TAKE, 2), (FIN, 4), (ROWS, 1), (FIN, 7), (EXP, 1), (EXP, 3), (SEL, 2),
    (ROWS, 6), (CONV, 0), (ROWS, 5), (EXP, 2), (HH, 3), (TAKE, 0), (EXP, 5),
    (EXP, 0), (EXP, 6), (HH, 1), (Q2S, 2), (HH, 0), (HH, 5), (FIN, 3),
    (Q2S, 0), (Q2S, 3), (HH, 2), (Q2S, 1), (FIN, 1), (FIN, 5), (FIN, 2),
    (FIN, 0), (HH, 6), (FIN, 6), (CONVG, 0), (PROJ, 0),
)


DISP, F2, F1, G1, H2, H1, HG, RET, DISP2, M2, Q2, FARR, FARI, GD = range(14)
M1, MG, Q1, QG, RIM, DX = range(6)


def looked_up(values, i):
    bit = 1
    while len(values) > 1:
        odd = (i // bit) % 2 == 1
        values = [
            jnp.where(odd, pair[-1], pair[0]) if pair[0] is not pair[-1] else pair[0]
            for pair in (values[n : n + 2] for n in range(0, len(values), 2))
        ]
        bit *= 2
    return values[0]


def choose(stage, low, high, bodies):
    if high - low == 1:
        bodies[low]()
        return
    middle = (low + high) // 2
    for below in (True, False):
        @pl.when((stage < middle) if below else (stage >= middle))
        def _(below=below):
            choose(stage, *((low, middle) if below else (middle, high)), bodies)


def exchange_kernel(
    mixer_in, expert_in, mixer_gain, expert_gain, ids, shares, all_taps,
    w_in, w_out, w_val, w_proj, w_gate, w_up, w_down,
    mixer_out, expert_out,
    v_in, v_out, v_val, v_proj, v_gate, v_up, v_down,
    v_mixer, v_expert, v_mixer_gain, v_expert_gain, v_ids, v_shares, taps,
    columns, normed, own_rows, own_table, outgoing, partner_table, combine,
    rows, arrived, hid, res, returned, gates, ext, rim_out, rim_in, gated, dense, outgoing2, routes, far_rows, far_routes, far_columns, far_tables, far_out,
    send, recv, send1, recv1, wsem, fsem,
):
    count = outgoing.shape[0]
    group, tok_dev, width = rows.shape
    half = count // 2
    all_rows = group * tok_dev
    chan = v_in.shape[1]
    slot_cap = outgoing.shape[1]
    hid_width = v_gate.shape[1]
    e = lax.axis_index("ep")
    t = lax.axis_index("tp")
    t1 = t + 1 - 2 * (t % 2)
    t2 = (t + 2) % group
    t3 = (t1 + 2) % group

    firsts = [
        pltpu.make_async_copy(a, b, fsem.at[n])
        for n, (a, b) in enumerate(
            [(expert_in, v_expert), (expert_gain, v_expert_gain), (ids, v_ids), (shares, v_shares),
             (mixer_in, v_mixer), (mixer_gain, v_mixer_gain),
             (all_taps.at[:, pl.ds(pl.multiple_of(t * chan, 128), chan)], taps)]
        )
    ]
    for load in firsts:
        load.start()
    loads = [
        pltpu.make_async_copy(a, b, wsem.at[n])
        for n, (a, b) in enumerate(
            [(w_in, v_in), (w_val, v_val), (w_out, v_out), (w_gate.at[0], v_gate),
             (w_up.at[0], v_up), (w_down.at[0], v_down), (w_proj, v_proj)]
        )
    ]
    def xor(a, b):
        value, bit = 0, 1
        while bit < count:
            value = value + ((a // bit + b // bit) % 2) * bit
            bit *= 2
        return value

    def mixed_with(s):
        return xor(e, s)

    middle = (e >= count // 4) & (e < 3 * count // 4)

    barrier = pltpu.get_barrier_semaphore()
    for s in range(1, count):
        pl.semaphore_signal(barrier, inc=1, device_id=(mixed_with(s), t), device_id_type=MESH)
    for peer in (t1, t2):
        pl.semaphore_signal(barrier, inc=1, device_id=(e, peer), device_id_type=MESH)
    for load in firsts[:4]:
        load.wait()
    for load in loads:
        load.start()
    picks = v_ids.shape[0]
    slots = combine.shape[1]

    def table_of(source, block):
        sent = placed(source, block, tok_dev, picks, slots, slot_cap, False)
        return jnp.transpose(sent).astype(BF16).reshape(slots // slot_cap, slot_cap, tok_dev)

    own_rows[...] = rms_rows(v_expert[...], v_expert_gain[...])
    fill_columns(v_ids, v_shares, routes, columns)
    own_table[...] = table_of(columns, t)
    pl.semaphore_wait(barrier, count + 1)

    def chunk(kind, i, src, dst, dev):
        return pltpu.make_async_remote_copy(
            src_ref=src, dst_ref=dst, send_sem=send.at[kind, i], recv_sem=recv.at[kind, i],
            device_id=dev, device_id_type=MESH,
        )

    def once(kind, src, dst, dev):
        return pltpu.make_async_remote_copy(
            src_ref=src, dst_ref=dst, send_sem=send1.at[kind], recv_sem=recv1.at[kind],
            device_id=dev, device_id_type=MESH,
        )

    near, across = (e, t1), (e, t2)
    after = ((e + 1) % count, t)

    def came(kind, i, dst):
        chunk(kind, i, dst, dst, near).wait_recv()

    def came_once(kind, dst):
        once(kind, dst, dst, near).wait_recv()

    def disp(i):
        return chunk(DISP, i, outgoing.at[i], arrived.at[e, t], (mixed_with(i), t))

    def disp2(i):
        return chunk(DISP2, i, outgoing2.at[i], arrived.at[e, t2], (mixed_with(i), t))

    def ret(i):
        return chunk(RET, i, res.at[i], returned.at[e], (mixed_with(i), t))

    def far_pair(gate):
        dev = (mixed_with(gate), t)
        slot = GATES.index(gate)
        return (
            chunk(FARR, slot, own_rows, far_rows.at[slot], dev),
            chunk(FARI, slot, routes, far_routes.at[slot], dev),
        )

    def for_far(act):
        for gate in GATES:
            @pl.when(middle if gate == count - 2 else ~middle)
            def _(gate=gate):
                for copy in far_pair(gate):
                    act(copy)

    for_far(lambda copy: copy.start())
    once(DX, own_rows, dense, across).start()

    def farw(i):
        slot = (i - half) // 2 if len(GATES) > 1 else 0
        for copy in (
            chunk(FARR, slot, far_rows.at[slot], far_rows.at[slot], near),
            chunk(FARI, slot, far_routes.at[slot], far_routes.at[slot], near),
        ):
            copy.wait_recv()
        far_columns[...] = jnp.transpose(far_routes[slot])
        far_tables[slot] = table_of(far_columns, t)

    def passed(i):
        gate = jnp.where(i >= count, GATES[-1], GATES[0])
        slot = i // count
        shift = i % count
        return gate, slot, shift, xor(mixed_with(gate), shift)

    def gsend(i):
        gate, slot, shift, expert = passed(i)
        return pltpu.make_async_remote_copy(
            src_ref=far_out.at[slot, shift - half], dst_ref=arrived.at[mixed_with(gate), t],
            send_sem=send.at[GD, slot * half + shift - half], recv_sem=recv.at[DISP, shift],
            device_id=(expert, t), device_id_type=MESH,
        )

    def gsel(i):
        gate, slot, shift, expert = passed(i)
        picked = dot(far_tables[slot, expert], far_rows[slot]).astype(BF16)

        @pl.when(shift == gate)
        def _():
            arrived[mixed_with(gate), t] = picked

        @pl.when(shift != gate)
        def _():
            far_out[slot, shift - half] = picked
            gsend(i).start()

    def sel(i):
        picked = dot(own_table[mixed_with(i)], own_rows[...]).astype(BF16)

        @pl.when(i == 0)
        def _():
            arrived[e, t] = picked

        @pl.when(i != 0)
        def _():
            outgoing[i] = picked
            disp(i).start()

    def dxw(i):
        came_once(DX, dense)

    def d2(i):
        picked = dot(partner_table[mixed_with(i)], dense[...]).astype(BF16)

        @pl.when(i == 0)
        def _():
            arrived[e, t2] = picked

        @pl.when(i != 0)
        def _():
            outgoing2[i] = picked
            disp2(i).start()

    def mixp(i):
        for load in firsts[4:]:
            load.wait()
        normed[...] = rms_rows(v_mixer[...], v_mixer_gain[...])
        rows[t] = normed[...]
        once(M1, normed, rows.at[t], near).start()

    def ptab(i):
        partner_table[...] = table_of(columns, t2)

    def comb(i):
        def one(block, carry):
            part = pl.ds(pl.multiple_of(block * tok_dev, tok_dev), tok_dev)
            combine[part, :] = placed(columns, block, tok_dev, picks, slots, slot_cap, True)
            return carry

        lax.fori_loop(0, group, one, 0)

    def m2_piece(i, home, dev):
        cols = pl.ds(pl.multiple_of(i * (width // PIECES), 128), width // PIECES)
        return chunk(M2, i, normed.at[:, cols], rows.at[home, :, cols], dev)

    def q2_piece(i, home, dev):
        part = pl.ds(pl.multiple_of(i * (all_rows // PIECES), 16), all_rows // PIECES)
        return chunk(Q2, i, gated.at[home, part], gated.at[home, part], dev)

    def m2(i):
        m2_piece(i, t, across).start()

    def mixg(i):
        for n in range(PIECES):
            m2_piece(n, t2, near).wait_recv()
        once(MG, rows.at[t2], rows.at[t2], near).start()

    def loadw(i):
        for load in loads:
            load.wait()

    def take(i):
        src = mixed_with(i)
        here = i == 0
        for gate in GATES:
            here = here | (middle & (i == gate))

        @pl.when(~here)
        def _():
            came(DISP, i, arrived.at[src, t])

        @pl.when(i >= half)
        def _():
            chunk(F2, i, arrived.at[src, t], arrived.at[src, t], across).start()

        chunk(F1, i, arrived.at[src, t], arrived.at[src, t], near).start()

    def hand_rows(i):
        src = mixed_with(i)

        @pl.when(i >= half)
        def _():
            came(F2, i, arrived.at[src, t2])

        @pl.when((i < half) & (i != 0))
        def _():
            came(DISP2, i, arrived.at[src, t2])

        chunk(G1, i, arrived.at[src, t2], arrived.at[src, t2], near).start()

    def expand(i):
        src = mixed_with(i)
        came(F1, i, arrived.at[src, t1])
        came(G1, i, arrived.at[src, t3])
        x = arrived[src].reshape(group * slot_cap, width)
        gate = dot(x, v_gate[...])
        up = dot(x, v_up[...])
        hid[src, t] = (gate / (1.0 + jnp.exp(-gate)) * up).astype(BF16)
        chunk(H2, i, hid.at[src, t], hid.at[src, t], across).start()
        chunk(H1, i, hid.at[src, t], hid.at[src, t], near).start()

    def hand_hidden(i):
        src = mixed_with(i)
        came(H2, i, hid.at[src, t2])
        chunk(HG, i, hid.at[src, t2], hid.at[src, t2], near).start()

    def finish(i):
        src = mixed_with(i)
        came(H1, i, hid.at[src, t1])
        came(HG, i, hid.at[src, t3])
        total = dot(hid[src, 0], v_down[0:hid_width, :])
        for other in range(1, group):
            total += dot(hid[src, other], v_down[other * hid_width : (other + 1) * hid_width, :])
        total = total.astype(BF16).reshape(group, slot_cap, chan)

        @pl.when(i != 0)
        def _():
            res[i] = total
            ret(i).start()

        @pl.when(i == 0)
        def _():
            returned[src] = total

    tile = 256

    def mixer_products(i):
        came_once(M1, rows.at[t1])
        came_once(MG, rows.at[t3])

        def one(n, carry):
            cols = pl.ds(pl.multiple_of(n * tile, tile), tile)
            x = rows[...].reshape(all_rows, width)
            product = (dot(x, v_in[:, cols]) * dot(x, v_val[:, cols])).astype(BF16)
            ext[pl.ds(8, all_rows), cols] = product.astype(F32)
            rim_out[:, cols] = product[all_rows - 16 :]
            gates[:, cols] = dot(x, v_out[:, cols])
            return carry

        lax.fori_loop(0, chan // tile, one, 0)
        once(RIM, rim_out, rim_in, after).start()

    def mixer_conv(i):
        came_once(RIM, rim_in)
        edge = rim_in[...].astype(F32)[8:16]
        ext[0:8, :] = jnp.where(e == 0, jnp.zeros_like(edge), edge)
        tap_count = taps.shape[0]
        total = taps[0:1, :] * ext[pl.ds(8 - (tap_count - 1), all_rows), :]
        for n in range(1, tap_count):
            total += taps[n : n + 1, :] * ext[pl.ds(8 - (tap_count - 1) + n, all_rows), :]
        gated[t] = (gates[...] * total).astype(BF16)
        once(Q1, gated.at[t], gated.at[t], near).start()

    def q2(i):
        q2_piece(i, t, across).start()

    def convg(i):
        for n in range(PIECES):
            q2_piece(n, t2, near).wait_recv()
        once(QG, gated.at[t2], gated.at[t2], near).start()

    def mixer_project(i):
        came_once(Q1, gated.at[t1])
        came_once(QG, gated.at[t3])

        def one(n, carry):
            cols = pl.ds(pl.multiple_of(n * tile, tile), tile)
            total = dot(gated[0], v_proj[0:chan, cols])
            for other in range(1, group):
                total += dot(gated[other], v_proj[other * chan : (other + 1) * chan, cols])
            mixer_out[:, cols] = total.astype(BF16)
            return carry

        lax.fori_loop(0, chan // tile, one, 0)

    def rest(i):
        pass

    bodies = (
        sel, dxw, d2, ptab, comb, mixp, m2, mixg, loadw, mixer_products, mixer_conv, q2, convg, mixer_project,
        take, hand_rows, expand, hand_hidden, finish, rest, farw, gsel,
    )
    steps = max(len(END_STEPS), len(MIDDLE_STEPS))
    tables = [table + ((REST, 0),) * (steps - len(table)) for table in (END_STEPS, MIDDLE_STEPS)]

    def step(n, carry):
        at = [[looked_up(list(part), n) for part in zip(*table)] for table in tables]
        stage, shift = [jnp.where(middle, inner, outer) for outer, inner in zip(*at)]
        choose(stage, 0, len(bodies), [functools.partial(body, shift) for body in bodies])
        return carry

    lax.fori_loop(0, steps, step, 0)

    def landed(i, carry):
        came(RET, i, returned.at[mixed_with(i)])
        return carry

    lax.fori_loop(1, count, landed, 0)
    for block in range(group):
        part = pl.ds(block * tok_dev, tok_dev)
        mix = combine[part, :]
        high = mix.astype(BF16)
        low = (mix - high.astype(F32)).astype(BF16)
        values = returned[:, block].reshape(count * slot_cap, chan)
        expert_out[part, :] = (dot(high, values) + dot(low, values)).astype(BF16)

    def drain(i, carry):
        src = mixed_with(i)
        chunk(F1, i, arrived.at[src, t], arrived.at[src, t], near).wait_send()

        @pl.when(i >= half)
        def _():
            chunk(F2, i, arrived.at[src, t], arrived.at[src, t], near).wait_send()

        @pl.when(i != 0)
        def _():
            ret(i).wait_send()

        direct = (i < half) | jnp.where(middle, True, False)

        @pl.when((i != 0) & direct)
        def _():
            disp(i).wait_send()

        @pl.when((i != 0) & (i < half))
        def _():
            disp2(i).wait_send()

        chunk(G1, i, arrived.at[src, t2], arrived.at[src, t2], near).wait_send()
        for kind in (H2, H1):
            chunk(kind, i, hid.at[src, t], hid.at[src, t], near).wait_send()
        chunk(HG, i, hid.at[src, t2], hid.at[src, t2], near).wait_send()
        return carry

    lax.fori_loop(0, count, drain, 0)
    for_far(lambda copy: copy.wait_send())

    @pl.when(middle)
    def _():
        for slot, gate in enumerate(GATES):
            for shift in range(half, count):
                if shift != gate:
                    gsend(slot * count + shift).wait_send()

    once(M1, normed, rows.at[t], near).wait_send()
    for n in range(PIECES):
        m2_piece(n, t, near).wait_send()
        q2_piece(n, t, near).wait_send()
    once(MG, rows.at[t2], rows.at[t2], near).wait_send()
    once(DX, own_rows, dense, near).wait_send()
    once(Q1, gated.at[t], gated.at[t], near).wait_send()
    once(QG, gated.at[t2], gated.at[t2], near).wait_send()
    once(RIM, rim_out, rim_in, after).wait_send()


def write_kernel(mixer_sum, expert_sum, mixer_out, expert_out, held, sem):
    pairs = [(mixer_sum, mixer_out), (expert_sum, expert_out)]
    inward = [pltpu.make_async_copy(a, held.at[n], sem.at[n]) for n, (a, _) in enumerate(pairs)]
    outward = [pltpu.make_async_copy(held.at[n], b, sem.at[2 + n]) for n, (_, b) in enumerate(pairs)]
    for copy in inward:
        copy.start()
    for first, second in zip(inward, outward):
        first.wait()
        second.start()
    for copy in outward:
        copy.wait()


def fused_on_device(
    mixer_in, expert_in, mixer_gain, in_gate_weight, out_gate_weight, value_weight, conv_taps,
    mixer_proj, expert_gain, route_ids, route_weights, gate_weight, up_weight, down_weight,
):
    tok_dev, width = mixer_in.shape
    group = lax.axis_size("tp")
    count = lax.axis_size("ep")
    experts = count * gate_weight.shape[0]
    slot_cap = 2 * tok_dev * route_ids.shape[1] // experts
    chan = in_gate_weight.shape[1]
    hid_width = gate_weight.shape[2]
    all_rows = group * tok_dev
    vm = pl.BlockSpec(memory_space=pltpu.VMEM)
    anywhere = pl.BlockSpec(memory_space=pl.ANY)
    shape = jax.ShapeDtypeStruct
    weights = (
        in_gate_weight, out_gate_weight, value_weight, mixer_proj, gate_weight, up_weight, down_weight,
    )
    dma = pltpu.SemaphoreType.DMA
    results = pl.pallas_call(
        exchange_kernel,
        out_shape=(shape((all_rows, chan), BF16), shape((all_rows, chan), BF16)),
        in_specs=[pl.BlockSpec(memory_space=pltpu.HBM)] * 14,
        out_specs=(vm, vm),
        scratch_shapes=[
            pltpu.VMEM(w.shape[-2:], BF16)
            for w in (in_gate_weight, out_gate_weight, value_weight, mixer_proj,
                      gate_weight, up_weight, down_weight)
        ] + [
            pltpu.VMEM((tok_dev, width), BF16),
            pltpu.VMEM((tok_dev, width), BF16),
            pltpu.VMEM((1, width), F32),
            pltpu.VMEM((1, width), F32),
            pltpu.VMEM(route_ids.shape[::-1], jnp.int32),
            pltpu.VMEM(route_ids.shape[::-1], F32),
            pltpu.VMEM((conv_taps.shape[0], chan), F32),
            pltpu.VMEM((all_rows, 8), F32),
            pltpu.VMEM((tok_dev, width), BF16),
            pltpu.VMEM((tok_dev, width), BF16),
            pltpu.VMEM((experts, slot_cap, tok_dev), BF16),
            pltpu.VMEM((experts, slot_cap, width), BF16),
            pltpu.VMEM((experts, slot_cap, tok_dev), BF16),
            pltpu.VMEM((all_rows, experts * slot_cap), F32),
            pltpu.VMEM((group, tok_dev, width), BF16),
            pltpu.VMEM((count, group, slot_cap, width), BF16),
            pltpu.VMEM((count, group, group * slot_cap, hid_width), BF16),
            pltpu.VMEM((count, group, slot_cap, chan), BF16),
            pltpu.VMEM((count, group, slot_cap, chan), BF16),
            pltpu.VMEM((all_rows, chan), F32),
            pltpu.VMEM((all_rows + 8, chan), F32),
            pltpu.VMEM((16, chan), BF16),
            pltpu.VMEM((16, chan), BF16),
            pltpu.VMEM((group, all_rows, chan), BF16),
            pltpu.VMEM((tok_dev, width), BF16),
            pltpu.VMEM((count // 2, slot_cap, width), BF16),
            pltpu.VMEM((8, all_rows), F32),
            pltpu.VMEM((len(GATES), tok_dev, width), BF16),
            pltpu.VMEM((len(GATES), 8, all_rows), F32),
            pltpu.VMEM((all_rows, 8), F32),
            pltpu.VMEM((len(GATES), experts, slot_cap, tok_dev), BF16),
            pltpu.VMEM((len(GATES), count // 2, slot_cap, width), BF16),
            dma((14, count)), dma((14, count)), dma((6,)), dma((6,)), dma((7,)), dma((7,)),
        ],
        compiler_params=pltpu.CompilerParams(
            collective_id=0, has_side_effects=True, vmem_limit_bytes=VMEM_BYTES
        ),
        name="exchange",
    )(
        mixer_in, expert_in, mixer_gain[None, :], expert_gain[None, :],
        route_ids.T, route_weights.T, conv_taps, *weights,
    )
    return pl.pallas_call(
        write_kernel,
        out_shape=(shape((all_rows, chan), BF16), shape((all_rows, chan), BF16)),
        in_specs=[anywhere, anywhere],
        out_specs=(anywhere, anywhere),
        scratch_shapes=[pltpu.VMEM((2, all_rows, chan), BF16), dma((4,))],
        compiler_params=pltpu.CompilerParams(vmem_limit_bytes=VMEM_BYTES),
        name="write",
    )(*results)


def body_for(mesh):
    count, group = mesh.shape["ep"], mesh.shape["tp"]

    def body(*args):
        tok_dev, picks, held = args[0].shape[0], args[9].shape[1], args[11].shape[0]
        slot_cap = 2 * tok_dev * picks // (count * held)
        fits = count == 8 and group == 4 and held == 1 and slot_cap % 16 == 0
        return (fused_on_device if fits and tok_dev % 16 == 0 else on_device)(*args)

    return body


def solution(mesh):
    return jax.shard_map(
        body_for(mesh),
        mesh=mesh,
        in_specs=(
            P(("ep", "tp"), None),
            P(("ep", "tp"), None),
            P(),
            P(None, "tp"),
            P(None, "tp"),
            P(None, "tp"),
            P(),
            P(None, "tp"),
            P(),
            P("ep", None),
            P("ep", None),
            P("ep", None, "tp"),
            P("ep", None, "tp"),
            P("ep", None, "tp"),
        ),
        out_specs=(P("ep", "tp"), P("ep", "tp")),
        check_vma=False,
    )
```

```python
import functools

import jax
import jax.numpy as jnp
from jax import lax
from jax.experimental import pallas as pl
from jax.experimental.pallas import tpu as pltpu
from jax.sharding import PartitionSpec as P

norm_eps = 1e-06


def passed_along(value, axis, steps):
    count = lax.axis_size(axis)
    leading, last = (max(0, -steps), min(count, count - steps))
    return lax.ppermute(value, axis, [(source, source + steps) for source in range(leading, last)])


def rms_rows(values, gain_row):
    wide = values.astype(jnp.float32)
    scale = lax.rsqrt(jnp.mean(wide * wide, axis=-1, keepdims=True) + norm_eps)
    return (wide * scale * gain_row).astype(jnp.bfloat16)


def place_slots(route_ids, group_rows, experts, slot_cap):
    row_total, top_count = route_ids.shape
    groups = row_total // group_rows
    labels = jnp.arange(experts, dtype=jnp.int32)
    onehot = (
        route_ids.reshape(groups, group_rows * top_count)[:, :, None] == labels[None, None, :]
    ).astype(jnp.int32)
    earlier = jnp.cumsum(onehot, axis=1) - onehot
    within = jnp.sum(earlier * onehot, axis=2)
    slot_index = jnp.arange(groups, dtype=jnp.int32)[:, None] * slot_cap + within
    return slot_index.reshape(row_total, top_count)


def on_device(
    mixer_in,
    expert_in,
    mixer_gain,
    in_gate_weight,
    out_gate_weight,
    value_weight,
    conv_taps,
    mixer_proj,
    expert_gain,
    route_ids,
    route_weights,
    gate_weight,
    up_weight,
    down_weight,
):
    tok_dev = mixer_in.shape[0]
    tp_count = lax.axis_size("tp")
    ep_count = lax.axis_size("ep")
    top_count = route_ids.shape[1]
    experts = ep_count * gate_weight.shape[0]
    slot_cap = max(2, 2 * tok_dev * top_count // experts)
    tp_index = lax.axis_index("tp")
    mixer_normed = rms_rows(mixer_in, mixer_gain)
    expert_normed = rms_rows(expert_in, expert_gain)
    block_slot = place_slots(route_ids, tok_dev, experts, slot_cap)
    mixer_rows = lax.all_gather(mixer_normed, "tp", axis=0, tiled=True)
    send_ids = lax.dynamic_slice_in_dim(route_ids, tp_index * tok_dev, tok_dev, 0)
    send_slot = (
        lax.dynamic_slice_in_dim(block_slot, tp_index * tok_dev, tok_dev, 0) - tp_index * slot_cap
    )
    source_count = expert_normed.shape[0]
    flat_index = (send_ids * slot_cap + send_slot).reshape(-1)
    row_table = (
        jnp.full((experts * slot_cap,), source_count, jnp.int32)
        .at[flat_index]
        .set(jnp.repeat(jnp.arange(source_count, dtype=jnp.int32), top_count))
    )
    padded_rows = jnp.concatenate(
        [expert_normed, jnp.zeros((1, expert_normed.shape[1]), jnp.bfloat16)], axis=0
    )
    outgoing = padded_rows[row_table].reshape(experts, slot_cap, expert_normed.shape[1])
    arrived = lax.all_to_all(outgoing, "ep", split_axis=0, concat_axis=0, tiled=True)
    arrived = lax.all_gather(arrived, "tp", axis=1, tiled=True)
    chan_width = in_gate_weight.shape[1]
    in_gate = jnp.dot(mixer_rows, in_gate_weight, preferred_element_type=jnp.float32)
    out_gate = jnp.dot(mixer_rows, out_gate_weight, preferred_element_type=jnp.float32)
    values = jnp.dot(mixer_rows, value_weight, preferred_element_type=jnp.float32)
    product = (in_gate * values).astype(jnp.bfloat16)
    tap_count = conv_taps.shape[0]
    rim_rows = passed_along(product[product.shape[0] - (tap_count - 1) :], "ep", 1)
    extended = jnp.concatenate([rim_rows, product], axis=0).astype(jnp.float32)
    tap_rows = lax.dynamic_slice_in_dim(conv_taps, tp_index * chan_width, chan_width, 1)
    row_count = product.shape[0]
    conv_sum = tap_rows[0] * extended[0:row_count]
    for tap_index in range(1, tap_count):
        conv_sum = conv_sum + tap_rows[tap_index] * extended[tap_index : tap_index + row_count]
    gated = (out_gate * conv_sum).astype(jnp.bfloat16)
    slots_in = arrived.reshape(-1, arrived.shape[2])
    gate_pre = jnp.dot(slots_in, gate_weight[0], preferred_element_type=jnp.float32)
    up_pre = jnp.dot(slots_in, up_weight[0], preferred_element_type=jnp.float32)
    hidden = (jax.nn.silu(gate_pre) * up_pre).astype(jnp.bfloat16)
    down_slice = down_weight[0]
    gated_all, hidden_all = (
        lax.all_gather(gated, "tp", axis=1, tiled=True),
        lax.all_gather(hidden, "tp", axis=1, tiled=True),
    )
    mixer_sum = jnp.dot(gated_all, mixer_proj, preferred_element_type=jnp.float32)
    expert_sum = jnp.dot(hidden_all, down_slice, preferred_element_type=jnp.float32)
    mixer_out = mixer_sum.astype(jnp.bfloat16)
    results = expert_sum.astype(jnp.bfloat16).reshape(ep_count, -1, expert_sum.shape[1])
    returned = lax.all_to_all(results, "ep", split_axis=0, concat_axis=0, tiled=True)
    back_index = (route_ids * (tp_count * slot_cap) + block_slot).reshape(-1)
    picked = returned.reshape(-1, returned.shape[2])[back_index].reshape(
        route_ids.shape[0], top_count, -1
    )
    shares = route_weights / jnp.sum(route_weights, axis=1, keepdims=True)
    expert_out = jnp.sum(picked.astype(jnp.float32) * shares[:, :, None], axis=1).astype(
        jnp.bfloat16
    )
    return (mixer_out, expert_out)


MESH = pl.DeviceIdType.MESH
F32 = jnp.float32
BF16 = jnp.bfloat16
VMEM_BYTES = 60 * 1024 * 1024


def dot(a, b):
    return jnp.dot(a, b, preferred_element_type=F32)


def fill_columns(ids, weights, routes, columns):
    picks, all_rows = ids.shape
    filler = jnp.zeros((8 - 2 * picks, all_rows), F32)
    routes[...] = jnp.concatenate([ids[...].astype(F32), weights[...], filler], axis=0)
    columns[...] = jnp.transpose(routes[...])


def placed(columns, block, tok_dev, picks, slots, slot_cap, shared):
    own = columns[pl.ds(pl.multiple_of(block * tok_dev, tok_dev), tok_dev), :]
    below = (
        lax.broadcasted_iota(jnp.int32, (tok_dev, tok_dev), 1)
        < lax.broadcasted_iota(jnp.int32, (tok_dev, tok_dev), 0)
    ).astype(BF16)
    labels = lax.broadcasted_iota(jnp.int32, (tok_dev, 128), 1)
    places = lax.broadcasted_iota(jnp.int32, (tok_dev, slots), 1)
    named = [own[:, k : k + 1].astype(jnp.int32) for k in range(picks)]
    share = [own[:, picks + k : picks + k + 1] for k in range(picks)]
    total = functools.reduce(jnp.add, share)
    hot = [(labels == n).astype(F32) for n in named]
    rank = dot(below, functools.reduce(jnp.add, hot).astype(BF16))
    result = jnp.zeros((tok_dev, slots), F32)
    for k in range(picks):
        within = jnp.sum(rank * hot[k], axis=1, keepdims=True).astype(jnp.int32)
        spot = places == named[k] * slot_cap + within
        result = result + jnp.where(spot, share[k] / total if shared else 1.0, 0.0)
    return result


(
    SEL, DXW, D2, PTAB, COMB, MIXP, M2S, MIXG, LOADW, MIXPROD, CONV, Q2S, CONVG, PROJ,
    TAKE, ROWS, EXP, HH, FIN, REST, FARW, GSEL,
) = range(22)

PIECES = 4

GATES = (6,)

END_STEPS = (
    (SEL, 7), (MIXP, 0), (SEL, 0), (SEL, 2), (PTAB, 0), (SEL, 3), (M2S, 1),
    (M2S, 0), (TAKE, 7), (TAKE, 3), (DXW, 0), (D2, 0), (D2, 1), (M2S, 3),
    (ROWS, 0), (M2S, 2), (SEL, 6), (SEL, 1), (SEL, 5), (ROWS, 7), (SEL, 4),
    (TAKE, 6), (MIXG, 0), (LOADW, 0), (EXP, 7), (ROWS, 1), (D2, 3), (D2, 2),
    (TAKE, 4), (TAKE, 1), (COMB, 0), (ROWS, 6), (EXP, 6), (ROWS, 3), (HH, 7),
    (MIXPROD, 0), (FIN, 7), (EXP, 3), (ROWS, 4), (EXP, 4), (HH, 6), (TAKE, 0),
    (TAKE, 5), (FIN, 6), (HH, 3), (EXP, 1), (CONV, 0), (HH, 4), (FIN, 4),
    (EXP, 0), (FIN, 3), (ROWS, 5), (ROWS, 2), (TAKE, 2), (EXP, 5), (EXP, 2),
    (Q2S, 3), (HH, 0), (Q2S, 1), (HH, 5), (HH, 2), (Q2S, 2), (Q2S, 0),
    (FIN, 5), (HH, 1), (FIN, 2), (FIN, 1), (CONVG, 0), (FIN, 0), (PROJ, 0),
)

MIDDLE_STEPS = (
    (MIXP, 0), (SEL, 0), (M2S, 3), (SEL, 3), (PTAB, 0), (M2S, 1), (M2S, 0),
    (M2S, 2), (SEL, 1), (DXW, 0), (D2, 3), (FARW, 6), (GSEL, 4), (TAKE, 0),
    (GSEL, 6), (TAKE, 6), (D2, 0), (GSEL, 7), (D2, 2), (MIXG, 0), (ROWS, 0),
    (LOADW, 0), (EXP, 0), (ROWS, 6), (EXP, 6), (GSEL, 5), (TAKE, 5), (HH, 6),
    (SEL, 2), (TAKE, 4), (D2, 1), (FIN, 6), (MIXPROD, 0), (ROWS, 5), (TAKE, 1),
    (TAKE, 7), (HH, 0), (ROWS, 3), (CONV, 0), (TAKE, 3), (EXP, 3), (ROWS, 4),
    (ROWS, 2), (TAKE, 2), (EXP, 5), (EXP, 4), (ROWS, 1), (HH, 3), (EXP, 1),
    (FIN, 3), (HH, 5), (EXP, 2), (FIN, 5), (ROWS, 7), (HH, 4), (Q2S, 0),
    (HH, 1), (EXP, 7), (Q2S, 1), (FIN, 4), (FIN, 1), (Q2S, 2), (HH, 2),
    (FIN, 2), (HH, 7), (COMB, 0), (FIN, 7), (Q2S, 3), (CONVG, 0), (PROJ, 0),
    (FIN, 0),
)


DISP, F2, F1, G1, H2, H1, HG, RET, DISP2, M2, Q2, FARR, FARI, GD = range(14)
M1, MG, Q1, QG, RIM, DX = range(6)


def looked_up(values, i):
    bit = 1
    while len(values) > 1:
        odd = (i // bit) % 2 == 1
        values = [
            jnp.where(odd, pair[-1], pair[0]) if pair[0] is not pair[-1] else pair[0]
            for pair in (values[n : n + 2] for n in range(0, len(values), 2))
        ]
        bit *= 2
    return values[0]


def choose(stage, low, high, bodies):
    if high - low == 1:
        bodies[low]()
        return
    middle = (low + high) // 2
    for below in (True, False):
        @pl.when((stage < middle) if below else (stage >= middle))
        def _(below=below):
            choose(stage, *((low, middle) if below else (middle, high)), bodies)


def exchange_kernel(
    mixer_in, expert_in, mixer_gain, expert_gain, ids, shares, all_taps,
    w_in, w_out, w_val, w_proj, w_gate, w_up, w_down,
    mixer_out, expert_out,
    v_in, v_out, v_val, v_proj, v_gate, v_up, v_down,
    v_mixer, v_expert, v_mixer_gain, v_expert_gain, v_ids, v_shares, taps,
    columns, normed, own_rows, own_table, outgoing, partner_table, combine,
    rows, arrived, hid, res, returned, gates, ext, rim_out, rim_in, gated, dense, outgoing2, routes, far_rows, far_routes, far_columns, far_tables, far_out, projected, mixed,
    send, recv, send1, recv1, wsem, fsem, osem,
):
    count = outgoing.shape[0]
    group, tok_dev, width = rows.shape
    half = count // 2
    all_rows = group * tok_dev
    chan = v_in.shape[1]
    slot_cap = outgoing.shape[1]
    hid_width = v_gate.shape[1]
    e = lax.axis_index("ep")
    t = lax.axis_index("tp")
    t1 = t + 1 - 2 * (t % 2)
    t2 = (t + 2) % group
    t3 = (t1 + 2) % group

    firsts = [
        pltpu.make_async_copy(a, b, fsem.at[n])
        for n, (a, b) in enumerate(
            [(expert_in, v_expert), (expert_gain, v_expert_gain), (ids, v_ids), (shares, v_shares),
             (mixer_in, v_mixer), (mixer_gain, v_mixer_gain),
             (all_taps.at[:, pl.ds(pl.multiple_of(t * chan, 128), chan)], taps)]
        )
    ]
    for load in firsts:
        load.start()
    loads = [
        pltpu.make_async_copy(a, b, wsem.at[n])
        for n, (a, b) in enumerate(
            [(w_in, v_in), (w_val, v_val), (w_out, v_out), (w_gate.at[0], v_gate),
             (w_up.at[0], v_up), (w_down.at[0], v_down), (w_proj, v_proj)]
        )
    ]
    def xor(a, b):
        value, bit = 0, 1
        while bit < count:
            value = value + ((a // bit + b // bit) % 2) * bit
            bit *= 2
        return value

    def mixed_with(s):
        return xor(e, s)

    middle = (e >= count // 4) & (e < 3 * count // 4)

    barrier = pltpu.get_barrier_semaphore()
    for s in range(1, count):
        pl.semaphore_signal(barrier, inc=1, device_id=(mixed_with(s), t), device_id_type=MESH)
    for peer in (t1, t2):
        pl.semaphore_signal(barrier, inc=1, device_id=(e, peer), device_id_type=MESH)
    for load in firsts[:4]:
        load.wait()
    for load in loads:
        load.start()
    picks = v_ids.shape[0]
    slots = combine.shape[1]

    def table_of(source, block):
        sent = placed(source, block, tok_dev, picks, slots, slot_cap, False)
        return jnp.transpose(sent).astype(BF16).reshape(slots // slot_cap, slot_cap, tok_dev)

    own_rows[...] = rms_rows(v_expert[...], v_expert_gain[...])
    fill_columns(v_ids, v_shares, routes, columns)
    pl.semaphore_wait(barrier, count + 1)

    def chunk(kind, i, src, dst, dev):
        return pltpu.make_async_remote_copy(
            src_ref=src, dst_ref=dst, send_sem=send.at[kind, i], recv_sem=recv.at[kind, i],
            device_id=dev, device_id_type=MESH,
        )

    def once(kind, src, dst, dev):
        return pltpu.make_async_remote_copy(
            src_ref=src, dst_ref=dst, send_sem=send1.at[kind], recv_sem=recv1.at[kind],
            device_id=dev, device_id_type=MESH,
        )

    near, across = (e, t1), (e, t2)
    after = ((e + 1) % count, t)

    def came(kind, i, dst):
        chunk(kind, i, dst, dst, near).wait_recv()

    def came_once(kind, dst):
        once(kind, dst, dst, near).wait_recv()

    def disp(i):
        return chunk(DISP, i, outgoing.at[i], arrived.at[e, t], (mixed_with(i), t))

    def disp2(i):
        return chunk(DISP2, i, outgoing2.at[i], arrived.at[e, t2], (mixed_with(i), t))

    def ret(i):
        return chunk(RET, i, res.at[i], returned.at[e], (mixed_with(i), t))

    def far_pair(gate):
        dev = (mixed_with(gate), t)
        slot = GATES.index(gate)
        return (
            chunk(FARR, slot, own_rows, far_rows.at[slot], dev),
            chunk(FARI, slot, routes, far_routes.at[slot], dev),
        )

    def for_far(act):
        for gate in GATES:
            @pl.when(middle if gate == count - 2 else ~middle)
            def _(gate=gate):
                for copy in far_pair(gate):
                    act(copy)

    for_far(lambda copy: copy.start())
    once(DX, own_rows, dense, across).start()
    own_table[...] = table_of(columns, t)

    def farw(i):
        slot = (i - half) // 2 if len(GATES) > 1 else 0
        for copy in (
            chunk(FARR, slot, far_rows.at[slot], far_rows.at[slot], near),
            chunk(FARI, slot, far_routes.at[slot], far_routes.at[slot], near),
        ):
            copy.wait_recv()
        far_columns[...] = jnp.transpose(far_routes[slot])
        far_tables[slot] = table_of(far_columns, t)

    def passed(i):
        gate = jnp.where(i >= count, GATES[-1], GATES[0])
        slot = i // count
        shift = i % count
        return gate, slot, shift, xor(mixed_with(gate), shift)

    def gsend(i):
        gate, slot, shift, expert = passed(i)
        return pltpu.make_async_remote_copy(
            src_ref=far_out.at[slot, shift - half], dst_ref=arrived.at[mixed_with(gate), t],
            send_sem=send.at[GD, slot * half + shift - half], recv_sem=recv.at[DISP, shift],
            device_id=(expert, t), device_id_type=MESH,
        )

    def gsel(i):
        gate, slot, shift, expert = passed(i)
        picked = dot(far_tables[slot, expert], far_rows[slot]).astype(BF16)

        @pl.when(shift == gate)
        def _():
            arrived[mixed_with(gate), t] = picked

        @pl.when(shift != gate)
        def _():
            far_out[slot, shift - half] = picked
            gsend(i).start()

    def sel(i):
        picked = dot(own_table[mixed_with(i)], own_rows[...]).astype(BF16)

        @pl.when(i == 0)
        def _():
            arrived[e, t] = picked

        @pl.when(i != 0)
        def _():
            outgoing[i] = picked
            disp(i).start()

    def dxw(i):
        came_once(DX, dense)

    def d2(i):
        picked = dot(partner_table[mixed_with(i)], dense[...]).astype(BF16)

        @pl.when(i == 0)
        def _():
            arrived[e, t2] = picked

        @pl.when(i != 0)
        def _():
            outgoing2[i] = picked
            disp2(i).start()

    def mixp(i):
        for load in firsts[4:]:
            load.wait()
        normed[...] = rms_rows(v_mixer[...], v_mixer_gain[...])
        rows[t] = normed[...]
        once(M1, normed, rows.at[t], near).start()

    def ptab(i):
        partner_table[...] = table_of(columns, t2)

    def comb(i):
        def one(block, carry):
            part = pl.ds(pl.multiple_of(block * tok_dev, tok_dev), tok_dev)
            combine[part, :] = placed(columns, block, tok_dev, picks, slots, slot_cap, True)
            return carry

        lax.fori_loop(0, group, one, 0)

    def m2_piece(i, home, dev):
        cols = pl.ds(pl.multiple_of(i * (width // PIECES), 128), width // PIECES)
        return chunk(M2, i, normed.at[:, cols], rows.at[home, :, cols], dev)

    def q2_piece(i, home, dev):
        part = pl.ds(pl.multiple_of(i * (all_rows // PIECES), 16), all_rows // PIECES)
        return chunk(Q2, i, gated.at[home, part], gated.at[home, part], dev)

    def m2(i):
        m2_piece(i, t, across).start()

    def mixg(i):
        for n in range(PIECES):
            m2_piece(n, t2, near).wait_recv()
        once(MG, rows.at[t2], rows.at[t2], near).start()

    def loadw(i):
        for load in loads:
            load.wait()

    def take(i):
        src = mixed_with(i)
        here = i == 0
        for gate in GATES:
            here = here | (middle & (i == gate))

        @pl.when(~here)
        def _():
            came(DISP, i, arrived.at[src, t])

        @pl.when(i >= half)
        def _():
            chunk(F2, i, arrived.at[src, t], arrived.at[src, t], across).start()

        chunk(F1, i, arrived.at[src, t], arrived.at[src, t], near).start()

    def hand_rows(i):
        src = mixed_with(i)

        @pl.when(i >= half)
        def _():
            came(F2, i, arrived.at[src, t2])

        @pl.when((i < half) & (i != 0))
        def _():
            came(DISP2, i, arrived.at[src, t2])

        chunk(G1, i, arrived.at[src, t2], arrived.at[src, t2], near).start()

    def expand(i):
        src = mixed_with(i)
        came(F1, i, arrived.at[src, t1])
        came(G1, i, arrived.at[src, t3])
        x = arrived[src].reshape(group * slot_cap, width)
        gate = dot(x, v_gate[...])
        up = dot(x, v_up[...])
        hid[src, t] = (gate / (1.0 + jnp.exp(-gate)) * up).astype(BF16)
        chunk(H2, i, hid.at[src, t], hid.at[src, t], across).start()
        chunk(H1, i, hid.at[src, t], hid.at[src, t], near).start()

    def hand_hidden(i):
        src = mixed_with(i)
        came(H2, i, hid.at[src, t2])
        chunk(HG, i, hid.at[src, t2], hid.at[src, t2], near).start()

    def finish(i):
        src = mixed_with(i)
        came(H1, i, hid.at[src, t1])
        came(HG, i, hid.at[src, t3])
        total = dot(hid[src, 0], v_down[0:hid_width, :])
        for other in range(1, group):
            total += dot(hid[src, other], v_down[other * hid_width : (other + 1) * hid_width, :])
        total = total.astype(BF16).reshape(group, slot_cap, chan)

        @pl.when(i != 0)
        def _():
            res[i] = total
            ret(i).start()

        @pl.when(i == 0)
        def _():
            returned[src] = total

    tile = 256

    def mixer_products(i):
        came_once(M1, rows.at[t1])
        came_once(MG, rows.at[t3])

        def one(n, carry):
            cols = pl.ds(pl.multiple_of(n * tile, tile), tile)
            x = rows[...].reshape(all_rows, width)
            product = (dot(x, v_in[:, cols]) * dot(x, v_val[:, cols])).astype(BF16)
            ext[pl.ds(8, all_rows), cols] = product.astype(F32)
            rim_out[:, cols] = product[all_rows - 16 :]
            gates[:, cols] = dot(x, v_out[:, cols])
            return carry

        lax.fori_loop(0, chan // tile, one, 0)
        once(RIM, rim_out, rim_in, after).start()

    def mixer_conv(i):
        came_once(RIM, rim_in)
        edge = rim_in[...].astype(F32)[8:16]
        ext[0:8, :] = jnp.where(e == 0, jnp.zeros_like(edge), edge)
        tap_count = taps.shape[0]
        total = taps[0:1, :] * ext[pl.ds(8 - (tap_count - 1), all_rows), :]
        for n in range(1, tap_count):
            total += taps[n : n + 1, :] * ext[pl.ds(8 - (tap_count - 1) + n, all_rows), :]
        gated[t] = (gates[...] * total).astype(BF16)
        once(Q1, gated.at[t], gated.at[t], near).start()

    def q2(i):
        q2_piece(i, t, across).start()

    def convg(i):
        for n in range(PIECES):
            q2_piece(n, t2, near).wait_recv()
        once(QG, gated.at[t2], gated.at[t2], near).start()

    def mixer_project(i):
        came_once(Q1, gated.at[t1])
        came_once(QG, gated.at[t3])

        def one(n, carry):
            cols = pl.ds(pl.multiple_of(n * tile, tile), tile)
            total = dot(gated[0], v_proj[0:chan, cols])
            for other in range(1, group):
                total += dot(gated[other], v_proj[other * chan : (other + 1) * chan, cols])
            projected[:, cols] = total.astype(BF16)
            return carry

        lax.fori_loop(0, chan // tile, one, 0)
        pltpu.make_async_copy(projected, mixer_out, osem.at[group]).start()

    def rest(i):
        pass

    bodies = (
        sel, dxw, d2, ptab, comb, mixp, m2, mixg, loadw, mixer_products, mixer_conv, q2, convg, mixer_project,
        take, hand_rows, expand, hand_hidden, finish, rest, farw, gsel,
    )
    steps = max(len(END_STEPS), len(MIDDLE_STEPS))
    tables = [table + ((REST, 0),) * (steps - len(table)) for table in (END_STEPS, MIDDLE_STEPS)]

    def step(n, carry):
        at = [[looked_up(list(part), n) for part in zip(*table)] for table in tables]
        stage, shift = [jnp.where(middle, inner, outer) for outer, inner in zip(*at)]
        choose(stage, 0, len(bodies), [functools.partial(body, shift) for body in bodies])
        return carry

    lax.fori_loop(0, steps, step, 0)

    def landed(i, carry):
        came(RET, i, returned.at[mixed_with(i)])
        return carry

    lax.fori_loop(1, count, landed, 0)
    for block in range(group):
        part = pl.ds(block * tok_dev, tok_dev)
        mix = combine[part, :]
        high = mix.astype(BF16)
        low = (mix - high.astype(F32)).astype(BF16)
        values = returned[:, block].reshape(count * slot_cap, chan)
        mixed[part, :] = (dot(high, values) + dot(low, values)).astype(BF16)
        pltpu.make_async_copy(mixed.at[part], expert_out.at[part], osem.at[block]).start()

    def drain(i, carry):
        src = mixed_with(i)
        chunk(F1, i, arrived.at[src, t], arrived.at[src, t], near).wait_send()

        @pl.when(i >= half)
        def _():
            chunk(F2, i, arrived.at[src, t], arrived.at[src, t], near).wait_send()

        @pl.when(i != 0)
        def _():
            ret(i).wait_send()

        direct = (i < half) | jnp.where(middle, False, True)

        @pl.when((i != 0) & direct)
        def _():
            disp(i).wait_send()

        @pl.when((i != 0) & (i < half))
        def _():
            disp2(i).wait_send()

        chunk(G1, i, arrived.at[src, t2], arrived.at[src, t2], near).wait_send()
        for kind in (H2, H1):
            chunk(kind, i, hid.at[src, t], hid.at[src, t], near).wait_send()
        chunk(HG, i, hid.at[src, t2], hid.at[src, t2], near).wait_send()
        return carry

    lax.fori_loop(0, count, drain, 0)
    for_far(lambda copy: copy.wait_send())
    pltpu.make_async_copy(projected, mixer_out, osem.at[group]).wait()
    for block in range(group):
        part = pl.ds(block * tok_dev, tok_dev)
        pltpu.make_async_copy(mixed.at[part], expert_out.at[part], osem.at[block]).wait()

    @pl.when(middle)
    def _():
        for slot, gate in enumerate(GATES):
            for shift in range(half, count):
                if shift != gate:
                    gsend(slot * count + shift).wait_send()

    once(M1, normed, rows.at[t], near).wait_send()
    for n in range(PIECES):
        m2_piece(n, t, near).wait_send()
        q2_piece(n, t, near).wait_send()
    once(MG, rows.at[t2], rows.at[t2], near).wait_send()
    once(DX, own_rows, dense, near).wait_send()
    once(Q1, gated.at[t], gated.at[t], near).wait_send()
    once(QG, gated.at[t2], gated.at[t2], near).wait_send()
    once(RIM, rim_out, rim_in, after).wait_send()


def write_kernel(mixer_sum, expert_sum, mixer_out, expert_out, held, sem):
    pairs = [(mixer_sum, mixer_out), (expert_sum, expert_out)]
    inward = [pltpu.make_async_copy(a, held.at[n], sem.at[n]) for n, (a, _) in enumerate(pairs)]
    outward = [pltpu.make_async_copy(held.at[n], b, sem.at[2 + n]) for n, (_, b) in enumerate(pairs)]
    for copy in inward:
        copy.start()
    for first, second in zip(inward, outward):
        first.wait()
        second.start()
    for copy in outward:
        copy.wait()


def fused_on_device(
    mixer_in, expert_in, mixer_gain, in_gate_weight, out_gate_weight, value_weight, conv_taps,
    mixer_proj, expert_gain, route_ids, route_weights, gate_weight, up_weight, down_weight,
):
    tok_dev, width = mixer_in.shape
    group = lax.axis_size("tp")
    count = lax.axis_size("ep")
    experts = count * gate_weight.shape[0]
    slot_cap = 2 * tok_dev * route_ids.shape[1] // experts
    chan = in_gate_weight.shape[1]
    hid_width = gate_weight.shape[2]
    all_rows = group * tok_dev
    anywhere = pl.BlockSpec(memory_space=pl.ANY)
    shape = jax.ShapeDtypeStruct
    weights = (
        in_gate_weight, out_gate_weight, value_weight, mixer_proj, gate_weight, up_weight, down_weight,
    )
    dma = pltpu.SemaphoreType.DMA
    results = pl.pallas_call(
        exchange_kernel,
        out_shape=(shape((all_rows, chan), BF16), shape((all_rows, chan), BF16)),
        in_specs=[pl.BlockSpec(memory_space=pltpu.HBM)] * 14,
        out_specs=(pl.BlockSpec(memory_space=pltpu.HBM),) * 2,
        scratch_shapes=[
            pltpu.VMEM(w.shape[-2:], BF16)
            for w in (in_gate_weight, out_gate_weight, value_weight, mixer_proj,
                      gate_weight, up_weight, down_weight)
        ] + [
            pltpu.VMEM((tok_dev, width), BF16),
            pltpu.VMEM((tok_dev, width), BF16),
            pltpu.VMEM((1, width), F32),
            pltpu.VMEM((1, width), F32),
            pltpu.VMEM(route_ids.shape[::-1], jnp.int32),
            pltpu.VMEM(route_ids.shape[::-1], F32),
            pltpu.VMEM((conv_taps.shape[0], chan), F32),
            pltpu.VMEM((all_rows, 8), F32),
            pltpu.VMEM((tok_dev, width), BF16),
            pltpu.VMEM((tok_dev, width), BF16),
            pltpu.VMEM((experts, slot_cap, tok_dev), BF16),
            pltpu.VMEM((experts, slot_cap, width), BF16),
            pltpu.VMEM((experts, slot_cap, tok_dev), BF16),
            pltpu.VMEM((all_rows, experts * slot_cap), F32),
            pltpu.VMEM((group, tok_dev, width), BF16),
            pltpu.VMEM((count, group, slot_cap, width), BF16),
            pltpu.VMEM((count, group, group * slot_cap, hid_width), BF16),
            pltpu.VMEM((count, group, slot_cap, chan), BF16),
            pltpu.VMEM((count, group, slot_cap, chan), BF16),
            pltpu.VMEM((all_rows, chan), F32),
            pltpu.VMEM((all_rows + 8, chan), F32),
            pltpu.VMEM((16, chan), BF16),
            pltpu.VMEM((16, chan), BF16),
            pltpu.VMEM((group, all_rows, chan), BF16),
            pltpu.VMEM((tok_dev, width), BF16),
            pltpu.VMEM((count // 2, slot_cap, width), BF16),
            pltpu.VMEM((8, all_rows), F32),
            pltpu.VMEM((len(GATES), tok_dev, width), BF16),
            pltpu.VMEM((len(GATES), 8, all_rows), F32),
            pltpu.VMEM((all_rows, 8), F32),
            pltpu.VMEM((len(GATES), experts, slot_cap, tok_dev), BF16),
            pltpu.VMEM((len(GATES), count // 2, slot_cap, width), BF16),
            pltpu.VMEM((all_rows, chan), BF16),
            pltpu.VMEM((all_rows, chan), BF16),
            dma((14, count)), dma((14, count)), dma((6,)), dma((6,)), dma((7,)), dma((7,)), dma((group + 1,)),
        ],
        compiler_params=pltpu.CompilerParams(
            collective_id=0, has_side_effects=True, vmem_limit_bytes=VMEM_BYTES
        ),
        name="exchange",
    )(
        mixer_in, expert_in, mixer_gain[None, :], expert_gain[None, :],
        route_ids.T, route_weights.T, conv_taps, *weights,
    )
    return pl.pallas_call(
        write_kernel,
        out_shape=(shape((all_rows, chan), BF16), shape((all_rows, chan), BF16)),
        in_specs=[anywhere, anywhere],
        out_specs=(anywhere, anywhere),
        scratch_shapes=[pltpu.VMEM((2, all_rows, chan), BF16), dma((4,))],
        compiler_params=pltpu.CompilerParams(vmem_limit_bytes=VMEM_BYTES),
        name="write",
    )(*results)


def body_for(mesh):
    count, group = mesh.shape["ep"], mesh.shape["tp"]

    def body(*args):
        tok_dev, picks, held = args[0].shape[0], args[9].shape[1], args[11].shape[0]
        slot_cap = 2 * tok_dev * picks // (count * held)
        fits = count == 8 and group == 4 and held == 1 and slot_cap % 16 == 0
        return (fused_on_device if fits and tok_dev % 16 == 0 else on_device)(*args)

    return body


def solution(mesh):
    return jax.shard_map(
        body_for(mesh),
        mesh=mesh,
        in_specs=(
            P(("ep", "tp"), None),
            P(("ep", "tp"), None),
            P(),
            P(None, "tp"),
            P(None, "tp"),
            P(None, "tp"),
            P(),
            P(None, "tp"),
            P(),
            P("ep", None),
            P("ep", None),
            P("ep", None, "tp"),
            P("ep", None, "tp"),
            P("ep", None, "tp"),
        ),
        out_specs=(P("ep", "tp"), P("ep", "tp")),
        check_vma=False,
    )
```

```python
import functools

import jax
import jax.numpy as jnp
from jax import lax
from jax.experimental import pallas as pl
from jax.experimental.pallas import tpu as pltpu
from jax.sharding import PartitionSpec as P

norm_eps = 1e-06


def passed_along(value, axis, steps):
    count = lax.axis_size(axis)
    leading, last = (max(0, -steps), min(count, count - steps))
    return lax.ppermute(value, axis, [(source, source + steps) for source in range(leading, last)])


def rms_rows(values, gain_row):
    wide = values.astype(jnp.float32)
    scale = lax.rsqrt(jnp.mean(wide * wide, axis=-1, keepdims=True) + norm_eps)
    return (wide * scale * gain_row).astype(jnp.bfloat16)


def place_slots(route_ids, group_rows, experts, slot_cap):
    row_total, top_count = route_ids.shape
    groups = row_total // group_rows
    labels = jnp.arange(experts, dtype=jnp.int32)
    onehot = (
        route_ids.reshape(groups, group_rows * top_count)[:, :, None] == labels[None, None, :]
    ).astype(jnp.int32)
    earlier = jnp.cumsum(onehot, axis=1) - onehot
    within = jnp.sum(earlier * onehot, axis=2)
    slot_index = jnp.arange(groups, dtype=jnp.int32)[:, None] * slot_cap + within
    return slot_index.reshape(row_total, top_count)


def on_device(
    mixer_in,
    expert_in,
    mixer_gain,
    in_gate_weight,
    out_gate_weight,
    value_weight,
    conv_taps,
    mixer_proj,
    expert_gain,
    route_ids,
    route_weights,
    gate_weight,
    up_weight,
    down_weight,
):
    tok_dev = mixer_in.shape[0]
    tp_count = lax.axis_size("tp")
    ep_count = lax.axis_size("ep")
    top_count = route_ids.shape[1]
    experts = ep_count * gate_weight.shape[0]
    slot_cap = max(2, 2 * tok_dev * top_count // experts)
    tp_index = lax.axis_index("tp")
    mixer_normed = rms_rows(mixer_in, mixer_gain)
    expert_normed = rms_rows(expert_in, expert_gain)
    block_slot = place_slots(route_ids, tok_dev, experts, slot_cap)
    mixer_rows = lax.all_gather(mixer_normed, "tp", axis=0, tiled=True)
    send_ids = lax.dynamic_slice_in_dim(route_ids, tp_index * tok_dev, tok_dev, 0)
    send_slot = (
        lax.dynamic_slice_in_dim(block_slot, tp_index * tok_dev, tok_dev, 0) - tp_index * slot_cap
    )
    source_count = expert_normed.shape[0]
    flat_index = (send_ids * slot_cap + send_slot).reshape(-1)
    row_table = (
        jnp.full((experts * slot_cap,), source_count, jnp.int32)
        .at[flat_index]
        .set(jnp.repeat(jnp.arange(source_count, dtype=jnp.int32), top_count))
    )
    padded_rows = jnp.concatenate(
        [expert_normed, jnp.zeros((1, expert_normed.shape[1]), jnp.bfloat16)], axis=0
    )
    outgoing = padded_rows[row_table].reshape(experts, slot_cap, expert_normed.shape[1])
    arrived = lax.all_to_all(outgoing, "ep", split_axis=0, concat_axis=0, tiled=True)
    arrived = lax.all_gather(arrived, "tp", axis=1, tiled=True)
    chan_width = in_gate_weight.shape[1]
    in_gate = jnp.dot(mixer_rows, in_gate_weight, preferred_element_type=jnp.float32)
    out_gate = jnp.dot(mixer_rows, out_gate_weight, preferred_element_type=jnp.float32)
    values = jnp.dot(mixer_rows, value_weight, preferred_element_type=jnp.float32)
    product = (in_gate * values).astype(jnp.bfloat16)
    tap_count = conv_taps.shape[0]
    rim_rows = passed_along(product[product.shape[0] - (tap_count - 1) :], "ep", 1)
    extended = jnp.concatenate([rim_rows, product], axis=0).astype(jnp.float32)
    tap_rows = lax.dynamic_slice_in_dim(conv_taps, tp_index * chan_width, chan_width, 1)
    row_count = product.shape[0]
    conv_sum = tap_rows[0] * extended[0:row_count]
    for tap_index in range(1, tap_count):
        conv_sum = conv_sum + tap_rows[tap_index] * extended[tap_index : tap_index + row_count]
    gated = (out_gate * conv_sum).astype(jnp.bfloat16)
    slots_in = arrived.reshape(-1, arrived.shape[2])
    gate_pre = jnp.dot(slots_in, gate_weight[0], preferred_element_type=jnp.float32)
    up_pre = jnp.dot(slots_in, up_weight[0], preferred_element_type=jnp.float32)
    hidden = (jax.nn.silu(gate_pre) * up_pre).astype(jnp.bfloat16)
    down_slice = down_weight[0]
    gated_all, hidden_all = (
        lax.all_gather(gated, "tp", axis=1, tiled=True),
        lax.all_gather(hidden, "tp", axis=1, tiled=True),
    )
    mixer_sum = jnp.dot(gated_all, mixer_proj, preferred_element_type=jnp.float32)
    expert_sum = jnp.dot(hidden_all, down_slice, preferred_element_type=jnp.float32)
    mixer_out = mixer_sum.astype(jnp.bfloat16)
    results = expert_sum.astype(jnp.bfloat16).reshape(ep_count, -1, expert_sum.shape[1])
    returned = lax.all_to_all(results, "ep", split_axis=0, concat_axis=0, tiled=True)
    back_index = (route_ids * (tp_count * slot_cap) + block_slot).reshape(-1)
    picked = returned.reshape(-1, returned.shape[2])[back_index].reshape(
        route_ids.shape[0], top_count, -1
    )
    shares = route_weights / jnp.sum(route_weights, axis=1, keepdims=True)
    expert_out = jnp.sum(picked.astype(jnp.float32) * shares[:, :, None], axis=1).astype(
        jnp.bfloat16
    )
    return (mixer_out, expert_out)


MESH = pl.DeviceIdType.MESH
F32 = jnp.float32
BF16 = jnp.bfloat16
VMEM_BYTES = 60 * 1024 * 1024


def dot(a, b):
    return jnp.dot(a, b, preferred_element_type=F32)


def fill_columns(ids, weights, routes, columns):
    picks, all_rows = ids.shape
    filler = jnp.zeros((8 - 2 * picks, all_rows), F32)
    routes[...] = jnp.concatenate([ids[...].astype(F32), weights[...], filler], axis=0)
    columns[...] = jnp.transpose(routes[...])


def placed(columns, block, tok_dev, picks, slots, slot_cap, shared):
    own = columns[pl.ds(pl.multiple_of(block * tok_dev, tok_dev), tok_dev), :]
    below = (
        lax.broadcasted_iota(jnp.int32, (tok_dev, tok_dev), 1)
        < lax.broadcasted_iota(jnp.int32, (tok_dev, tok_dev), 0)
    ).astype(BF16)
    labels = lax.broadcasted_iota(jnp.int32, (tok_dev, 128), 1)
    places = lax.broadcasted_iota(jnp.int32, (tok_dev, slots), 1)
    named = [own[:, k : k + 1].astype(jnp.int32) for k in range(picks)]
    share = [own[:, picks + k : picks + k + 1] for k in range(picks)]
    total = functools.reduce(jnp.add, share)
    hot = [(labels == n).astype(F32) for n in named]
    rank = dot(below, functools.reduce(jnp.add, hot).astype(BF16))
    result = jnp.zeros((tok_dev, slots), F32)
    for k in range(picks):
        within = jnp.sum(rank * hot[k], axis=1, keepdims=True).astype(jnp.int32)
        spot = places == named[k] * slot_cap + within
        result = result + jnp.where(spot, share[k] / total if shared else 1.0, 0.0)
    return result


(
    SEL, DXW, D2, PTAB, COMB, MIXP, M2S, MIXG, LOADW, MIXPROD, CONV, Q2S, CONVG, PROJ,
    TAKE, ROWS, EXP, HH, FIN, REST, FARW, GSEL,
) = range(22)

PIECES = 4

CODES = 512

GATES = (6,)

END_STEPS = (
    (SEL, 7), (MIXP, 0), (SEL, 0), (SEL, 2), (PTAB, 0), (SEL, 3), (M2S, 1),
    (M2S, 0), (TAKE, 7), (TAKE, 3), (DXW, 0), (D2, 0), (D2, 1), (M2S, 3),
    (ROWS, 0), (M2S, 2), (SEL, 6), (SEL, 1), (SEL, 5), (ROWS, 7), (SEL, 4),
    (TAKE, 6), (MIXG, 0), (LOADW, 0), (EXP, 7), (ROWS, 1), (D2, 3), (D2, 2),
    (TAKE, 4), (TAKE, 1), (COMB, 0), (ROWS, 6), (EXP, 6), (ROWS, 3), (HH, 7),
    (MIXPROD, 0), (FIN, 7), (EXP, 3), (ROWS, 4), (EXP, 4), (HH, 6), (TAKE, 0),
    (TAKE, 5), (FIN, 6), (HH, 3), (EXP, 1), (CONV, 0), (HH, 4), (FIN, 4),
    (EXP, 0), (FIN, 3), (ROWS, 5), (ROWS, 2), (TAKE, 2), (EXP, 5), (EXP, 2),
    (Q2S, 3), (HH, 0), (Q2S, 1), (HH, 5), (HH, 2), (Q2S, 2), (Q2S, 0),
    (FIN, 5), (HH, 1), (FIN, 2), (FIN, 1), (CONVG, 0), (FIN, 0), (PROJ, 0),
)

MIDDLE_STEPS = (
    (MIXP, 0), (SEL, 0), (M2S, 3), (SEL, 3), (PTAB, 0), (M2S, 1), (M2S, 0),
    (M2S, 2), (SEL, 1), (DXW, 0), (D2, 3), (FARW, 6), (GSEL, 4), (TAKE, 0),
    (GSEL, 6), (TAKE, 6), (D2, 0), (GSEL, 7), (D2, 2), (MIXG, 0), (ROWS, 0),
    (LOADW, 0), (EXP, 0), (ROWS, 6), (EXP, 6), (GSEL, 5), (TAKE, 5), (HH, 6),
    (SEL, 2), (TAKE, 4), (D2, 1), (FIN, 6), (MIXPROD, 0), (ROWS, 5), (TAKE, 1),
    (TAKE, 7), (HH, 0), (ROWS, 3), (CONV, 0), (TAKE, 3), (EXP, 3), (ROWS, 4),
    (ROWS, 2), (TAKE, 2), (EXP, 5), (EXP, 4), (ROWS, 1), (HH, 3), (EXP, 1),
    (FIN, 3), (HH, 5), (EXP, 2), (FIN, 5), (ROWS, 7), (HH, 4), (Q2S, 0),
    (HH, 1), (EXP, 7), (Q2S, 1), (FIN, 4), (FIN, 1), (Q2S, 2), (HH, 2),
    (FIN, 2), (HH, 7), (COMB, 0), (FIN, 7), (Q2S, 3), (CONVG, 0), (PROJ, 0),
    (FIN, 0),
)


DISP, F2, F1, G1, H2, H1, HG, RET, DISP2, M2, Q2, FARR, FARI, GD = range(14)
M1, MG, Q1, QG, RIM, DX = range(6)


def looked_up(values, i):
    bit = 1
    while len(values) > 1:
        odd = (i // bit) % 2 == 1
        values = [
            jnp.where(odd, pair[-1], pair[0]) if pair[0] is not pair[-1] else pair[0]
            for pair in (values[n : n + 2] for n in range(0, len(values), 2))
        ]
        bit *= 2
    return values[0]


def choose(stage, low, high, bodies):
    if high - low == 1:
        bodies[low]()
        return
    middle = (low + high) // 2
    for below in (True, False):
        @pl.when((stage < middle) if below else (stage >= middle))
        def _(below=below):
            choose(stage, *((low, middle) if below else (middle, high)), bodies)


def exchange_kernel(
    mixer_in, expert_in, mixer_gain, expert_gain, ids, shares, all_taps,
    w_in, w_out, w_val, w_proj, w_gate, w_up, w_down,
    mixer_out, expert_out,
    v_in, v_out, v_val, v_proj, v_gate, v_up, v_down,
    v_mixer, v_expert, v_mixer_gain, v_expert_gain, v_ids, v_shares, taps,
    columns, normed, own_rows, own_table, outgoing, partner_table, combine,
    rows, arrived, hid, res, returned, gates, ext, rim_out, rim_in, gated, dense, outgoing2, routes, far_rows, far_routes, far_columns, far_tables, far_out, projected, mixed,
    send, recv, send1, recv1, wsem, fsem, osem,
):
    count = outgoing.shape[0]
    group, tok_dev, width = rows.shape
    half = count // 2
    all_rows = group * tok_dev
    chan = v_in.shape[1]
    slot_cap = outgoing.shape[1]
    hid_width = v_gate.shape[1]
    e = lax.axis_index("ep")
    t = lax.axis_index("tp")
    t1 = t + 1 - 2 * (t % 2)
    t2 = (t + 2) % group
    t3 = (t1 + 2) % group

    firsts = [
        pltpu.make_async_copy(a, b, fsem.at[n])
        for n, (a, b) in enumerate(
            [(expert_in, v_expert), (expert_gain, v_expert_gain), (ids, v_ids), (shares, v_shares),
             (mixer_in, v_mixer), (mixer_gain, v_mixer_gain),
             (all_taps.at[:, pl.ds(pl.multiple_of(t * chan, 128), chan)], taps)]
        )
    ]
    for load in firsts:
        load.start()
    loads = [
        pltpu.make_async_copy(a, b, wsem.at[n])
        for n, (a, b) in enumerate(
            [(w_in, v_in), (w_val, v_val), (w_out, v_out), (w_gate.at[0], v_gate),
             (w_up.at[0], v_up), (w_down.at[0], v_down), (w_proj, v_proj)]
        )
    ]
    def xor(a, b):
        value, bit = 0, 1
        while bit < count:
            value = value + ((a // bit + b // bit) % 2) * bit
            bit *= 2
        return value

    def mixed_with(s):
        return xor(e, s)

    middle = (e >= count // 4) & (e < 3 * count // 4)

    barrier = pltpu.get_barrier_semaphore()
    for s in range(1, count):
        pl.semaphore_signal(barrier, inc=1, device_id=(mixed_with(s), t), device_id_type=MESH)
    for peer in (t1, t2):
        pl.semaphore_signal(barrier, inc=1, device_id=(e, peer), device_id_type=MESH)
    for load in firsts[:4]:
        load.wait()
    for load in loads:
        load.start()
    picks = v_ids.shape[0]
    slots = combine.shape[1]

    def table_of(source, block):
        sent = placed(source, block, tok_dev, picks, slots, slot_cap, False)
        return jnp.transpose(sent).astype(BF16).reshape(slots // slot_cap, slot_cap, tok_dev)

    own_rows[...] = rms_rows(v_expert[...], v_expert_gain[...])
    fill_columns(v_ids, v_shares, routes, columns)
    own_table[...] = table_of(columns, t)
    pl.semaphore_wait(barrier, count + 1)

    def chunk(kind, i, src, dst, dev):
        return pltpu.make_async_remote_copy(
            src_ref=src, dst_ref=dst, send_sem=send.at[kind, i], recv_sem=recv.at[kind, i],
            device_id=dev, device_id_type=MESH,
        )

    def once(kind, src, dst, dev):
        return pltpu.make_async_remote_copy(
            src_ref=src, dst_ref=dst, send_sem=send1.at[kind], recv_sem=recv1.at[kind],
            device_id=dev, device_id_type=MESH,
        )

    near, across = (e, t1), (e, t2)
    after = ((e + 1) % count, t)

    def came(kind, i, dst):
        chunk(kind, i, dst, dst, near).wait_recv()

    def came_once(kind, dst):
        once(kind, dst, dst, near).wait_recv()

    def disp(i):
        return chunk(DISP, i, outgoing.at[i], arrived.at[e, t], (mixed_with(i), t))

    def disp2(i):
        return chunk(DISP2, i, outgoing2.at[i], arrived.at[e, t2], (mixed_with(i), t))

    def ret(i):
        return chunk(RET, i, res.at[i], returned.at[e], (mixed_with(i), t))

    def far_pair(gate):
        dev = (mixed_with(gate), t)
        slot = GATES.index(gate)
        return (
            chunk(FARR, slot, own_rows, far_rows.at[slot], dev),
            chunk(FARI, slot, routes, far_routes.at[slot], dev),
        )

    def for_far(act):
        for gate in GATES:
            @pl.when(middle if gate == count - 2 else ~middle)
            def _(gate=gate):
                for copy in far_pair(gate):
                    act(copy)

    for_far(lambda copy: copy.start())
    once(DX, own_rows, dense, across).start()

    def farw(i):
        slot = (i - half) // 2 if len(GATES) > 1 else 0
        for copy in (
            chunk(FARR, slot, far_rows.at[slot], far_rows.at[slot], near),
            chunk(FARI, slot, far_routes.at[slot], far_routes.at[slot], near),
        ):
            copy.wait_recv()
        far_columns[...] = jnp.transpose(far_routes[slot])
        far_tables[slot] = table_of(far_columns, t)

    def passed(i):
        gate = jnp.where(i >= count, GATES[-1], GATES[0])
        slot = i // count
        shift = i % count
        return gate, slot, shift, xor(mixed_with(gate), shift)

    def gsend(i):
        gate, slot, shift, expert = passed(i)
        return pltpu.make_async_remote_copy(
            src_ref=far_out.at[slot, shift - half], dst_ref=arrived.at[mixed_with(gate), t],
            send_sem=send.at[GD, slot * half + shift - half], recv_sem=recv.at[DISP, shift],
            device_id=(expert, t), device_id_type=MESH,
        )

    def gsel(i):
        gate, slot, shift, expert = passed(i)
        picked = dot(far_tables[slot, expert], far_rows[slot]).astype(BF16)

        @pl.when(shift == gate)
        def _():
            arrived[mixed_with(gate), t] = picked

        @pl.when(shift != gate)
        def _():
            far_out[slot, shift - half] = picked
            gsend(i).start()

    def sel(i):
        picked = dot(own_table[mixed_with(i)], own_rows[...]).astype(BF16)

        @pl.when(i == 0)
        def _():
            arrived[e, t] = picked

        @pl.when(i != 0)
        def _():
            outgoing[i] = picked
            disp(i).start()

    def dxw(i):
        came_once(DX, dense)

    def d2(i):
        picked = dot(partner_table[mixed_with(i)], dense[...]).astype(BF16)

        @pl.when(i == 0)
        def _():
            arrived[e, t2] = picked

        @pl.when(i != 0)
        def _():
            outgoing2[i] = picked
            disp2(i).start()

    def mixp(i):
        for load in firsts[4:]:
            load.wait()
        normed[...] = rms_rows(v_mixer[...], v_mixer_gain[...])
        rows[t] = normed[...]
        once(M1, normed, rows.at[t], near).start()

    def ptab(i):
        partner_table[...] = table_of(columns, t2)

    def comb(i):
        def one(block, carry):
            part = pl.ds(pl.multiple_of(block * tok_dev, tok_dev), tok_dev)
            combine[part, :] = placed(columns, block, tok_dev, picks, slots, slot_cap, True)
            return carry

        lax.fori_loop(0, group, one, 0)

    def m2_piece(i, home, dev):
        cols = pl.ds(pl.multiple_of(i * (width // PIECES), 128), width // PIECES)
        return chunk(M2, i, normed.at[:, cols], rows.at[home, :, cols], dev)

    def q2_piece(i, home, dev):
        part = pl.ds(pl.multiple_of(i * (all_rows // PIECES), 16), all_rows // PIECES)
        return chunk(Q2, i, gated.at[home, part], gated.at[home, part], dev)

    def m2(i):
        m2_piece(i, t, across).start()

    def mixg(i):
        for n in range(PIECES):
            m2_piece(n, t2, near).wait_recv()
        once(MG, rows.at[t2], rows.at[t2], near).start()

    def loadw(i):
        for load in loads:
            load.wait()

    def take(i):
        src = mixed_with(i)
        here = i == 0
        for gate in GATES:
            here = here | (middle & (i == gate))

        @pl.when(~here)
        def _():
            came(DISP, i, arrived.at[src, t])

        @pl.when(i >= half)
        def _():
            chunk(F2, i, arrived.at[src, t], arrived.at[src, t], across).start()

        chunk(F1, i, arrived.at[src, t], arrived.at[src, t], near).start()

    def hand_rows(i):
        src = mixed_with(i)

        @pl.when(i >= half)
        def _():
            came(F2, i, arrived.at[src, t2])

        @pl.when((i < half) & (i != 0))
        def _():
            came(DISP2, i, arrived.at[src, t2])

        chunk(G1, i, arrived.at[src, t2], arrived.at[src, t2], near).start()

    def expand(i):
        src = mixed_with(i)
        came(F1, i, arrived.at[src, t1])
        came(G1, i, arrived.at[src, t3])
        x = arrived[src].reshape(group * slot_cap, width)
        gate = dot(x, v_gate[...])
        up = dot(x, v_up[...])
        hid[src, t] = (gate / (1.0 + jnp.exp(-gate)) * up).astype(BF16)
        chunk(H2, i, hid.at[src, t], hid.at[src, t], across).start()
        chunk(H1, i, hid.at[src, t], hid.at[src, t], near).start()

    def hand_hidden(i):
        src = mixed_with(i)
        came(H2, i, hid.at[src, t2])
        chunk(HG, i, hid.at[src, t2], hid.at[src, t2], near).start()

    def finish(i):
        src = mixed_with(i)
        came(H1, i, hid.at[src, t1])
        came(HG, i, hid.at[src, t3])
        total = dot(hid[src, 0], v_down[0:hid_width, :])
        for other in range(1, group):
            total += dot(hid[src, other], v_down[other * hid_width : (other + 1) * hid_width, :])
        total = total.astype(BF16).reshape(group, slot_cap, chan)

        @pl.when(i != 0)
        def _():
            res[i] = total
            ret(i).start()

        @pl.when(i == 0)
        def _():
            returned[src] = total

    tile = 256

    def mixer_products(i):
        came_once(M1, rows.at[t1])
        came_once(MG, rows.at[t3])

        def one(n, carry):
            cols = pl.ds(pl.multiple_of(n * tile, tile), tile)
            x = rows[...].reshape(all_rows, width)
            product = (dot(x, v_in[:, cols]) * dot(x, v_val[:, cols])).astype(BF16)
            ext[pl.ds(8, all_rows), cols] = product.astype(F32)
            rim_out[:, cols] = product[all_rows - 16 :]
            gates[:, cols] = dot(x, v_out[:, cols])
            return carry

        lax.fori_loop(0, chan // tile, one, 0)
        once(RIM, rim_out, rim_in, after).start()

    def mixer_conv(i):
        came_once(RIM, rim_in)
        edge = rim_in[...].astype(F32)[8:16]
        ext[0:8, :] = jnp.where(e == 0, jnp.zeros_like(edge), edge)
        tap_count = taps.shape[0]
        total = taps[0:1, :] * ext[pl.ds(8 - (tap_count - 1), all_rows), :]
        for n in range(1, tap_count):
            total += taps[n : n + 1, :] * ext[pl.ds(8 - (tap_count - 1) + n, all_rows), :]
        gated[t] = (gates[...] * total).astype(BF16)
        once(Q1, gated.at[t], gated.at[t], near).start()

    def q2(i):
        q2_piece(i, t, across).start()

    def convg(i):
        for n in range(PIECES):
            q2_piece(n, t2, near).wait_recv()
        once(QG, gated.at[t2], gated.at[t2], near).start()

    def mixer_project(i):
        came_once(Q1, gated.at[t1])
        came_once(QG, gated.at[t3])

        def one(n, carry):
            cols = pl.ds(pl.multiple_of(n * tile, tile), tile)
            total = dot(gated[0], v_proj[0:chan, cols])
            for other in range(1, group):
                total += dot(gated[other], v_proj[other * chan : (other + 1) * chan, cols])
            projected[:, cols] = total.astype(BF16)
            return carry

        lax.fori_loop(0, chan // tile, one, 0)
        pltpu.make_async_copy(projected, mixer_out, osem.at[group]).start()

    def rest(i):
        pass

    bodies = (
        sel, dxw, d2, ptab, comb, mixp, m2, mixg, loadw, mixer_products, mixer_conv, q2, convg, mixer_project,
        take, hand_rows, expand, hand_hidden, finish, rest, farw, gsel,
    )
    steps = max(len(END_STEPS), len(MIDDLE_STEPS))
    tables = [table + ((REST, 0),) * (steps - len(table)) for table in (END_STEPS, MIDDLE_STEPS)]

    packed = [
        (inner[0] * 16 + inner[1]) * CODES + outer[0] * 16 + outer[1]
        for outer, inner in zip(*tables)
    ]

    def step(n, carry):
        both = looked_up(packed, n)
        mine = jnp.where(middle, both // CODES, both % CODES)
        stage, shift = mine // 16, mine % 16
        choose(stage, 0, len(bodies), [functools.partial(body, shift) for body in bodies])
        return carry

    lax.fori_loop(0, steps, step, 0)

    def landed(i, carry):
        came(RET, i, returned.at[mixed_with(i)])
        return carry

    lax.fori_loop(1, count, landed, 0)
    for block in range(group):
        part = pl.ds(block * tok_dev, tok_dev)
        mix = combine[part, :]
        high = mix.astype(BF16)
        low = (mix - high.astype(F32)).astype(BF16)
        values = returned[:, block].reshape(count * slot_cap, chan)
        mixed[part, :] = (dot(high, values) + dot(low, values)).astype(BF16)
        pltpu.make_async_copy(mixed.at[part], expert_out.at[part], osem.at[block]).start()

    def drain(i, carry):
        src = mixed_with(i)
        chunk(F1, i, arrived.at[src, t], arrived.at[src, t], near).wait_send()

        @pl.when(i >= half)
        def _():
            chunk(F2, i, arrived.at[src, t], arrived.at[src, t], near).wait_send()

        @pl.when(i != 0)
        def _():
            ret(i).wait_send()

        direct = (i < half) | jnp.where(middle, False, True)

        @pl.when((i != 0) & direct)
        def _():
            disp(i).wait_send()

        @pl.when((i != 0) & (i < half))
        def _():
            disp2(i).wait_send()

        chunk(G1, i, arrived.at[src, t2], arrived.at[src, t2], near).wait_send()
        for kind in (H2, H1):
            chunk(kind, i, hid.at[src, t], hid.at[src, t], near).wait_send()
        chunk(HG, i, hid.at[src, t2], hid.at[src, t2], near).wait_send()
        return carry

    lax.fori_loop(0, count, drain, 0)
    for_far(lambda copy: copy.wait_send())
    pltpu.make_async_copy(projected, mixer_out, osem.at[group]).wait()
    for block in range(group):
        part = pl.ds(block * tok_dev, tok_dev)
        pltpu.make_async_copy(mixed.at[part], expert_out.at[part], osem.at[block]).wait()

    @pl.when(middle)
    def _():
        for slot, gate in enumerate(GATES):
            for shift in range(half, count):
                if shift != gate:
                    gsend(slot * count + shift).wait_send()

    once(M1, normed, rows.at[t], near).wait_send()
    for n in range(PIECES):
        m2_piece(n, t, near).wait_send()
        q2_piece(n, t, near).wait_send()
    once(MG, rows.at[t2], rows.at[t2], near).wait_send()
    once(DX, own_rows, dense, near).wait_send()
    once(Q1, gated.at[t], gated.at[t], near).wait_send()
    once(QG, gated.at[t2], gated.at[t2], near).wait_send()
    once(RIM, rim_out, rim_in, after).wait_send()


def write_kernel(mixer_sum, expert_sum, mixer_out, expert_out, held, sem):
    pairs = [(mixer_sum, mixer_out), (expert_sum, expert_out)]
    inward = [pltpu.make_async_copy(a, held.at[n], sem.at[n]) for n, (a, _) in enumerate(pairs)]
    outward = [pltpu.make_async_copy(held.at[n], b, sem.at[2 + n]) for n, (_, b) in enumerate(pairs)]
    for copy in inward:
        copy.start()
    for first, second in zip(inward, outward):
        first.wait()
        second.start()
    for copy in outward:
        copy.wait()


def fused_on_device(
    mixer_in, expert_in, mixer_gain, in_gate_weight, out_gate_weight, value_weight, conv_taps,
    mixer_proj, expert_gain, route_ids, route_weights, gate_weight, up_weight, down_weight,
):
    tok_dev, width = mixer_in.shape
    group = lax.axis_size("tp")
    count = lax.axis_size("ep")
    experts = count * gate_weight.shape[0]
    slot_cap = 2 * tok_dev * route_ids.shape[1] // experts
    chan = in_gate_weight.shape[1]
    hid_width = gate_weight.shape[2]
    all_rows = group * tok_dev
    anywhere = pl.BlockSpec(memory_space=pl.ANY)
    shape = jax.ShapeDtypeStruct
    weights = (
        in_gate_weight, out_gate_weight, value_weight, mixer_proj, gate_weight, up_weight, down_weight,
    )
    dma = pltpu.SemaphoreType.DMA
    results = pl.pallas_call(
        exchange_kernel,
        out_shape=(shape((all_rows, chan), BF16), shape((all_rows, chan), BF16)),
        in_specs=[pl.BlockSpec(memory_space=pltpu.HBM)] * 14,
        out_specs=(pl.BlockSpec(memory_space=pltpu.HBM),) * 2,
        scratch_shapes=[
            pltpu.VMEM(w.shape[-2:], BF16)
            for w in (in_gate_weight, out_gate_weight, value_weight, mixer_proj,
                      gate_weight, up_weight, down_weight)
        ] + [
            pltpu.VMEM((tok_dev, width), BF16),
            pltpu.VMEM((tok_dev, width), BF16),
            pltpu.VMEM((1, width), F32),
            pltpu.VMEM((1, width), F32),
            pltpu.VMEM(route_ids.shape[::-1], jnp.int32),
            pltpu.VMEM(route_ids.shape[::-1], F32),
            pltpu.VMEM((conv_taps.shape[0], chan), F32),
            pltpu.VMEM((all_rows, 8), F32),
            pltpu.VMEM((tok_dev, width), BF16),
            pltpu.VMEM((tok_dev, width), BF16),
            pltpu.VMEM((experts, slot_cap, tok_dev), BF16),
            pltpu.VMEM((experts, slot_cap, width), BF16),
            pltpu.VMEM((experts, slot_cap, tok_dev), BF16),
            pltpu.VMEM((all_rows, experts * slot_cap), F32),
            pltpu.VMEM((group, tok_dev, width), BF16),
            pltpu.VMEM((count, group, slot_cap, width), BF16),
            pltpu.VMEM((count, group, group * slot_cap, hid_width), BF16),
            pltpu.VMEM((count, group, slot_cap, chan), BF16),
            pltpu.VMEM((count, group, slot_cap, chan), BF16),
            pltpu.VMEM((all_rows, chan), F32),
            pltpu.VMEM((all_rows + 8, chan), F32),
            pltpu.VMEM((16, chan), BF16),
            pltpu.VMEM((16, chan), BF16),
            pltpu.VMEM((group, all_rows, chan), BF16),
            pltpu.VMEM((tok_dev, width), BF16),
            pltpu.VMEM((count // 2, slot_cap, width), BF16),
            pltpu.VMEM((8, all_rows), F32),
            pltpu.VMEM((len(GATES), tok_dev, width), BF16),
            pltpu.VMEM((len(GATES), 8, all_rows), F32),
            pltpu.VMEM((all_rows, 8), F32),
            pltpu.VMEM((len(GATES), experts, slot_cap, tok_dev), BF16),
            pltpu.VMEM((len(GATES), count // 2, slot_cap, width), BF16),
            pltpu.VMEM((all_rows, chan), BF16),
            pltpu.VMEM((all_rows, chan), BF16),
            dma((14, count)), dma((14, count)), dma((6,)), dma((6,)), dma((7,)), dma((7,)), dma((group + 1,)),
        ],
        compiler_params=pltpu.CompilerParams(
            collective_id=0, has_side_effects=True, vmem_limit_bytes=VMEM_BYTES
        ),
        name="exchange",
    )(
        mixer_in, expert_in, mixer_gain[None, :], expert_gain[None, :],
        route_ids.T, route_weights.T, conv_taps, *weights,
    )
    return pl.pallas_call(
        write_kernel,
        out_shape=(shape((all_rows, chan), BF16), shape((all_rows, chan), BF16)),
        in_specs=[anywhere, anywhere],
        out_specs=(anywhere, anywhere),
        scratch_shapes=[pltpu.VMEM((2, all_rows, chan), BF16), dma((4,))],
        compiler_params=pltpu.CompilerParams(vmem_limit_bytes=VMEM_BYTES),
        name="write",
    )(*results)


def body_for(mesh):
    count, group = mesh.shape["ep"], mesh.shape["tp"]

    def body(*args):
        tok_dev, picks, held = args[0].shape[0], args[9].shape[1], args[11].shape[0]
        slot_cap = 2 * tok_dev * picks // (count * held)
        fits = count == 8 and group == 4 and held == 1 and slot_cap % 16 == 0
        return (fused_on_device if fits and tok_dev % 16 == 0 else on_device)(*args)

    return body


def solution(mesh):
    return jax.shard_map(
        body_for(mesh),
        mesh=mesh,
        in_specs=(
            P(("ep", "tp"), None),
            P(("ep", "tp"), None),
            P(),
            P(None, "tp"),
            P(None, "tp"),
            P(None, "tp"),
            P(),
            P(None, "tp"),
            P(),
            P("ep", None),
            P("ep", None),
            P("ep", None, "tp"),
            P("ep", None, "tp"),
            P("ep", None, "tp"),
        ),
        out_specs=(P("ep", "tp"), P("ep", "tp")),
        check_vma=False,
    )
```

```python
import functools

import jax
import jax.numpy as jnp
from jax import lax
from jax.experimental import pallas as pl
from jax.experimental.pallas import tpu as pltpu
from jax.sharding import PartitionSpec as P

norm_eps = 1e-06


def passed_along(value, axis, steps):
    count = lax.axis_size(axis)
    leading, last = (max(0, -steps), min(count, count - steps))
    return lax.ppermute(value, axis, [(source, source + steps) for source in range(leading, last)])


def rms_rows(values, gain_row):
    wide = values.astype(jnp.float32)
    scale = lax.rsqrt(jnp.mean(wide * wide, axis=-1, keepdims=True) + norm_eps)
    return (wide * scale * gain_row).astype(jnp.bfloat16)


def place_slots(route_ids, group_rows, experts, slot_cap):
    row_total, top_count = route_ids.shape
    groups = row_total // group_rows
    labels = jnp.arange(experts, dtype=jnp.int32)
    onehot = (
        route_ids.reshape(groups, group_rows * top_count)[:, :, None] == labels[None, None, :]
    ).astype(jnp.int32)
    earlier = jnp.cumsum(onehot, axis=1) - onehot
    within = jnp.sum(earlier * onehot, axis=2)
    slot_index = jnp.arange(groups, dtype=jnp.int32)[:, None] * slot_cap + within
    return slot_index.reshape(row_total, top_count)


def on_device(
    mixer_in,
    expert_in,
    mixer_gain,
    in_gate_weight,
    out_gate_weight,
    value_weight,
    conv_taps,
    mixer_proj,
    expert_gain,
    route_ids,
    route_weights,
    gate_weight,
    up_weight,
    down_weight,
):
    tok_dev = mixer_in.shape[0]
    tp_count = lax.axis_size("tp")
    ep_count = lax.axis_size("ep")
    top_count = route_ids.shape[1]
    experts = ep_count * gate_weight.shape[0]
    slot_cap = max(2, 2 * tok_dev * top_count // experts)
    tp_index = lax.axis_index("tp")
    mixer_normed = rms_rows(mixer_in, mixer_gain)
    expert_normed = rms_rows(expert_in, expert_gain)
    block_slot = place_slots(route_ids, tok_dev, experts, slot_cap)
    mixer_rows = lax.all_gather(mixer_normed, "tp", axis=0, tiled=True)
    send_ids = lax.dynamic_slice_in_dim(route_ids, tp_index * tok_dev, tok_dev, 0)
    send_slot = (
        lax.dynamic_slice_in_dim(block_slot, tp_index * tok_dev, tok_dev, 0) - tp_index * slot_cap
    )
    source_count = expert_normed.shape[0]
    flat_index = (send_ids * slot_cap + send_slot).reshape(-1)
    row_table = (
        jnp.full((experts * slot_cap,), source_count, jnp.int32)
        .at[flat_index]
        .set(jnp.repeat(jnp.arange(source_count, dtype=jnp.int32), top_count))
    )
    padded_rows = jnp.concatenate(
        [expert_normed, jnp.zeros((1, expert_normed.shape[1]), jnp.bfloat16)], axis=0
    )
    outgoing = padded_rows[row_table].reshape(experts, slot_cap, expert_normed.shape[1])
    arrived = lax.all_to_all(outgoing, "ep", split_axis=0, concat_axis=0, tiled=True)
    arrived = lax.all_gather(arrived, "tp", axis=1, tiled=True)
    chan_width = in_gate_weight.shape[1]
    in_gate = jnp.dot(mixer_rows, in_gate_weight, preferred_element_type=jnp.float32)
    out_gate = jnp.dot(mixer_rows, out_gate_weight, preferred_element_type=jnp.float32)
    values = jnp.dot(mixer_rows, value_weight, preferred_element_type=jnp.float32)
    product = (in_gate * values).astype(jnp.bfloat16)
    tap_count = conv_taps.shape[0]
    rim_rows = passed_along(product[product.shape[0] - (tap_count - 1) :], "ep", 1)
    extended = jnp.concatenate([rim_rows, product], axis=0).astype(jnp.float32)
    tap_rows = lax.dynamic_slice_in_dim(conv_taps, tp_index * chan_width, chan_width, 1)
    row_count = product.shape[0]
    conv_sum = tap_rows[0] * extended[0:row_count]
    for tap_index in range(1, tap_count):
        conv_sum = conv_sum + tap_rows[tap_index] * extended[tap_index : tap_index + row_count]
    gated = (out_gate * conv_sum).astype(jnp.bfloat16)
    slots_in = arrived.reshape(-1, arrived.shape[2])
    gate_pre = jnp.dot(slots_in, gate_weight[0], preferred_element_type=jnp.float32)
    up_pre = jnp.dot(slots_in, up_weight[0], preferred_element_type=jnp.float32)
    hidden = (jax.nn.silu(gate_pre) * up_pre).astype(jnp.bfloat16)
    down_slice = down_weight[0]
    gated_all, hidden_all = (
        lax.all_gather(gated, "tp", axis=1, tiled=True),
        lax.all_gather(hidden, "tp", axis=1, tiled=True),
    )
    mixer_sum = jnp.dot(gated_all, mixer_proj, preferred_element_type=jnp.float32)
    expert_sum = jnp.dot(hidden_all, down_slice, preferred_element_type=jnp.float32)
    mixer_out = mixer_sum.astype(jnp.bfloat16)
    results = expert_sum.astype(jnp.bfloat16).reshape(ep_count, -1, expert_sum.shape[1])
    returned = lax.all_to_all(results, "ep", split_axis=0, concat_axis=0, tiled=True)
    back_index = (route_ids * (tp_count * slot_cap) + block_slot).reshape(-1)
    picked = returned.reshape(-1, returned.shape[2])[back_index].reshape(
        route_ids.shape[0], top_count, -1
    )
    shares = route_weights / jnp.sum(route_weights, axis=1, keepdims=True)
    expert_out = jnp.sum(picked.astype(jnp.float32) * shares[:, :, None], axis=1).astype(
        jnp.bfloat16
    )
    return (mixer_out, expert_out)


MESH = pl.DeviceIdType.MESH
F32 = jnp.float32
BF16 = jnp.bfloat16
VMEM_BYTES = 60 * 1024 * 1024


def dot(a, b):
    return jnp.dot(a, b, preferred_element_type=F32)


def fill_columns(ids, weights, routes, columns):
    picks, all_rows = ids.shape
    filler = jnp.zeros((8 - 2 * picks, all_rows), F32)
    routes[...] = jnp.concatenate([ids[...].astype(F32), weights[...], filler], axis=0)
    columns[...] = jnp.transpose(routes[...])


def placed(columns, block, tok_dev, picks, slots, slot_cap, shared):
    own = columns[pl.ds(pl.multiple_of(block * tok_dev, tok_dev), tok_dev), :]
    below = (
        lax.broadcasted_iota(jnp.int32, (tok_dev, tok_dev), 1)
        < lax.broadcasted_iota(jnp.int32, (tok_dev, tok_dev), 0)
    ).astype(BF16)
    labels = lax.broadcasted_iota(jnp.int32, (tok_dev, 128), 1)
    places = lax.broadcasted_iota(jnp.int32, (tok_dev, slots), 1)
    named = [own[:, k : k + 1].astype(jnp.int32) for k in range(picks)]
    share = [own[:, picks + k : picks + k + 1] for k in range(picks)]
    total = functools.reduce(jnp.add, share)
    hot = [(labels == n).astype(F32) for n in named]
    rank = dot(below, functools.reduce(jnp.add, hot).astype(BF16))
    result = jnp.zeros((tok_dev, slots), F32)
    for k in range(picks):
        within = jnp.sum(rank * hot[k], axis=1, keepdims=True).astype(jnp.int32)
        spot = places == named[k] * slot_cap + within
        result = result + jnp.where(spot, share[k] / total if shared else 1.0, 0.0)
    return result


(
    SEL, DXW, D2, PTAB, COMB, MIXP, M2S, MIXG, LOADW, MIXPROD, CONV, Q2S, CONVG, PROJ,
    TAKE, ROWS, EXP, HH, FIN, REST, FARW, GSEL,
) = range(22)

PIECES = 4

CODES = 512

GATES = (6,)

END_STEPS = (
    (SEL, 7), (MIXP, 0), (SEL, 0), (SEL, 2), (PTAB, 0), (SEL, 3), (M2S, 1),
    (M2S, 0), (TAKE, 7), (TAKE, 3), (DXW, 0), (D2, 0), (D2, 1), (M2S, 3),
    (ROWS, 0), (M2S, 2), (SEL, 6), (SEL, 1), (SEL, 5), (ROWS, 7), (SEL, 4),
    (TAKE, 6), (MIXG, 0), (LOADW, 0), (EXP, 7), (ROWS, 1), (D2, 3), (D2, 2),
    (TAKE, 4), (TAKE, 1), (COMB, 0), (ROWS, 6), (EXP, 6), (ROWS, 3), (HH, 7),
    (MIXPROD, 0), (FIN, 7), (EXP, 3), (ROWS, 4), (EXP, 4), (HH, 6), (TAKE, 0),
    (TAKE, 5), (FIN, 6), (HH, 3), (EXP, 1), (CONV, 0), (HH, 4), (FIN, 4),
    (EXP, 0), (FIN, 3), (ROWS, 5), (ROWS, 2), (TAKE, 2), (EXP, 5), (EXP, 2),
    (Q2S, 3), (HH, 0), (Q2S, 1), (HH, 5), (HH, 2), (Q2S, 2), (Q2S, 0),
    (FIN, 5), (HH, 1), (FIN, 2), (FIN, 1), (CONVG, 0), (FIN, 0), (PROJ, 0),
)

MIDDLE_STEPS = (
    (MIXP, 0), (SEL, 0), (M2S, 3), (SEL, 3), (PTAB, 0), (M2S, 1), (M2S, 0),
    (M2S, 2), (SEL, 1), (DXW, 0), (D2, 3), (FARW, 6), (GSEL, 4), (TAKE, 0),
    (GSEL, 6), (TAKE, 6), (D2, 0), (GSEL, 7), (D2, 2), (MIXG, 0), (ROWS, 0),
    (LOADW, 0), (EXP, 0), (ROWS, 6), (EXP, 6), (GSEL, 5), (TAKE, 5), (HH, 6),
    (SEL, 2), (TAKE, 4), (D2, 1), (FIN, 6), (MIXPROD, 0), (ROWS, 5), (TAKE, 1),
    (TAKE, 7), (HH, 0), (ROWS, 3), (CONV, 0), (TAKE, 3), (EXP, 3), (ROWS, 4),
    (ROWS, 2), (TAKE, 2), (EXP, 5), (EXP, 4), (ROWS, 1), (HH, 3), (EXP, 1),
    (FIN, 3), (HH, 5), (EXP, 2), (FIN, 5), (ROWS, 7), (HH, 4), (Q2S, 0),
    (HH, 1), (EXP, 7), (Q2S, 1), (FIN, 4), (FIN, 1), (Q2S, 2), (HH, 2),
    (FIN, 2), (HH, 7), (COMB, 0), (FIN, 7), (Q2S, 3), (CONVG, 0), (PROJ, 0),
    (FIN, 0),
)


DISP, F2, F1, G1, H2, H1, HG, RET, DISP2, M2, Q2, FARR, FARI, GD = range(14)
M1, MG, Q1, QG, RIM, DX = range(6)


def looked_up(values, i):
    bit = 1
    while len(values) > 1:
        odd = (i // bit) % 2 == 1
        values = [
            jnp.where(odd, pair[-1], pair[0]) if pair[0] is not pair[-1] else pair[0]
            for pair in (values[n : n + 2] for n in range(0, len(values), 2))
        ]
        bit *= 2
    return values[0]


def choose(stage, low, high, bodies):
    if high - low == 1:
        bodies[low]()
        return
    middle = (low + high) // 2
    for below in (True, False):
        @pl.when((stage < middle) if below else (stage >= middle))
        def _(below=below):
            choose(stage, *((low, middle) if below else (middle, high)), bodies)


def exchange_kernel(
    mixer_in, expert_in, mixer_gain, expert_gain, ids, shares, all_taps,
    w_in, w_out, w_val, w_proj, w_gate, w_up, w_down,
    mixer_out, expert_out,
    v_in, v_out, v_val, v_proj, v_gate, v_up, v_down,
    v_mixer, v_expert, v_mixer_gain, v_expert_gain, v_ids, v_shares, taps,
    columns, normed, own_rows, own_table, outgoing, partner_table, combine,
    rows, arrived, hid, res, returned, gates, ext, rim_out, rim_in, gated, dense, outgoing2, routes, far_rows, far_routes, far_columns, far_tables, far_out, projected, mixed,
    send, recv, send1, recv1, wsem, fsem, osem,
):
    count = outgoing.shape[0]
    group, tok_dev, width = rows.shape
    half = count // 2
    all_rows = group * tok_dev
    chan = v_in.shape[1]
    slot_cap = outgoing.shape[1]
    hid_width = v_gate.shape[1]
    e = lax.axis_index("ep")
    t = lax.axis_index("tp")
    t1 = t + 1 - 2 * (t % 2)
    t2 = (t + 2) % group
    t3 = (t1 + 2) % group

    firsts = [
        pltpu.make_async_copy(a, b, fsem.at[n])
        for n, (a, b) in enumerate(
            [(expert_in, v_expert), (expert_gain, v_expert_gain), (ids, v_ids), (shares, v_shares),
             (mixer_in, v_mixer), (mixer_gain, v_mixer_gain),
             (all_taps.at[:, pl.ds(pl.multiple_of(t * chan, 128), chan)], taps)]
        )
    ]
    for load in firsts:
        load.start()
    loads = [
        pltpu.make_async_copy(a, b, wsem.at[n])
        for n, (a, b) in enumerate(
            [(w_in, v_in), (w_val, v_val), (w_out, v_out), (w_gate.at[0], v_gate),
             (w_up.at[0], v_up), (w_down.at[0], v_down), (w_proj, v_proj)]
        )
    ]
    def xor(a, b):
        value, bit = 0, 1
        while bit < count:
            value = value + ((a // bit + b // bit) % 2) * bit
            bit *= 2
        return value

    def mixed_with(s):
        return xor(e, s)

    middle = (e >= count // 4) & (e < 3 * count // 4)

    barrier = pltpu.get_barrier_semaphore()
    for s in range(1, count):
        pl.semaphore_signal(barrier, inc=1, device_id=(mixed_with(s), t), device_id_type=MESH)
    for peer in (t1, t2):
        pl.semaphore_signal(barrier, inc=1, device_id=(e, peer), device_id_type=MESH)
    for load in firsts[:4]:
        load.wait()
    for load in loads:
        load.start()
    picks = v_ids.shape[0]
    slots = combine.shape[2]

    def table_of(source, block):
        sent = placed(source, block, tok_dev, picks, slots, slot_cap, False)
        return jnp.transpose(sent).astype(BF16).reshape(slots // slot_cap, slot_cap, tok_dev)

    own_rows[...] = rms_rows(v_expert[...], v_expert_gain[...])
    fill_columns(v_ids, v_shares, routes, columns)
    own_table[...] = table_of(columns, t)
    pl.semaphore_wait(barrier, count + 1)

    def chunk(kind, i, src, dst, dev):
        return pltpu.make_async_remote_copy(
            src_ref=src, dst_ref=dst, send_sem=send.at[kind, i], recv_sem=recv.at[kind, i],
            device_id=dev, device_id_type=MESH,
        )

    def once(kind, src, dst, dev):
        return pltpu.make_async_remote_copy(
            src_ref=src, dst_ref=dst, send_sem=send1.at[kind], recv_sem=recv1.at[kind],
            device_id=dev, device_id_type=MESH,
        )

    near, across = (e, t1), (e, t2)
    after = ((e + 1) % count, t)

    def came(kind, i, dst):
        chunk(kind, i, dst, dst, near).wait_recv()

    def came_once(kind, dst):
        once(kind, dst, dst, near).wait_recv()

    def disp(i):
        return chunk(DISP, i, outgoing.at[i], arrived.at[e, t], (mixed_with(i), t))

    def disp2(i):
        return chunk(DISP2, i, outgoing2.at[i], arrived.at[e, t2], (mixed_with(i), t))

    def ret(i):
        return chunk(RET, i, res.at[i], returned.at[e], (mixed_with(i), t))

    def far_pair(gate):
        dev = (mixed_with(gate), t)
        slot = GATES.index(gate)
        return (
            chunk(FARR, slot, own_rows, far_rows.at[slot], dev),
            chunk(FARI, slot, routes, far_routes.at[slot], dev),
        )

    def for_far(act):
        for gate in GATES:
            @pl.when(middle if gate == count - 2 else ~middle)
            def _(gate=gate):
                for copy in far_pair(gate):
                    act(copy)

    for_far(lambda copy: copy.start())
    once(DX, own_rows, dense, across).start()

    def farw(i):
        slot = (i - half) // 2 if len(GATES) > 1 else 0
        for copy in (
            chunk(FARR, slot, far_rows.at[slot], far_rows.at[slot], near),
            chunk(FARI, slot, far_routes.at[slot], far_routes.at[slot], near),
        ):
            copy.wait_recv()
        far_columns[...] = jnp.transpose(far_routes[slot])
        far_tables[slot] = table_of(far_columns, t)

    def passed(i):
        gate = jnp.where(i >= count, GATES[-1], GATES[0])
        slot = i // count
        shift = i % count
        return gate, slot, shift, xor(mixed_with(gate), shift)

    def gsend(i):
        gate, slot, shift, expert = passed(i)
        return pltpu.make_async_remote_copy(
            src_ref=far_out.at[slot, shift - half], dst_ref=arrived.at[mixed_with(gate), t],
            send_sem=send.at[GD, slot * half + shift - half], recv_sem=recv.at[DISP, shift],
            device_id=(expert, t), device_id_type=MESH,
        )

    def gsel(i):
        gate, slot, shift, expert = passed(i)
        picked = dot(far_tables[slot, expert], far_rows[slot]).astype(BF16)

        @pl.when(shift == gate)
        def _():
            arrived[mixed_with(gate), t] = picked

        @pl.when(shift != gate)
        def _():
            far_out[slot, shift - half] = picked
            gsend(i).start()

    def sel(i):
        picked = dot(own_table[mixed_with(i)], own_rows[...]).astype(BF16)

        @pl.when(i == 0)
        def _():
            arrived[e, t] = picked

        @pl.when(i != 0)
        def _():
            outgoing[i] = picked
            disp(i).start()

    def dxw(i):
        came_once(DX, dense)

    def d2(i):
        picked = dot(partner_table[mixed_with(i)], dense[...]).astype(BF16)

        @pl.when(i == 0)
        def _():
            arrived[e, t2] = picked

        @pl.when(i != 0)
        def _():
            outgoing2[i] = picked
            disp2(i).start()

    def mixp(i):
        for load in firsts[4:]:
            load.wait()
        normed[...] = rms_rows(v_mixer[...], v_mixer_gain[...])
        rows[t] = normed[...]
        once(M1, normed, rows.at[t], near).start()

    def ptab(i):
        partner_table[...] = table_of(columns, t2)

    def comb(i):
        def one(block, carry):
            part = pl.ds(pl.multiple_of(block * tok_dev, tok_dev), tok_dev)
            mix = placed(columns, block, tok_dev, picks, slots, slot_cap, True)
            high = mix.astype(BF16)
            combine[0, part, :] = high
            combine[1, part, :] = (mix - high.astype(F32)).astype(BF16)
            return carry

        lax.fori_loop(0, group, one, 0)

    def m2_piece(i, home, dev):
        cols = pl.ds(pl.multiple_of(i * (width // PIECES), 128), width // PIECES)
        return chunk(M2, i, normed.at[:, cols], rows.at[home, :, cols], dev)

    def q2_piece(i, home, dev):
        part = pl.ds(pl.multiple_of(i * (all_rows // PIECES), 16), all_rows // PIECES)
        return chunk(Q2, i, gated.at[home, part], gated.at[home, part], dev)

    def m2(i):
        m2_piece(i, t, across).start()

    def mixg(i):
        for n in range(PIECES):
            m2_piece(n, t2, near).wait_recv()
        once(MG, rows.at[t2], rows.at[t2], near).start()

    def loadw(i):
        for load in loads:
            load.wait()

    def take(i):
        src = mixed_with(i)
        here = i == 0
        for gate in GATES:
            here = here | (middle & (i == gate))

        @pl.when(~here)
        def _():
            came(DISP, i, arrived.at[src, t])

        @pl.when(i >= half)
        def _():
            chunk(F2, i, arrived.at[src, t], arrived.at[src, t], across).start()

        chunk(F1, i, arrived.at[src, t], arrived.at[src, t], near).start()

    def hand_rows(i):
        src = mixed_with(i)

        @pl.when(i >= half)
        def _():
            came(F2, i, arrived.at[src, t2])

        @pl.when((i < half) & (i != 0))
        def _():
            came(DISP2, i, arrived.at[src, t2])

        chunk(G1, i, arrived.at[src, t2], arrived.at[src, t2], near).start()

    def expand(i):
        src = mixed_with(i)
        came(F1, i, arrived.at[src, t1])
        came(G1, i, arrived.at[src, t3])
        x = arrived[src].reshape(group * slot_cap, width)
        gate = dot(x, v_gate[...])
        up = dot(x, v_up[...])
        hid[src, t] = (gate / (1.0 + jnp.exp(-gate)) * up).astype(BF16)
        chunk(H2, i, hid.at[src, t], hid.at[src, t], across).start()
        chunk(H1, i, hid.at[src, t], hid.at[src, t], near).start()

    def hand_hidden(i):
        src = mixed_with(i)
        came(H2, i, hid.at[src, t2])
        chunk(HG, i, hid.at[src, t2], hid.at[src, t2], near).start()

    def finish(i):
        src = mixed_with(i)
        came(H1, i, hid.at[src, t1])
        came(HG, i, hid.at[src, t3])
        total = dot(hid[src, 0], v_down[0:hid_width, :])
        for other in range(1, group):
            total += dot(hid[src, other], v_down[other * hid_width : (other + 1) * hid_width, :])
        total = total.astype(BF16).reshape(group, slot_cap, chan)

        @pl.when(i != 0)
        def _():
            res[i] = total
            ret(i).start()

        @pl.when(i == 0)
        def _():
            returned[src] = total

    tile = 256

    def mixer_products(i):
        came_once(M1, rows.at[t1])
        came_once(MG, rows.at[t3])

        def one(n, carry):
            cols = pl.ds(pl.multiple_of(n * tile, tile), tile)
            x = rows[...].reshape(all_rows, width)
            product = (dot(x, v_in[:, cols]) * dot(x, v_val[:, cols])).astype(BF16)
            ext[pl.ds(8, all_rows), cols] = product.astype(F32)
            rim_out[:, cols] = product[all_rows - 16 :]
            gates[:, cols] = dot(x, v_out[:, cols])
            return carry

        lax.fori_loop(0, chan // tile, one, 0)
        once(RIM, rim_out, rim_in, after).start()

    def mixer_conv(i):
        came_once(RIM, rim_in)
        edge = rim_in[...].astype(F32)[8:16]
        ext[0:8, :] = jnp.where(e == 0, jnp.zeros_like(edge), edge)
        tap_count = taps.shape[0]
        total = taps[0:1, :] * ext[pl.ds(8 - (tap_count - 1), all_rows), :]
        for n in range(1, tap_count):
            total += taps[n : n + 1, :] * ext[pl.ds(8 - (tap_count - 1) + n, all_rows), :]
        gated[t] = (gates[...] * total).astype(BF16)
        once(Q1, gated.at[t], gated.at[t], near).start()

    def q2(i):
        q2_piece(i, t, across).start()

    def convg(i):
        for n in range(PIECES):
            q2_piece(n, t2, near).wait_recv()
        once(QG, gated.at[t2], gated.at[t2], near).start()

    def mixer_project(i):
        came_once(Q1, gated.at[t1])
        came_once(QG, gated.at[t3])

        def one(n, carry):
            cols = pl.ds(pl.multiple_of(n * tile, tile), tile)
            total = dot(gated[0], v_proj[0:chan, cols])
            for other in range(1, group):
                total += dot(gated[other], v_proj[other * chan : (other + 1) * chan, cols])
            projected[:, cols] = total.astype(BF16)
            return carry

        lax.fori_loop(0, chan // tile, one, 0)
        pltpu.make_async_copy(projected, mixer_out, osem.at[group]).start()

    def rest(i):
        pass

    bodies = (
        sel, dxw, d2, ptab, comb, mixp, m2, mixg, loadw, mixer_products, mixer_conv, q2, convg, mixer_project,
        take, hand_rows, expand, hand_hidden, finish, rest, farw, gsel,
    )
    steps = max(len(END_STEPS), len(MIDDLE_STEPS))
    tables = [table + ((REST, 0),) * (steps - len(table)) for table in (END_STEPS, MIDDLE_STEPS)]

    packed = [
        (inner[0] * 16 + inner[1]) * CODES + outer[0] * 16 + outer[1]
        for outer, inner in zip(*tables)
    ]

    def step(n, carry):
        both = looked_up(packed, n)
        mine = jnp.where(middle, both // CODES, both % CODES)
        stage, shift = mine // 16, mine % 16
        choose(stage, 0, len(bodies), [functools.partial(body, shift) for body in bodies])
        return carry

    lax.fori_loop(0, steps, step, 0)

    def landed(i, carry):
        came(RET, i, returned.at[mixed_with(i)])
        return carry

    lax.fori_loop(1, count, landed, 0)
    for block in range(group):
        part = pl.ds(block * tok_dev, tok_dev)
        high, low = combine[0, part, :], combine[1, part, :]
        values = returned[:, block].reshape(count * slot_cap, chan)
        mixed[part, :] = (dot(high, values) + dot(low, values)).astype(BF16)
        pltpu.make_async_copy(mixed.at[part], expert_out.at[part], osem.at[block]).start()

    def drain(i, carry):
        src = mixed_with(i)
        chunk(F1, i, arrived.at[src, t], arrived.at[src, t], near).wait_send()

        @pl.when(i >= half)
        def _():
            chunk(F2, i, arrived.at[src, t], arrived.at[src, t], near).wait_send()

        @pl.when(i != 0)
        def _():
            ret(i).wait_send()

        direct = (i < half) | jnp.where(middle, False, True)

        @pl.when((i != 0) & direct)
        def _():
            disp(i).wait_send()

        @pl.when((i != 0) & (i < half))
        def _():
            disp2(i).wait_send()

        chunk(G1, i, arrived.at[src, t2], arrived.at[src, t2], near).wait_send()
        for kind in (H2, H1):
            chunk(kind, i, hid.at[src, t], hid.at[src, t], near).wait_send()
        chunk(HG, i, hid.at[src, t2], hid.at[src, t2], near).wait_send()
        return carry

    lax.fori_loop(0, count, drain, 0)
    for_far(lambda copy: copy.wait_send())
    pltpu.make_async_copy(projected, mixer_out, osem.at[group]).wait()
    for block in range(group):
        part = pl.ds(block * tok_dev, tok_dev)
        pltpu.make_async_copy(mixed.at[part], expert_out.at[part], osem.at[block]).wait()

    @pl.when(middle)
    def _():
        for slot, gate in enumerate(GATES):
            for shift in range(half, count):
                if shift != gate:
                    gsend(slot * count + shift).wait_send()

    once(M1, normed, rows.at[t], near).wait_send()
    for n in range(PIECES):
        m2_piece(n, t, near).wait_send()
        q2_piece(n, t, near).wait_send()
    once(MG, rows.at[t2], rows.at[t2], near).wait_send()
    once(DX, own_rows, dense, near).wait_send()
    once(Q1, gated.at[t], gated.at[t], near).wait_send()
    once(QG, gated.at[t2], gated.at[t2], near).wait_send()
    once(RIM, rim_out, rim_in, after).wait_send()


def write_kernel(mixer_sum, expert_sum, mixer_out, expert_out, held, sem):
    pairs = [(mixer_sum, mixer_out), (expert_sum, expert_out)]
    inward = [pltpu.make_async_copy(a, held.at[n], sem.at[n]) for n, (a, _) in enumerate(pairs)]
    outward = [pltpu.make_async_copy(held.at[n], b, sem.at[2 + n]) for n, (_, b) in enumerate(pairs)]
    for copy in inward:
        copy.start()
    for first, second in zip(inward, outward):
        first.wait()
        second.start()
    for copy in outward:
        copy.wait()


def fused_on_device(
    mixer_in, expert_in, mixer_gain, in_gate_weight, out_gate_weight, value_weight, conv_taps,
    mixer_proj, expert_gain, route_ids, route_weights, gate_weight, up_weight, down_weight,
):
    tok_dev, width = mixer_in.shape
    group = lax.axis_size("tp")
    count = lax.axis_size("ep")
    experts = count * gate_weight.shape[0]
    slot_cap = 2 * tok_dev * route_ids.shape[1] // experts
    chan = in_gate_weight.shape[1]
    hid_width = gate_weight.shape[2]
    all_rows = group * tok_dev
    anywhere = pl.BlockSpec(memory_space=pl.ANY)
    shape = jax.ShapeDtypeStruct
    weights = (
        in_gate_weight, out_gate_weight, value_weight, mixer_proj, gate_weight, up_weight, down_weight,
    )
    dma = pltpu.SemaphoreType.DMA
    results = pl.pallas_call(
        exchange_kernel,
        out_shape=(shape((all_rows, chan), BF16), shape((all_rows, chan), BF16)),
        in_specs=[pl.BlockSpec(memory_space=pltpu.HBM)] * 14,
        out_specs=(pl.BlockSpec(memory_space=pltpu.HBM),) * 2,
        scratch_shapes=[
            pltpu.VMEM(w.shape[-2:], BF16)
            for w in (in_gate_weight, out_gate_weight, value_weight, mixer_proj,
                      gate_weight, up_weight, down_weight)
        ] + [
            pltpu.VMEM((tok_dev, width), BF16),
            pltpu.VMEM((tok_dev, width), BF16),
            pltpu.VMEM((1, width), F32),
            pltpu.VMEM((1, width), F32),
            pltpu.VMEM(route_ids.shape[::-1], jnp.int32),
            pltpu.VMEM(route_ids.shape[::-1], F32),
            pltpu.VMEM((conv_taps.shape[0], chan), F32),
            pltpu.VMEM((all_rows, 8), F32),
            pltpu.VMEM((tok_dev, width), BF16),
            pltpu.VMEM((tok_dev, width), BF16),
            pltpu.VMEM((experts, slot_cap, tok_dev), BF16),
            pltpu.VMEM((experts, slot_cap, width), BF16),
            pltpu.VMEM((experts, slot_cap, tok_dev), BF16),
            pltpu.VMEM((2, all_rows, experts * slot_cap), BF16),
            pltpu.VMEM((group, tok_dev, width), BF16),
            pltpu.VMEM((count, group, slot_cap, width), BF16),
            pltpu.VMEM((count, group, group * slot_cap, hid_width), BF16),
            pltpu.VMEM((count, group, slot_cap, chan), BF16),
            pltpu.VMEM((count, group, slot_cap, chan), BF16),
            pltpu.VMEM((all_rows, chan), F32),
            pltpu.VMEM((all_rows + 8, chan), F32),
            pltpu.VMEM((16, chan), BF16),
            pltpu.VMEM((16, chan), BF16),
            pltpu.VMEM((group, all_rows, chan), BF16),
            pltpu.VMEM((tok_dev, width), BF16),
            pltpu.VMEM((count // 2, slot_cap, width), BF16),
            pltpu.VMEM((8, all_rows), F32),
            pltpu.VMEM((len(GATES), tok_dev, width), BF16),
            pltpu.VMEM((len(GATES), 8, all_rows), F32),
            pltpu.VMEM((all_rows, 8), F32),
            pltpu.VMEM((len(GATES), experts, slot_cap, tok_dev), BF16),
            pltpu.VMEM((len(GATES), count // 2, slot_cap, width), BF16),
            pltpu.VMEM((all_rows, chan), BF16),
            pltpu.VMEM((all_rows, chan), BF16),
            dma((14, count)), dma((14, count)), dma((6,)), dma((6,)), dma((7,)), dma((7,)), dma((group + 1,)),
        ],
        compiler_params=pltpu.CompilerParams(
            collective_id=0, has_side_effects=True, vmem_limit_bytes=VMEM_BYTES
        ),
        name="exchange",
    )(
        mixer_in, expert_in, mixer_gain[None, :], expert_gain[None, :],
        route_ids.T, route_weights.T, conv_taps, *weights,
    )
    return pl.pallas_call(
        write_kernel,
        out_shape=(shape((all_rows, chan), BF16), shape((all_rows, chan), BF16)),
        in_specs=[anywhere, anywhere],
        out_specs=(anywhere, anywhere),
        scratch_shapes=[pltpu.VMEM((2, all_rows, chan), BF16), dma((4,))],
        compiler_params=pltpu.CompilerParams(vmem_limit_bytes=VMEM_BYTES),
        name="write",
    )(*results)


def body_for(mesh):
    count, group = mesh.shape["ep"], mesh.shape["tp"]

    def body(*args):
        tok_dev, picks, held = args[0].shape[0], args[9].shape[1], args[11].shape[0]
        slot_cap = 2 * tok_dev * picks // (count * held)
        fits = count == 8 and group == 4 and held == 1 and slot_cap % 16 == 0
        return (fused_on_device if fits and tok_dev % 16 == 0 else on_device)(*args)

    return body


def solution(mesh):
    return jax.shard_map(
        body_for(mesh),
        mesh=mesh,
        in_specs=(
            P(("ep", "tp"), None),
            P(("ep", "tp"), None),
            P(),
            P(None, "tp"),
            P(None, "tp"),
            P(None, "tp"),
            P(),
            P(None, "tp"),
            P(),
            P("ep", None),
            P("ep", None),
            P("ep", None, "tp"),
            P("ep", None, "tp"),
            P("ep", None, "tp"),
        ),
        out_specs=(P("ep", "tp"), P("ep", "tp")),
        check_vma=False,
    )
```
